256 devices in a mesh: sp: 32 (over z, x), tp: 8 (over y, core).
Axes of the slice: x: 4, y: 4, z: 8, core: 2. Of those that a mesh axis runs over, the one named last changes fastest.
Arguments:
- tokens: bfloat16 [32768, 2048], P('sp', 'tp'), may hold values from -6 to 6
- norm_gain: float32 [2048], replicated, may hold values from 0.1 to 1.9
- att_query: bfloat16 [2048, 1024], P(None, 'tp'), may hold values from -1 to 1, as said below
- att_key: bfloat16 [2048, 512], P(None, 'tp'), may hold values from -16 to 16, as said below
- att_value: bfloat16 [2048, 512], P(None, 'tp'), may hold values from -0.125 to 0.125
- ret_query: bfloat16 [2048, 512], P(None, 'tp'), may hold values from -0.125 to 0.125
- ret_key: bfloat16 [2048, 512], P(None, 'tp'), may hold values from -0.125 to 0.125
- ret_value: bfloat16 [2048, 1024], P(None, 'tp'), may hold values from -0.125 to 0.125
- ret_gate: bfloat16 [2048, 1024], P(None, 'tp'), may hold values from -0.125 to 0.125
- att_sink: float32 [16], P('tp'), may hold values from 4 to 7
- decay_log: float32 [8, 32768], P('tp', 'sp'), may hold values from -2 to 0, as said below
- init_state: float32 [2, 8, 64, 128], P(None, 'tp'), may hold values from -24 to 24
- out_att: bfloat16 [1024, 2048], P('tp'), may hold values from -0.125 to 0.125
- out_ret: bfloat16 [1024, 2048], P('tp'), may hold values from -0.125 to 0.125
Outputs:
- mixed: bfloat16 [32768, 2048], P('sp', 'tp')
The draws below stay inside these ranges and needn't reach their ends.
Inputs may be any that keep to these rules, and one draw needn't show every extreme that they name: `att_query`: entries of order D ** -0.5. `att_key`: entries of order D ** -0.5 or larger. `decay_log`: log decays, negative.
All inputs are finite; a program needn't handle non-finite values.
Results may differ from the reference program's by a relative error of at most 0.02.
Values may be sent and summed in bfloat16 or wider, within the bound.
A program may use at most 64 MiB of HBM per device.

```python
import math
import jax
import jax.numpy as jnp
from jax import lax

D = 2048
ATT_HEADS = 16
KV_HEADS = 8
HD = 64
RET_HEADS = 8
RK = 64
RV = 128
WINDOW = 128
RET_BLOCK = 128
TOK_DEV = 1024
SEQUENCE_LENGTH = 32768
N_TP = 8


def draw_tokens(key, part):
    base_rows = jnp.clip(jax.random.normal(key, (SEQUENCE_LENGTH, D), jnp.float32), -6.0, 6.0)
    return base_rows.astype(jnp.bfloat16)


def attention_weights(key):
    query_w = jnp.clip(jax.random.normal(jax.random.fold_in(key, 11), (D, ATT_HEADS * HD), jnp.float32), -4.0, 4.0) * D ** (-0.5)
    key_w = jnp.clip(jax.random.normal(jax.random.fold_in(key, 12), (D, KV_HEADS * HD), jnp.float32), -4.0, 4.0) * D ** (-0.5)
    return (query_w, key_w)


def draw_att_query(key, part):
    return attention_weights(key)[0].astype(jnp.bfloat16)


def draw_att_key(key, part):
    return attention_weights(key)[1].astype(jnp.bfloat16)


def draw_decay_log(key, part):
    child_random_keys = jax.random.split(key, 7)
    slow_heads = jax.random.uniform(child_random_keys[0], (RET_HEADS,)) < 0.5
    slow_rate = 0.15 * math.log(10.0) / SEQUENCE_LENGTH * jax.random.uniform(child_random_keys[1], (RET_HEADS,), minval=0.5, maxval=1.5)
    fast_rate = jax.random.uniform(child_random_keys[2], (RET_HEADS,), minval=1.0 / 100.0, maxval=1.0 / 30.0)
    baseline_rate = jnp.where(slow_heads, slow_rate, fast_rate)
    device_pace = jnp.exp(jax.random.uniform(child_random_keys[3], (SEQUENCE_LENGTH // TOK_DEV,), minval=math.log(0.5), maxval=math.log(2.0)))
    full_speed = jnp.repeat(device_pace, TOK_DEV, total_repeat_length=SEQUENCE_LENGTH)
    jaggedness = jax.random.uniform(child_random_keys[4], (RET_HEADS, SEQUENCE_LENGTH), minval=0.5, maxval=1.5)
    spike_positions = jax.random.randint(child_random_keys[5], (3,), 0, SEQUENCE_LENGTH)
    spike_depth = jax.random.uniform(child_random_keys[6], (3,), minval=0.55, maxval=0.85)
    spike_count = jnp.zeros((SEQUENCE_LENGTH,), jnp.float32).at[spike_positions].add(jnp.log(spike_depth))
    return -baseline_rate[:, None] * full_speed[None, :] * jaggedness + spike_count[None, :]


def block_scale(rng, dims, pieces, smallest, largest):
    def one(position, shards_of):
        heights = jax.random.uniform(jax.random.fold_in(jax.random.fold_in(rng, 6), position), (shards_of,), jnp.float32, smallest / len(pieces), largest / len(pieces))
        return jnp.repeat(jnp.exp(heights), dims[position] // shards_of).reshape((-1,) + (1,) * (len(dims) - position - 1))

    loudness = one(*pieces[0])
    for cut in pieces[1:]:
        loudness = loudness * one(*cut)
    return loudness


def scatter_about(own_key, extent, scale, limit, cuts=(), held_as=jnp.bfloat16):
    result = jax.random.normal(own_key, extent, jnp.float32) * scale
    if len(cuts) > 0:
        result = block_scale(own_key, extent, cuts, -0.22, 0.18) * result
    return jnp.clip(result, min=-limit, max=limit).astype(held_as)


def setup_inputs(seed: int = 0) -> dict:
    seeds = jax.random.split(jax.random.key(seed), 15)
    tokens = draw_tokens(jax.random.fold_in(seeds[14], 71), 0)
    norm_gain = jnp.clip(1.0 + 0.18 * jax.random.normal(seeds[1], (D,), jnp.float32), 0.1, 1.9)
    att_query = draw_att_query(jax.random.fold_in(seeds[14], 71), 0)
    att_key = draw_att_key(jax.random.fold_in(seeds[14], 71), 0)
    att_value = scatter_about(seeds[4], (D, KV_HEADS * HD), D ** -0.5, 0.125, ((1, 8),))
    ret_query = scatter_about(seeds[5], (D, RET_HEADS * RK), D ** -0.5, 0.125, ((1, 8),))
    ret_key = scatter_about(seeds[6], (D, RET_HEADS * RK), D ** -0.5, 0.125, ((1, 8),))
    ret_value = scatter_about(seeds[7], (D, RET_HEADS * RV), D ** -0.5, 0.125, ((1, 8),))
    ret_gate = scatter_about(seeds[8], (D, RET_HEADS * RV), D ** -0.5, 0.125, ((1, 8),))
    att_sink = jnp.clip(4.0 + 3.0 * jax.random.uniform(seeds[9], (ATT_HEADS,), jnp.float32) ** block_scale(seeds[9], (ATT_HEADS,), ((0, 8),), -0.2, 0.2), 4.0, 7.0)
    decay_log = draw_decay_log(jax.random.fold_in(seeds[14], 71), 0)
    init_state = scatter_about(seeds[11], (2, RET_HEADS, RK, RV), 4.0, 24.0, ((1, 8),), jnp.float32)
    out_att = scatter_about(seeds[12], (ATT_HEADS * HD, D), (ATT_HEADS * HD + RET_HEADS * RV) ** -0.5, 0.125, ((0, 8),))
    out_ret = scatter_about(seeds[13], (RET_HEADS * RV, D), (ATT_HEADS * HD + RET_HEADS * RV) ** -0.5, 0.125, ((0, 8),))
    return dict(tokens=tokens, norm_gain=norm_gain, att_query=att_query, att_key=att_key, att_value=att_value, ret_query=ret_query, ret_key=ret_key, ret_value=ret_value, ret_gate=ret_gate, att_sink=att_sink, decay_log=decay_log, init_state=init_state, out_att=out_att, out_ret=out_ret)


NORM_EPS = 1e-06
ROPE_BASE = 10000.0
HIGHEST = lax.Precision.HIGHEST

def rotated(values, positions):
    half_dim = values.shape[-1] // 2
    inverse = ROPE_BASE ** (-2.0 * jnp.arange(half_dim, dtype=jnp.float32) / values.shape[-1])
    angles = positions.astype(jnp.float32)[:, None] * inverse[None, :]
    cosine = jnp.cos(angles)[:, None, :]
    sine = jnp.sin(angles)[:, None, :]
    first_half = values[..., :half_dim]
    second_half = values[..., half_dim:]
    return jnp.concatenate([first_half * cosine - second_half * sine, first_half * sine + second_half * cosine], axis=-1)

def attend_all(queries, key_proj, value_proj, att_sink):
    seq_len = queries.shape[0]
    block_rows = 512
    groups = ATT_HEADS // KV_HEADS
    span_rows = block_rows + 2 * WINDOW
    padded_keys = jnp.pad(key_proj, ((WINDOW, WINDOW), (0, 0)))
    padded_vals = jnp.pad(value_proj, ((WINDOW, WINDOW), (0, 0)))
    sink_col = att_sink.astype(jnp.float32).reshape(KV_HEADS, groups, 1, 1)

    def one_block(block_index):
        first_row = block_index * block_rows
        query_block = lax.dynamic_slice_in_dim(queries, first_row, block_rows, 0).reshape(block_rows, KV_HEADS, groups, HD)
        key_block = lax.dynamic_slice_in_dim(padded_keys, first_row, span_rows, 0).reshape(span_rows, KV_HEADS, HD)
        value_block = lax.dynamic_slice_in_dim(padded_vals, first_row, span_rows, 0).reshape(span_rows, KV_HEADS, HD)
        scores = jnp.einsum('qkgd,skd->kgqs', query_block.astype(jnp.float32), key_block.astype(jnp.float32)) * HD ** (-0.5)
        query_pos = first_row + jnp.arange(block_rows, dtype=jnp.int32)
        key_pos = first_row - WINDOW + jnp.arange(span_rows, dtype=jnp.int32)
        allowed = (jnp.abs(query_pos[:, None] - key_pos[None, :]) <= WINDOW) & (key_pos >= 0)[None, :] & (key_pos < seq_len)[None, :]
        scores = jnp.where(allowed, scores, -jnp.inf)
        row_top = jnp.maximum(lax.optimization_barrier(jnp.max(scores, axis=-1, keepdims=True)), sink_col)
        raised = jnp.exp(scores - row_top)
        denominator = lax.optimization_barrier(jnp.sum(raised, axis=-1, keepdims=True)) + jnp.exp(sink_col - row_top)
        weights_bf = (raised / denominator).astype(jnp.bfloat16)
        block_out = jnp.einsum('kgqs,skd->qkgd', weights_bf.astype(jnp.float32), value_block.astype(jnp.float32))
        return block_out.reshape(block_rows, ATT_HEADS * HD).astype(jnp.bfloat16)
    blocks = lax.map(one_block, jnp.arange(seq_len // block_rows, dtype=jnp.int32))
    return blocks.reshape(seq_len, ATT_HEADS * HD)

def advance(state_now, item_pair):
    factor_now, term_now = item_pair
    return (factor_now[:, None, None] * state_now + term_now, state_now)

def retain_all(query_rot, key_rot, value_f, decay_log, init_state):
    seq_len = query_rot.shape[0]
    block_count = seq_len // RET_BLOCK

    def heads_first(values, width):
        return jnp.transpose(values.reshape(block_count, RET_BLOCK, RET_HEADS, width), (2, 0, 1, 3))
    query_h = heads_first(query_rot, RK)
    key_h = heads_first(key_rot, RK)
    value_h = heads_first(value_f, RV)
    block_logs = decay_log.reshape(RET_HEADS, block_count, RET_BLOCK)
    cumul = jnp.cumsum(block_logs, axis=-1)
    block_log = cumul[..., -1]
    inner_w = jnp.einsum('hbnk,hbmk->hbnm', query_h, key_h, precision=HIGHEST) * jnp.exp(-jnp.abs(cumul[..., :, None] - cumul[..., None, :]))
    local_out = jnp.einsum('hbnm,hbmv->hbnv', inner_w, value_h, precision=HIGHEST)
    fwd_terms = jnp.einsum('hbmk,hbmv->bhkv', key_h * jnp.exp(block_log[..., None] - cumul)[..., None], value_h, precision=HIGHEST)
    bwd_terms = jnp.einsum('hbmk,hbmv->bhkv', key_h * jnp.exp(cumul)[..., None], value_h, precision=HIGHEST)
    factors = jnp.exp(block_log).T
    _, fwd_in = lax.scan(advance, init_state[0], (factors, fwd_terms))
    _, bwd_in = lax.scan(advance, init_state[1], (factors, bwd_terms), reverse=True)
    cross_out = jnp.exp(cumul)[..., None] * jnp.einsum('hbnk,bhkv->hbnv', query_h, fwd_in, precision=HIGHEST)
    cross_out = cross_out + jnp.exp(block_log[..., None] - cumul)[..., None] * jnp.einsum('hbnk,bhkv->hbnv', query_h, bwd_in, precision=HIGHEST)
    combined = local_out + cross_out
    centered = combined - lax.optimization_barrier(jnp.mean(combined, axis=-1, keepdims=True))
    normed = centered * lax.rsqrt(lax.optimization_barrier(jnp.mean(centered * centered, axis=-1, keepdims=True)) + NORM_EPS)
    return jnp.transpose(normed, (1, 2, 0, 3)).reshape(seq_len, RET_HEADS * RV)

def reference(tokens, norm_gain, att_query, att_key, att_value, ret_query, ret_key, ret_value, ret_gate, att_sink, decay_log, init_state, out_att, out_ret):
    seq_len = tokens.shape[0]
    tokens_f = tokens.astype(jnp.float32)
    inv_rms = lax.rsqrt(lax.optimization_barrier(jnp.mean(tokens_f * tokens_f, axis=-1, keepdims=True)) + NORM_EPS)
    normed = (tokens_f * norm_gain.astype(jnp.float32)[None, :]).astype(jnp.bfloat16)

    def project(weight):
        return (jnp.dot(normed, weight, preferred_element_type=jnp.float32) * inv_rms).astype(jnp.bfloat16)
    attended = attend_all(project(att_query), project(att_key), project(att_value), att_sink)
    positions = jnp.arange(seq_len, dtype=jnp.int32)
    query_rot = rotated(project(ret_query).astype(jnp.float32).reshape(seq_len, RET_HEADS, RK), positions)
    key_rot = rotated(project(ret_key).astype(jnp.float32).reshape(seq_len, RET_HEADS, RK), positions) * RK ** (-0.5)
    value_f = project(ret_value).astype(jnp.float32).reshape(seq_len, RET_HEADS, RV)
    retained = retain_all(query_rot, key_rot, value_f, decay_log, init_state)
    gate_f = project(ret_gate).astype(jnp.float32)
    ret_out = (jax.nn.silu(gate_f) * retained).astype(jnp.bfloat16)
    att_width = ATT_HEADS * HD // N_TP
    ret_width = RET_HEADS * RV // N_TP
    summed = jnp.zeros((seq_len, D), jnp.float32)
    for group_index in range(N_TP):
        att_lo = group_index * att_width
        ret_lo = group_index * ret_width
        partial_sum = jnp.dot(attended[:, att_lo:att_lo + att_width], out_att[att_lo:att_lo + att_width], preferred_element_type=jnp.float32)
        partial_sum = partial_sum + jnp.dot(ret_out[:, ret_lo:ret_lo + ret_width], out_ret[ret_lo:ret_lo + ret_width], preferred_element_type=jnp.float32)
        rounded = lax.optimization_barrier(partial_sum.astype(jnp.bfloat16))
        summed = summed + rounded.astype(jnp.float32)
    return summed.astype(jnp.bfloat16)
```

```python
import functools

import jax
import jax.numpy as jnp
import numpy as np
from jax import lax
from jax.experimental import pallas as pl
from jax.experimental.pallas import tpu as pltpu
from jax.sharding import PartitionSpec as P

HD = 64
RV = 128
BLK = 128
NORM_EPS = 1e-06
ROPE_BASE = 10000.0
MESH = pl.DeviceIdType.MESH
F32 = jnp.float32
BF16 = jnp.bfloat16
NT = (((1,), (1,)), ((), ()))
TN = (((0,), (0,)), ((), ()))

L1, R1, OPP, SIB = 0, 1, 2, 3


def kernel(n_sp, nx, tok_h, gain_h, wq_h, wk_h, wv_h, wrq_h, wrk_h, wrv_h, wrg_h, sink_ref, dec_h, init_h, inv_h, oa_h, or_h,
           out_h,
           X, W1, W2, gain, dec, init, inv, Q, KV, V, G, QR, QB, QX, RL, TT, SL, A, R, WO, OA, OUT,
           XS, ZG, ZS, DX, DZ, crow, bl8, pre8,
           lsem, xs_s, xs_r, as_s, as_r, rs_s, rs_r, w1_s, w1_r, w2_s, w2_r, sx_s, sx_r, dx_s, dx_r, sz_s, sz_r, dz_s, dz_r,
           h_s, h_r):
    rows, cw = tok_h.shape
    nb = rows // BLK
    arows = 2 * BLK
    na = rows // arows
    width = 8 * cw
    ocw = OUT.shape[1]
    nz = n_sp // nx
    quarter = BLK // nx
    s, t = lax.axis_index("sp"), lax.axis_index("tp")
    z, x = s // nx, s % nx
    y, c = t // 2, t % 2
    right = 2 * ((y + 1) % 4) + c
    left = 2 * ((y + 3) % 4) + c
    opp = 2 * ((y + 2) % 4) + c
    sib = 2 * y + (1 - c)
    up, down = (s + 1) % n_sp, (s + n_sp - 1) % n_sp

    loads = [
        (dec_h, dec), (tok_h, X.at[t]), (gain_h, gain), (inv_h, inv), (init_h, init),
        (wq_h, W1.at[:, 0:128]), (wrv_h, W1.at[:, 128:256]), (wrg_h, W1.at[:, 256:384]),
        (wk_h, W2.at[0:64]), (wv_h, W2.at[64:128]), (wrq_h, W2.at[128:192]), (wrk_h, W2.at[192:256]),
    ]
    mine = pl.ds(pl.multiple_of(x * quarter, quarter), quarter)
    my_cols = pl.ds(pl.multiple_of(t * ocw, 128), ocw)
    loads += [(oa_h.at[mine, my_cols], WO.at[0, t, mine, :]), (or_h.at[mine, my_cols], WO.at[1, t, mine, :])]
    copies = [pltpu.make_async_copy(a, b, lsem.at[i]) for i, (a, b) in enumerate(loads)]
    for cp in copies:
        cp.start()

    barrier = pltpu.get_barrier_semaphore()
    partners = [(s, (t + d) % 8) for d in range(1, 8)]
    partners += [(z * nx + (x + d) % nx, t) for d in range(1, nx)]
    partners += [(((z + d) % nz) * nx + x, t) for d in range(1, nz)]
    partners += [(up, t), (down, t)]
    for p in partners:
        pl.semaphore_signal(barrier, inc=1, device_id=p, device_id_type=MESH)

    copies[0].wait()
    for b in range(nb):
        crow[b : b + 1, :] = dec[:, b * BLK : (b + 1) * BLK]
    cum = crow[...]
    lane = lax.broadcasted_iota(jnp.int32, (nb, BLK), 1)
    for sh in (1, 2, 4, 8, 16, 32, 64):
        cum = cum + jnp.where(lane >= sh, pltpu.roll(cum, sh, 1), 0.0)
    crow[...] = cum
    bl8[...] = jnp.broadcast_to(cum[:, BLK - 1 : BLK], (nb, BLK))
    run = jnp.zeros((1, BLK), F32)
    for b in range(nb):
        pre8[b : b + 1, :] = run
        run = run + bl8[b : b + 1, :]
    tot = run
    DX[x] = jnp.broadcast_to(tot, (8, BLK))
    for i in range(1, 5):
        copies[i].wait()

    pl.semaphore_wait(barrier, len(partners))

    def put(src, dst, send, recv, dev):
        return pltpu.make_async_remote_copy(src_ref=src, dst_ref=dst, send_sem=send, recv_sem=recv, device_id=dev, device_id_type=MESH)

    def gather(buf, n_rows, ss, rs):
        def part(b, k):
            return buf.at[b, pl.ds(pl.multiple_of(k * n_rows, n_rows), n_rows), :]

        def hop(b, k, send, recv, tp):
            ref = part(b, k)
            return put(ref, ref, ss.at[send, k], rs.at[recv, k], (s, tp))

        def own(k):
            hop(t, k, 0, L1, right).start()
            hop(t, k, 1, R1, left).start()
            hop(t, k, 2, SIB, sib).start()

        def pass_on(k):
            hop(left, k, 3, L1, right).wait_recv()
            even = k % 2 == 0

            @pl.when(even)
            def _():
                hop(left, k, 6, OPP, right).start()

            hop(left, k, 3, SIB + 1, sib).start()
            hop(right, k, 4, R1, left).wait_recv()

            @pl.when(k % 2 == 1)
            def _():
                hop(right, k, 6, OPP, left).start()

            hop(right, k, 4, SIB + 2, sib).start()

        def pass_last(k):
            hop(opp, k, 5, OPP, right).wait_recv()
            hop(opp, k, 5, SIB + 3, sib).start()

        def arrived(k):
            hop(sib, k, 2, SIB, sib).wait_recv()
            hop(2 * ((y + 3) % 4) + 1 - c, k, 3, SIB + 1, sib).wait_recv()
            hop(2 * ((y + 1) % 4) + 1 - c, k, 4, SIB + 2, sib).wait_recv()
            hop(2 * ((y + 2) % 4) + 1 - c, k, 5, SIB + 3, sib).wait_recv()

        def sent(k):
            for i in range(7):
                hop(t, k, i, L1, right).wait_send()

        return own, pass_on, pass_last, arrived, sent

    own, pass_on, pass_last, arrived, sent = gather(X, BLK, xs_s, xs_r)
    a_own, a_pass, a_last, a_arrived, a_sent = gather(A, arows, as_s, as_r)
    r_own, r_pass, r_last, r_arrived, r_sent = gather(R, arows, rs_s, rs_r)

    own(0)
    own(1)
    for d in range(1, nx):
        put(DX.at[x], DX.at[x], dx_s.at[d], dx_r.at[d], (z * nx + (x + d) % nx, t)).start()

    lane_b = lax.broadcasted_iota(jnp.int32, (BLK, BLK), 1)
    row_b = lax.broadcasted_iota(jnp.int32, (BLK, BLK), 0)
    low = lane_b < 64

    def blk(j):
        return pl.ds(pl.multiple_of(j * BLK, BLK), BLK)

    def column(j):
        row = jnp.broadcast_to(crow[pl.ds(j, 1), :], (BLK, BLK))
        return jnp.sum(jnp.where(lane_b == row_b, row, 0.0), axis=1, keepdims=True)

    def project(j):
        pos = (s * rows + j * BLK + row_b).astype(F32)
        angle = pos * inv[...]
        scale = jnp.where(low, 1.0, 64**-0.5).astype(F32)
        cosine = jnp.cos(angle) * scale
        sine = jnp.sin(angle) * jnp.where(lane_b % 64 < 32, -scale, scale)
        cc = column(j)
        bl = bl8[pl.ds(j, 1), :]
        pre = pre8[pl.ds(j, 1), :]
        arrived(j)
        squares = jnp.zeros((BLK, cw), F32)
        parts = []
        for b in range(8):
            xf = X[b, blk(j), :].astype(F32)
            squares = squares + xf * xf
            parts.append((xf * gain[:, b * cw : (b + 1) * cw]).astype(BF16))
        normed = jnp.concatenate(parts, axis=1)
        inv_rms = lax.rsqrt(jnp.sum(squares, axis=1, keepdims=True) / width + NORM_EPS)
        p1 = (jnp.dot(normed, W1[...], preferred_element_type=F32) * inv_rms).astype(BF16)
        p2 = (lax.dot_general(normed, W2[...], NT, preferred_element_type=F32) * inv_rms).astype(BF16)
        Q[blk(j), :] = p1[:, 0:128]
        v = p1[:, 128:256]
        V[blk(j), :] = v
        G[blk(j), :] = p1[:, 256:384]
        KV[blk(j + 1), :] = p2[:, 0:128]
        rqk = p2[:, 128:256].astype(F32)
        swapped = jnp.where(lane_b % 64 < 32, pltpu.roll(rqk, 96, 1), pltpu.roll(rqk, 32, 1))
        rot = rqk * cosine + swapped * sine
        QR[blk(j), :] = rot.astype(BF16)
        other = pltpu.roll(rot, 64, 1)
        qq = jnp.where(low, rot, other)
        kk = jnp.where(low, other, rot)
        to_end = jnp.exp(bl - cc)
        to_here = jnp.exp(jnp.broadcast_to(cc, (BLK, BLK)))
        QB[blk(j), :] = (qq * jnp.where(low, to_here, to_end)).astype(BF16)
        full = cc + pre
        QX[blk(j), :] = (qq * jnp.exp(jnp.where(low, full, tot - full))).astype(BF16)
        kw = (kk * jnp.where(low, to_end, to_here)).astype(BF16)
        TT[j] = lax.dot_general(kw, v, TN, preferred_element_type=F32)

    for i in range(5, 12):
        copies[i].wait()

    def step(k, carry):
        @pl.when(k < nb - 2)
        def _():
            own(k + 2)

        @pl.when(k < nb)
        def _():
            pass_on(k)

        @pl.when((k >= 1) & (k < nb + 1))
        def _():
            pass_last(k - 1)

        @pl.when(k >= 2)
        def _():
            project(k - 2)

        return carry

    lax.fori_loop(0, nb + 2, step, 0)

    halo_up = put(KV.at[pl.ds(rows, BLK), :], KV.at[pl.ds(0, BLK), :], h_s.at[0], h_r.at[0], (up, t))
    halo_down = put(KV.at[pl.ds(BLK, BLK), :], KV.at[pl.ds(rows + BLK, BLK), :], h_s.at[1], h_r.at[1], (down, t))
    halo_up.start()
    halo_down.start()

    f = jnp.zeros((64, RV), F32)
    g = jnp.zeros((64, RV), F32)
    for b in range(nb):
        SL[b, 0:64, :] = f.astype(BF16)
        f = jnp.exp(bl8[b : b + 1, :]) * f + TT[b, 0:64, :]
        e = nb - 1 - b
        SL[e, 64:128, :] = g.astype(BF16)
        g = jnp.exp(bl8[e : e + 1, :]) * g + TT[e, 64:128, :]
    XS[x, 0:64, :] = f.astype(BF16)
    XS[x, 64:128, :] = g.astype(BF16)
    for d in range(1, nx):
        put(XS.at[x], XS.at[x], sx_s.at[d], sx_r.at[d], (z * nx + (x + d) % nx, t)).start()
    for d in range(1, nx):
        put(DX.at[(x + nx - d) % nx], DX.at[(x + nx - d) % nx], dx_s.at[d], dx_r.at[d], (s, sib)).wait_recv()
    total = DX[0]
    for i in range(1, nx):
        total = total + DX[i]
    DZ[z] = total
    for d in range(1, nz):
        put(DZ.at[z], DZ.at[z], dz_s.at[d], dz_r.at[d], (((z + d) % nz) * nx + x, t)).start()

    copies[12].wait()
    copies[13].wait()
    for d in range(1, 8):
        to = (t + d) % 8
        cols = pl.ds(pl.multiple_of(to * ocw, 128), ocw)
        put(oa_h.at[mine, cols], WO.at[0, t, mine, :], w1_s.at[0, d], w1_r.at[0, d], (s, to)).start()
        put(or_h.at[mine, cols], WO.at[1, t, mine, :], w1_s.at[1, d], w1_r.at[1, d], (s, to)).start()

    row_q = lax.broadcasted_iota(jnp.int32, (2 * BLK, BLK), 0) % BLK
    lane_q = lax.broadcasted_iota(jnp.int32, (2 * BLK, BLK), 1)
    sink = jnp.where(lax.broadcasted_iota(jnp.int32, (2 * BLK, 1), 0) < BLK, sink_ref[0], sink_ref[1])

    def attend(i, carry):
        j = (i + 2) % nb

        @pl.when(i == nb - 2)
        def _():
            halo_up.wait_recv()

        @pl.when(i == nb - 3)
        def _():
            halo_down.wait_recv()

        q = Q[blk(j), :]
        q2 = jnp.concatenate([q[:, 0:64], q[:, 64:128]], axis=0)
        kv = KV[pl.ds(pl.multiple_of(j * BLK, BLK), 3 * BLK), :]
        sc = lax.dot_general(q2, kv[:, 0:64], NT, preferred_element_type=F32) * HD**-0.5
        first = jnp.where(s * nb + j == 0, BLK, 0)
        last = jnp.where(s * nb + j == n_sp * nb - 1, BLK, 0)
        s0 = jnp.where(lane_q - first >= row_q, sc[:, 0:128], -jnp.inf)
        s1 = sc[:, 128:256]
        s2 = jnp.where(lane_q + last <= row_q, sc[:, 256:384], -jnp.inf)
        top = jnp.maximum(jnp.max(jnp.maximum(jnp.maximum(s0, s1), s2), axis=1, keepdims=True), sink)
        e0, e1, e2 = jnp.exp(s0 - top), jnp.exp(s1 - top), jnp.exp(s2 - top)
        den = jnp.sum(e0 + e1 + e2, axis=1, keepdims=True) + jnp.exp(sink - top)
        ee = jnp.concatenate([e0.astype(BF16), e1.astype(BF16), e2.astype(BF16)], axis=1)
        o = jnp.dot(ee, kv[:, 64:128], preferred_element_type=F32) / den
        A[t, blk(j), :] = jnp.concatenate([o[0:BLK], o[BLK : 2 * BLK]], axis=1).astype(BF16)

        @pl.when(i % 2 == 1)
        def _():
            a_own(j // 2)

        return carry

    lax.fori_loop(0, nb, attend, 0)

    for d in range(1, nx):
        o = (x + nx - d) % nx
        put(XS.at[o], XS.at[o], sx_s.at[d], sx_r.at[d], (s, sib)).wait_recv()
    ex = [jnp.exp(DX[i][0:1, :]) for i in range(nx)]
    fx = jnp.zeros((64, RV), F32)
    gx = jnp.zeros((64, RV), F32)
    fall = jnp.zeros((64, RV), F32)
    gall = jnp.zeros((64, RV), F32)
    dfx = jnp.zeros((1, RV), F32)
    dgx = jnp.zeros((1, RV), F32)
    for i in range(nx):
        term = XS[i, 0:64, :].astype(F32)
        fx = jnp.where(i < x, ex[i] * fx + term, fx)
        dfx = jnp.where(i < x, dfx + DX[i][0:1, :], dfx)
        fall = ex[i] * fall + term
        o = nx - 1 - i
        term = XS[o, 64:128, :].astype(F32)
        gx = jnp.where(o > x, ex[o] * gx + term, gx)
        dgx = jnp.where(o > x, dgx + DX[o][0:1, :], dgx)
        gall = ex[o] * gall + term
    ZG[0] = fall.astype(BF16)
    ZG[1] = gall.astype(BF16)
    ZS[z] = jnp.zeros((64, RV), BF16)
    for d in range(1, nz):
        put(ZG.at[(z + d) // nz], ZS.at[z], sz_s.at[d], sz_r.at[d], (((z + d) % nz) * nx + x, t)).start()

    a_order = [(i + 1) % na for i in range(na)]
    for k in a_order:
        a_pass(k)

    def inside(j, carry):
        cc = column(j)
        cr = crow[pl.ds(j, 1), :]
        qk = QR[blk(j), :]
        sc = lax.dot_general(qk[:, 0:64], qk[:, 64:128], NT, preferred_element_type=F32)
        w = (sc * jnp.exp(-jnp.abs(cc - cr))).astype(BF16)
        RL[blk(j), :] = jnp.dot(w, V[blk(j), :], preferred_element_type=F32) + jnp.dot(
            QB[blk(j), :], SL[j], preferred_element_type=F32
        )
        return carry

    lax.fori_loop(0, nb, inside, 0)

    for d in range(1, 8):
        fr = (t + 8 - d) % 8
        for i in range(2):
            ref = WO.at[i, fr, mine, :]
            put(ref, ref, w1_s.at[i, d], w1_r.at[i, d], (s, sib)).wait_recv()
    for d in range(1, nx):
        ref = WO.at[:, :, mine, :]
        put(ref, ref, w2_s.at[d], w2_r.at[d], (z * nx + (x + d) % nx, t)).start()

    for k in a_order:
        a_last(k)

    for d in range(1, nz):
        o = (z + nz - d) % nz
        put(DZ.at[o], DZ.at[o], dz_s.at[d], dz_r.at[d], (s, sib)).wait_recv()
        put(ZS.at[o], ZS.at[o], sz_s.at[d], sz_r.at[d], (s, sib)).wait_recv()
    fz = init[0:64, :]
    gz = init[64:128, :]
    for i in range(nz):
        term = ZS[i].astype(F32)
        fz = jnp.where(i < z, jnp.exp(DZ[i][0:1, :]) * fz + term, fz)
        o = nz - 1 - i
        term = ZS[o].astype(F32)
        gz = jnp.where(o > z, jnp.exp(DZ[o][0:1, :]) * gz + term, gz)
    ST = jnp.concatenate([fx + jnp.exp(dfx) * fz, gx + jnp.exp(dgx) * gz], axis=0).astype(BF16)

    def finish(j, carry):
        ret = RL[blk(j), :] + jnp.dot(QX[blk(j), :], carry, preferred_element_type=F32)
        cen = ret - jnp.mean(ret, axis=1, keepdims=True)
        nrm = cen * lax.rsqrt(jnp.mean(cen * cen, axis=1, keepdims=True) + NORM_EPS)
        gate = G[blk(j), :].astype(F32)
        R[t, blk(j), :] = (gate / (1.0 + jnp.exp(-gate)) * nrm).astype(BF16)

        @pl.when(j % 2 == 1)
        def _():
            r_own(j // 2)

        return carry

    lax.fori_loop(0, nb, finish, ST)

    for k in range(na):
        r_pass(k)

    for k in range(na):
        a_arrived(k)
    for d in range(1, nx):
        ref = WO.at[:, :, pl.ds(pl.multiple_of(((x + nx - d) % nx) * quarter, quarter), quarter), :]
        put(ref, ref, w2_s.at[d], w2_r.at[d], (s, sib)).wait_recv()

    def big(k):
        return pl.ds(pl.multiple_of(k * arows, arows), arows)

    def out_att(k, carry):
        lhs = jnp.concatenate([A[b, big(k), :] for b in range(8)], axis=1)
        OA[big(k), :] = jnp.dot(lhs, WO[0].reshape(8 * BLK, ocw), preferred_element_type=F32)
        return carry

    lax.fori_loop(0, na, out_att, 0)

    for k in range(na):
        r_last(k)

    def out_ret(k, carry):
        r_arrived(k)
        lhs = jnp.concatenate([R[b, big(k), :] for b in range(8)], axis=1)
        acc = OA[big(k), :] + jnp.dot(lhs, WO[1].reshape(8 * BLK, ocw), preferred_element_type=F32)
        OUT[big(k), :] = acc.astype(BF16)
        pltpu.make_async_copy(OUT.at[big(k), :], out_h.at[big(k), :], lsem.at[14 + k]).start()
        return carry

    lax.fori_loop(0, na, out_ret, 0)

    def drain(k, carry):
        sent(k)
        return carry

    lax.fori_loop(0, nb, drain, 0)
    for k in range(na):
        a_sent(k)
        r_sent(k)
        pltpu.make_async_copy(OUT.at[big(k), :], out_h.at[big(k), :], lsem.at[14 + k]).wait()
    for d in range(1, 8):
        for i in range(2):
            put(oa_h.at[mine, my_cols], WO.at[i, t, mine, :], w1_s.at[i, d], w1_r.at[i, d], (s, sib)).wait_send()
    for d in range(1, nx):
        ref = WO.at[:, :, mine, :]
        put(ref, ref, w2_s.at[d], w2_r.at[d], (s, sib)).wait_send()
        put(XS.at[x], XS.at[x], sx_s.at[d], sx_r.at[d], (s, sib)).wait_send()
        put(DX.at[x], DX.at[x], dx_s.at[d], dx_r.at[d], (s, sib)).wait_send()
    for d in range(1, nz):
        put(ZG.at[0], ZS.at[z], sz_s.at[d], sz_r.at[d], (s, sib)).wait_send()
        put(DZ.at[z], DZ.at[z], dz_s.at[d], dz_r.at[d], (s, sib)).wait_send()
    halo_up.wait_send()
    halo_down.wait_send()


def body(tokens, norm_gain, att_query, att_key, att_value, ret_query, ret_key, ret_value, ret_gate, att_sink, decay_log, init_state,
         out_att, out_ret, *, n_sp):
    rows, cw = tokens.shape
    width = 8 * cw
    ocw = out_att.shape[1] // 8
    nb, na = rows // BLK, rows // (2 * BLK)
    nx = 4 if n_sp >= 16 else 2
    nz = n_sp // nx
    inverse = (np.float64(ROPE_BASE) ** (-2.0 * (np.arange(128) % 32) / 64)).astype(np.float32)[None, :]
    dma = pltpu.SemaphoreType.DMA
    hbm = pl.BlockSpec(memory_space=pltpu.HBM)
    specs = [hbm] * 15
    specs[9] = pl.BlockSpec(memory_space=pltpu.SMEM)
    vm = pltpu.VMEM
    scratch = [
        vm((8, rows, cw), BF16), vm((width, 384), BF16), vm((256, width), BF16), vm((1, width), F32), vm((1, rows), F32),
        vm((128, 128), F32), vm((1, 128), F32),
        vm((rows, 128), BF16), vm((rows + 2 * BLK, 128), BF16), vm((rows, 128), BF16), vm((rows, 128), BF16),
        vm((rows, 128), BF16), vm((rows, 128), BF16), vm((rows, 128), BF16), vm((rows, 128), F32),
        vm((nb, 128, 128), F32), vm((nb, 128, 128), BF16),
        vm((8, rows, 128), BF16), vm((8, rows, 128), BF16), vm((2, 8, 128, ocw), BF16), vm((rows, ocw), F32), vm((rows, ocw), BF16),
        vm((nx, 128, 128), BF16), vm((2, 64, 128), BF16), vm((nz, 64, 128), BF16), vm((nx, 8, 128), F32), vm((nz, 8, 128), F32),
        vm((nb, 128), F32), vm((nb, 128), F32), vm((nb, 128), F32),
        dma((14 + na,)), dma((7, nb)), dma((7, nb)), dma((7, na)), dma((7, na)), dma((7, na)), dma((7, na)),
        dma((2, 8)), dma((2, 8)), dma((nx,)), dma((nx,)), dma((nx,)), dma((nx,)), dma((nx,)), dma((nx,)),
        dma((max(nz, 2),)), dma((max(nz, 2),)), dma((max(nz, 2),)), dma((max(nz, 2),)), dma((2,)), dma((2,)),
    ]
    call = pl.pallas_call(
        functools.partial(kernel, n_sp, nx),
        out_shape=jax.ShapeDtypeStruct((rows, ocw), BF16),
        in_specs=specs,
        out_specs=hbm,
        scratch_shapes=scratch,
        compiler_params=pltpu.CompilerParams(collective_id=0, has_side_effects=True, vmem_limit_bytes=48 * 1024 * 1024),
        name="layer",
    )
    return call(
        tokens, norm_gain.reshape(1, width), att_query, att_key.T, att_value.T, ret_query.T, ret_key.T, ret_value, ret_gate,
        att_sink, decay_log, init_state.reshape(128, 128), inverse, out_att, out_ret,
    )


def solution(mesh):
    in_specs = (
        P("sp", "tp"), P(), P(None, "tp"), P(None, "tp"), P(None, "tp"), P(None, "tp"), P(None, "tp"), P(None, "tp"), P(None, "tp"),
        P("tp"), P("tp", "sp"), P(None, "tp", None, None), P("tp", None), P("tp", None),
    )
    return jax.shard_map(
        functools.partial(body, n_sp=mesh.shape["sp"]), mesh=mesh, in_specs=in_specs, out_specs=P("sp", "tp"), check_vma=False
    )
```

```python
import functools

import jax
import jax.numpy as jnp
import numpy as np
from jax import lax
from jax.experimental import pallas as pl
from jax.experimental.pallas import tpu as pltpu
from jax.sharding import PartitionSpec as P

HD = 64
RV = 128
BLK = 128
NORM_EPS = 1e-06
ROPE_BASE = 10000.0
MESH = pl.DeviceIdType.MESH
F32 = jnp.float32
BF16 = jnp.bfloat16
NT = (((1,), (1,)), ((), ()))
TN = (((0,), (0,)), ((), ()))

L1, R1, OPP, SIB = 0, 1, 2, 3


def kernel(n_sp, nx, tok_h, gain_h, wq_h, wk_h, wv_h, wrq_h, wrk_h, wrv_h, wrg_h, sink_ref, dec_h, init_h, inv_h, oa_h, or_h,
           out_h,
           X, W1, W2, gain, dec, init, inv, Q, KV, V, G, QR, QB, QX, RL, TT, SL, A, R, WO, OA, OUT,
           XS, ZG, ZS, DX, DZ, crow, bl8, pre8,
           lsem, xs_s, xs_r, as_s, as_r, rs_s, rs_r, w1_s, w1_r, w2_s, w2_r, sx_s, sx_r, dx_s, dx_r, sz_s, sz_r, dz_s, dz_r,
           h_s, h_r):
    rows, cw = tok_h.shape
    nb = rows // BLK
    arows = 2 * BLK
    na = rows // arows
    width = 8 * cw
    ocw = OUT.shape[1]
    nz = n_sp // nx
    quarter = BLK // nx
    s, t = lax.axis_index("sp"), lax.axis_index("tp")
    z, x = s // nx, s % nx
    y, c = t // 2, t % 2
    right = 2 * ((y + 1) % 4) + c
    left = 2 * ((y + 3) % 4) + c
    opp = 2 * ((y + 2) % 4) + c
    sib = 2 * y + (1 - c)
    up, down = (s + 1) % n_sp, (s + n_sp - 1) % n_sp

    loads = [
        (dec_h, dec), (tok_h, X.at[t]), (gain_h, gain), (inv_h, inv), (init_h, init),
        (wq_h, W1.at[:, 0:128]), (wrv_h, W1.at[:, 128:256]), (wrg_h, W1.at[:, 256:384]),
        (wk_h, W2.at[0:64]), (wv_h, W2.at[64:128]), (wrq_h, W2.at[128:192]), (wrk_h, W2.at[192:256]),
    ]
    mine = pl.ds(pl.multiple_of(x * quarter, quarter), quarter)
    my_cols = pl.ds(pl.multiple_of(t * ocw, 128), ocw)
    loads += [(oa_h.at[mine, my_cols], WO.at[0, t, mine, :]), (or_h.at[mine, my_cols], WO.at[1, t, mine, :])]
    copies = [pltpu.make_async_copy(a, b, lsem.at[i]) for i, (a, b) in enumerate(loads)]
    for cp in copies:
        cp.start()

    barrier = pltpu.get_barrier_semaphore()
    partners = [(s, (t + d) % 8) for d in range(1, 8)]
    partners += [(z * nx + (x + d) % nx, t) for d in range(1, nx)]
    partners += [(((z + d) % nz) * nx + x, t) for d in range(1, nz)]
    partners += [(up, t), (down, t)]
    for p in partners:
        pl.semaphore_signal(barrier, inc=1, device_id=p, device_id_type=MESH)

    copies[0].wait()
    for b in range(nb):
        crow[b : b + 1, :] = dec[:, b * BLK : (b + 1) * BLK]
    cum = crow[...]
    lane = lax.broadcasted_iota(jnp.int32, (nb, BLK), 1)
    for sh in (1, 2, 4, 8, 16, 32, 64):
        cum = cum + jnp.where(lane >= sh, pltpu.roll(cum, sh, 1), 0.0)
    crow[...] = cum
    bl8[...] = jnp.broadcast_to(cum[:, BLK - 1 : BLK], (nb, BLK))
    run = jnp.zeros((1, BLK), F32)
    for b in range(nb):
        pre8[b : b + 1, :] = run
        run = run + bl8[b : b + 1, :]
    tot = run
    DX[x] = jnp.broadcast_to(tot, (8, BLK))
    for i in range(1, 5):
        copies[i].wait()

    pl.semaphore_wait(barrier, len(partners))

    def put(src, dst, send, recv, dev):
        return pltpu.make_async_remote_copy(src_ref=src, dst_ref=dst, send_sem=send, recv_sem=recv, device_id=dev, device_id_type=MESH)

    def gather(buf, n_rows, ss, rs):
        def part(b, k):
            return buf.at[b, pl.ds(pl.multiple_of(k * n_rows, n_rows), n_rows), :]

        def hop(b, k, send, recv, tp):
            ref = part(b, k)
            return put(ref, ref, ss.at[send, k], rs.at[recv, k], (s, tp))

        def own(k):
            hop(t, k, 0, L1, right).start()
            hop(t, k, 1, R1, left).start()
            hop(t, k, 2, SIB, sib).start()

        def pass_on(k):
            hop(left, k, 3, L1, right).wait_recv()
            even = k % 2 == 0

            @pl.when(even)
            def _():
                hop(left, k, 6, OPP, right).start()

            hop(left, k, 3, SIB + 1, sib).start()
            hop(right, k, 4, R1, left).wait_recv()

            @pl.when(k % 2 == 1)
            def _():
                hop(right, k, 6, OPP, left).start()

            hop(right, k, 4, SIB + 2, sib).start()

        def pass_last(k):
            hop(opp, k, 5, OPP, right).wait_recv()
            hop(opp, k, 5, SIB + 3, sib).start()

        def arrived(k):
            hop(sib, k, 2, SIB, sib).wait_recv()
            hop(2 * ((y + 3) % 4) + 1 - c, k, 3, SIB + 1, sib).wait_recv()
            hop(2 * ((y + 1) % 4) + 1 - c, k, 4, SIB + 2, sib).wait_recv()
            hop(2 * ((y + 2) % 4) + 1 - c, k, 5, SIB + 3, sib).wait_recv()

        def sent(k):
            for i in range(7):
                hop(t, k, i, L1, right).wait_send()

        return own, pass_on, pass_last, arrived, sent

    own, pass_on, pass_last, arrived, sent = gather(X, BLK, xs_s, xs_r)
    a_own, a_pass, a_last, a_arrived, a_sent = gather(A, arows, as_s, as_r)
    r_own, r_pass, r_last, r_arrived, r_sent = gather(R, arows, rs_s, rs_r)

    own(0)
    own(1)
    for d in range(1, nx):
        put(DX.at[x], DX.at[x], dx_s.at[d], dx_r.at[d], (z * nx + (x + d) % nx, t)).start()

    lane_b = lax.broadcasted_iota(jnp.int32, (BLK, BLK), 1)
    row_b = lax.broadcasted_iota(jnp.int32, (BLK, BLK), 0)
    low = lane_b < 64

    def blk(j):
        return pl.ds(pl.multiple_of(j * BLK, BLK), BLK)

    def column(j):
        row = jnp.broadcast_to(crow[pl.ds(j, 1), :], (BLK, BLK))
        return jnp.sum(jnp.where(lane_b == row_b, row, 0.0), axis=1, keepdims=True)

    def project(j):
        pos = (s * rows + j * BLK + row_b).astype(F32)
        angle = pos * inv[...]
        scale = jnp.where(low, 1.0, 64**-0.5).astype(F32)
        cosine = jnp.cos(angle) * scale
        sine = jnp.sin(angle) * jnp.where(lane_b % 64 < 32, -scale, scale)
        cc = column(j)
        bl = bl8[pl.ds(j, 1), :]
        pre = pre8[pl.ds(j, 1), :]
        arrived(j)
        squares = jnp.zeros((BLK, cw), F32)
        parts = []
        for b in range(8):
            xf = X[b, blk(j), :].astype(F32)
            squares = squares + xf * xf
            parts.append((xf * gain[:, b * cw : (b + 1) * cw]).astype(BF16))
        normed = jnp.concatenate(parts, axis=1)
        inv_rms = lax.rsqrt(jnp.sum(squares, axis=1, keepdims=True) / width + NORM_EPS)
        p1 = (jnp.dot(normed, W1[...], preferred_element_type=F32) * inv_rms).astype(BF16)
        p2 = (lax.dot_general(normed, W2[...], NT, preferred_element_type=F32) * inv_rms).astype(BF16)
        Q[blk(j), :] = p1[:, 0:128]
        v = p1[:, 128:256]
        V[blk(j), :] = v
        G[blk(j), :] = p1[:, 256:384]
        KV[blk(j + 1), :] = p2[:, 0:128]
        rqk = p2[:, 128:256].astype(F32)
        swapped = jnp.where(lane_b % 64 < 32, pltpu.roll(rqk, 96, 1), pltpu.roll(rqk, 32, 1))
        rot = rqk * cosine + swapped * sine
        QR[blk(j), :] = rot.astype(BF16)
        other = pltpu.roll(rot, 64, 1)
        qq = jnp.where(low, rot, other)
        kk = jnp.where(low, other, rot)
        to_end = jnp.exp(bl - cc)
        to_here = jnp.exp(jnp.broadcast_to(cc, (BLK, BLK)))
        QB[blk(j), :] = (qq * jnp.where(low, to_here, to_end)).astype(BF16)
        full = cc + pre
        QX[blk(j), :] = (qq * jnp.exp(jnp.where(low, full, tot - full))).astype(BF16)
        kw = (kk * jnp.where(low, to_end, to_here)).astype(BF16)
        TT[j] = lax.dot_general(kw, v, TN, preferred_element_type=F32)

    for i in range(5, 12):
        copies[i].wait()

    def step(k, carry):
        @pl.when(k < nb - 2)
        def _():
            own(k + 2)

        @pl.when(k < nb)
        def _():
            pass_on(k)

        @pl.when((k >= 1) & (k < nb + 1))
        def _():
            pass_last(k - 1)

        @pl.when(k >= 2)
        def _():
            project(k - 2)

        return carry

    lax.fori_loop(0, nb + 2, step, 0)

    halo_up = put(KV.at[pl.ds(rows, BLK), :], KV.at[pl.ds(0, BLK), :], h_s.at[0], h_r.at[0], (up, t))
    halo_down = put(KV.at[pl.ds(BLK, BLK), :], KV.at[pl.ds(rows + BLK, BLK), :], h_s.at[1], h_r.at[1], (down, t))
    halo_up.start()
    halo_down.start()

    f = jnp.zeros((64, RV), F32)
    g = jnp.zeros((64, RV), F32)
    for b in range(nb):
        SL[b, 0:64, :] = f.astype(BF16)
        f = jnp.exp(bl8[b : b + 1, :]) * f + TT[b, 0:64, :]
        e = nb - 1 - b
        SL[e, 64:128, :] = g.astype(BF16)
        g = jnp.exp(bl8[e : e + 1, :]) * g + TT[e, 64:128, :]
    XS[x, 0:64, :] = f.astype(BF16)
    XS[x, 64:128, :] = g.astype(BF16)
    for d in range(1, nx):
        put(XS.at[x], XS.at[x], sx_s.at[d], sx_r.at[d], (z * nx + (x + d) % nx, t)).start()
    for d in range(1, nx):
        put(DX.at[(x + nx - d) % nx], DX.at[(x + nx - d) % nx], dx_s.at[d], dx_r.at[d], (s, sib)).wait_recv()
    total = DX[0]
    for i in range(1, nx):
        total = total + DX[i]
    DZ[z] = total
    for d in range(1, nz):
        put(DZ.at[z], DZ.at[z], dz_s.at[d], dz_r.at[d], (((z + d) % nz) * nx + x, t)).start()

    copies[12].wait()
    copies[13].wait()
    for d in range(1, 8):
        to = (t + d) % 8
        cols = pl.ds(pl.multiple_of(to * ocw, 128), ocw)
        put(oa_h.at[mine, cols], WO.at[0, t, mine, :], w1_s.at[0, d], w1_r.at[0, d], (s, to)).start()
        put(or_h.at[mine, cols], WO.at[1, t, mine, :], w1_s.at[1, d], w1_r.at[1, d], (s, to)).start()

    row_q = lax.broadcasted_iota(jnp.int32, (2 * BLK, BLK), 0) % BLK
    lane_q = lax.broadcasted_iota(jnp.int32, (2 * BLK, BLK), 1)
    sink = jnp.where(lax.broadcasted_iota(jnp.int32, (2 * BLK, 1), 0) < BLK, sink_ref[0], sink_ref[1])

    def attend(i, carry):
        j = (i + 2) % nb

        @pl.when(i == nb - 2)
        def _():
            halo_up.wait_recv()

        @pl.when(i == nb - 3)
        def _():
            halo_down.wait_recv()

        q = Q[blk(j), :]
        q2 = jnp.concatenate([q[:, 0:64], q[:, 64:128]], axis=0)
        kv = KV[pl.ds(pl.multiple_of(j * BLK, BLK), 3 * BLK), :]
        sc = lax.dot_general(q2, kv[:, 0:64], NT, preferred_element_type=F32) * HD**-0.5
        first = jnp.where(s * nb + j == 0, BLK, 0)
        last = jnp.where(s * nb + j == n_sp * nb - 1, BLK, 0)
        s0 = jnp.where(lane_q - first >= row_q, sc[:, 0:128], -jnp.inf)
        s1 = sc[:, 128:256]
        s2 = jnp.where(lane_q + last <= row_q, sc[:, 256:384], -jnp.inf)
        top = jnp.maximum(jnp.max(jnp.maximum(jnp.maximum(s0, s1), s2), axis=1, keepdims=True), sink)
        e0, e1, e2 = jnp.exp(s0 - top), jnp.exp(s1 - top), jnp.exp(s2 - top)
        den = jnp.sum(e0 + e1 + e2, axis=1, keepdims=True) + jnp.exp(sink - top)
        ee = jnp.concatenate([e0.astype(BF16), e1.astype(BF16), e2.astype(BF16)], axis=1)
        o = jnp.dot(ee, kv[:, 64:128], preferred_element_type=F32) / den
        A[t, blk(j), :] = jnp.concatenate([o[0:BLK], o[BLK : 2 * BLK]], axis=1).astype(BF16)

        @pl.when(i % 2 == 1)
        def _():
            a_own(j // 2)

        return carry

    lax.fori_loop(0, nb, attend, 0)

    for d in range(1, nx):
        o = (x + nx - d) % nx
        put(XS.at[o], XS.at[o], sx_s.at[d], sx_r.at[d], (s, sib)).wait_recv()
    ex = [jnp.exp(DX[i][0:1, :]) for i in range(nx)]
    fx = jnp.zeros((64, RV), F32)
    gx = jnp.zeros((64, RV), F32)
    fall = jnp.zeros((64, RV), F32)
    gall = jnp.zeros((64, RV), F32)
    dfx = jnp.zeros((1, RV), F32)
    dgx = jnp.zeros((1, RV), F32)
    for i in range(nx):
        term = XS[i, 0:64, :].astype(F32)
        fx = jnp.where(i < x, ex[i] * fx + term, fx)
        dfx = jnp.where(i < x, dfx + DX[i][0:1, :], dfx)
        fall = ex[i] * fall + term
        o = nx - 1 - i
        term = XS[o, 64:128, :].astype(F32)
        gx = jnp.where(o > x, ex[o] * gx + term, gx)
        dgx = jnp.where(o > x, dgx + DX[o][0:1, :], dgx)
        gall = ex[o] * gall + term
    ZG[0] = fall.astype(BF16)
    ZG[1] = gall.astype(BF16)
    ZS[z] = jnp.zeros((64, RV), BF16)
    for d in range(1, nz):
        put(ZG.at[(z + d) // nz], ZS.at[z], sz_s.at[d], sz_r.at[d], (((z + d) % nz) * nx + x, t)).start()

    a_order = [(i + 1) % na for i in range(na)]
    for k in a_order:
        a_pass(k)

    def inside(j, carry):
        cc = column(j)
        cr = crow[pl.ds(j, 1), :]
        qk = QR[blk(j), :]
        sc = lax.dot_general(qk[:, 0:64], qk[:, 64:128], NT, preferred_element_type=F32)
        w = (sc * jnp.exp(-jnp.abs(cc - cr))).astype(BF16)
        RL[blk(j), :] = jnp.dot(w, V[blk(j), :], preferred_element_type=F32) + jnp.dot(
            QB[blk(j), :], SL[j], preferred_element_type=F32
        )
        return carry

    lax.fori_loop(0, nb, inside, 0)

    for d in range(1, 8):
        fr = (t + 8 - d) % 8
        for i in range(2):
            ref = WO.at[i, fr, mine, :]
            put(ref, ref, w1_s.at[i, d], w1_r.at[i, d], (s, sib)).wait_recv()
    for d in range(1, nx):
        ref = WO.at[:, :, mine, :]
        put(ref, ref, w2_s.at[d], w2_r.at[d], (z * nx + (x + d) % nx, t)).start()

    for k in a_order:
        a_last(k)

    for d in range(1, nz):
        o = (z + nz - d) % nz
        put(DZ.at[o], DZ.at[o], dz_s.at[d], dz_r.at[d], (s, sib)).wait_recv()
        put(ZS.at[o], ZS.at[o], sz_s.at[d], sz_r.at[d], (s, sib)).wait_recv()
    fz = init[0:64, :]
    gz = init[64:128, :]
    for i in range(nz):
        term = ZS[i].astype(F32)
        fz = jnp.where(i < z, jnp.exp(DZ[i][0:1, :]) * fz + term, fz)
        o = nz - 1 - i
        term = ZS[o].astype(F32)
        gz = jnp.where(o > z, jnp.exp(DZ[o][0:1, :]) * gz + term, gz)
    ST = jnp.concatenate([fx + jnp.exp(dfx) * fz, gx + jnp.exp(dgx) * gz], axis=0).astype(BF16)

    def finish(j, carry):
        ret = RL[blk(j), :] + jnp.dot(QX[blk(j), :], carry, preferred_element_type=F32)
        cen = ret - jnp.mean(ret, axis=1, keepdims=True)
        nrm = cen * lax.rsqrt(jnp.mean(cen * cen, axis=1, keepdims=True) + NORM_EPS)
        gate = G[blk(j), :].astype(F32)
        R[t, blk(j), :] = (gate / (1.0 + jnp.exp(-gate)) * nrm).astype(BF16)

        @pl.when(j % 2 == 1)
        def _():
            r_own(j // 2)

        return carry

    lax.fori_loop(0, nb, finish, ST)

    for k in range(na):
        r_pass(k)

    for k in range(na):
        a_arrived(k)
    for d in range(1, nx):
        ref = WO.at[:, :, pl.ds(pl.multiple_of(((x + nx - d) % nx) * quarter, quarter), quarter), :]
        put(ref, ref, w2_s.at[d], w2_r.at[d], (s, sib)).wait_recv()

    def big(k):
        return pl.ds(pl.multiple_of(k * arows, arows), arows)

    def out_att(k, carry):
        lhs = jnp.concatenate([A[b, big(k), :] for b in range(8)], axis=1)
        OA[big(k), :] = jnp.dot(lhs, WO[0].reshape(8 * BLK, ocw), preferred_element_type=F32)
        return carry

    lax.fori_loop(0, na, out_att, 0)

    for k in range(na):
        r_last(k)

    def out_ret(k, carry):
        r_arrived(k)
        lhs = jnp.concatenate([R[b, big(k), :] for b in range(8)], axis=1)
        acc = OA[big(k), :] + jnp.dot(lhs, WO[1].reshape(8 * BLK, ocw), preferred_element_type=F32)
        OUT[big(k), :] = acc.astype(BF16)
        pltpu.make_async_copy(OUT.at[big(k), :], out_h.at[big(k), :], lsem.at[14 + k]).start()
        return carry

    lax.fori_loop(0, na, out_ret, 0)

    def drain(k, carry):
        sent(k)
        return carry

    lax.fori_loop(0, nb, drain, 0)
    for k in range(na):
        a_sent(k)
        r_sent(k)
        pltpu.make_async_copy(OUT.at[big(k), :], out_h.at[big(k), :], lsem.at[14 + k]).wait()
    for d in range(1, 8):
        for i in range(2):
            put(oa_h.at[mine, my_cols], WO.at[i, t, mine, :], w1_s.at[i, d], w1_r.at[i, d], (s, sib)).wait_send()
    for d in range(1, nx):
        ref = WO.at[:, :, mine, :]
        put(ref, ref, w2_s.at[d], w2_r.at[d], (s, sib)).wait_send()
        put(XS.at[x], XS.at[x], sx_s.at[d], sx_r.at[d], (s, sib)).wait_send()
        put(DX.at[x], DX.at[x], dx_s.at[d], dx_r.at[d], (s, sib)).wait_send()
    for d in range(1, nz):
        put(ZG.at[0], ZS.at[z], sz_s.at[d], sz_r.at[d], (s, sib)).wait_send()
        put(DZ.at[z], DZ.at[z], dz_s.at[d], dz_r.at[d], (s, sib)).wait_send()
    halo_up.wait_send()
    halo_down.wait_send()


def body(tokens, norm_gain, att_query, att_key, att_value, ret_query, ret_key, ret_value, ret_gate, att_sink, decay_log, init_state,
         out_att, out_ret, *, n_sp):
    rows, cw = tokens.shape
    width = 8 * cw
    ocw = out_att.shape[1] // 8
    nb, na = rows // BLK, rows // (2 * BLK)
    nx = 4 if n_sp >= 16 else 2
    nz = n_sp // nx
    inverse = (np.float64(ROPE_BASE) ** (-2.0 * (np.arange(128) % 32) / 64)).astype(np.float32)[None, :]
    dma = pltpu.SemaphoreType.DMA
    hbm = pl.BlockSpec(memory_space=pltpu.HBM)
    specs = [hbm] * 15
    specs[9] = pl.BlockSpec(memory_space=pltpu.SMEM)
    vm = pltpu.VMEM
    scratch = [
        vm((8, rows, cw), BF16), vm((width, 384), BF16), vm((256, width), BF16), vm((1, width), F32), vm((1, rows), F32),
        vm((128, 128), F32), vm((1, 128), F32),
        vm((rows, 128), BF16), vm((rows + 2 * BLK, 128), BF16), vm((rows, 128), BF16), vm((rows, 128), BF16),
        vm((rows, 128), BF16), vm((rows, 128), BF16), vm((rows, 128), BF16), vm((rows, 128), F32),
        vm((nb, 128, 128), F32), vm((nb, 128, 128), BF16),
        vm((8, rows, 128), BF16), vm((8, rows, 128), BF16), vm((2, 8, 128, ocw), BF16), vm((rows, ocw), F32), vm((rows, ocw), BF16),
        vm((nx, 128, 128), BF16), vm((2, 64, 128), BF16), vm((nz, 64, 128), BF16), vm((nx, 8, 128), F32), vm((nz, 8, 128), F32),
        vm((nb, 128), F32), vm((nb, 128), F32), vm((nb, 128), F32),
        dma((14 + na,)), dma((7, nb)), dma((7, nb)), dma((7, na)), dma((7, na)), dma((7, na)), dma((7, na)),
        dma((2, 8)), dma((2, 8)), dma((nx,)), dma((nx,)), dma((nx,)), dma((nx,)), dma((nx,)), dma((nx,)),
        dma((max(nz, 2),)), dma((max(nz, 2),)), dma((max(nz, 2),)), dma((max(nz, 2),)), dma((2,)), dma((2,)),
    ]
    call = pl.pallas_call(
        functools.partial(kernel, n_sp, nx),
        out_shape=jax.ShapeDtypeStruct((rows, ocw), BF16),
        in_specs=specs,
        out_specs=hbm,
        scratch_shapes=scratch,
        compiler_params=pltpu.CompilerParams(collective_id=0, has_side_effects=True, vmem_limit_bytes=67_043_328),
        name="layer",
    )
    return call(
        tokens, norm_gain.reshape(1, width), att_query, att_key.T, att_value.T, ret_query.T, ret_key.T, ret_value, ret_gate,
        att_sink, decay_log, init_state.reshape(128, 128), inverse, out_att, out_ret,
    )


def solution(mesh):
    in_specs = (
        P("sp", "tp"), P(), P(None, "tp"), P(None, "tp"), P(None, "tp"), P(None, "tp"), P(None, "tp"), P(None, "tp"), P(None, "tp"),
        P("tp"), P("tp", "sp"), P(None, "tp", None, None), P("tp", None), P("tp", None),
    )
    return jax.shard_map(
        functools.partial(body, n_sp=mesh.shape["sp"]), mesh=mesh, in_specs=in_specs, out_specs=P("sp", "tp"), check_vma=False
    )
```

```python
import functools

import jax
import jax.numpy as jnp
import numpy as np
from jax import lax
from jax.experimental import pallas as pl
from jax.experimental.pallas import tpu as pltpu
from jax.sharding import PartitionSpec as P

HD = 64
RV = 128
BLK = 128
NORM_EPS = 1e-06
ROPE_BASE = 10000.0
MESH = pl.DeviceIdType.MESH
F32 = jnp.float32
BF16 = jnp.bfloat16
NT = (((1,), (1,)), ((), ()))
TN = (((0,), (0,)), ((), ()))
AHEAD = 3

L1, R1, OPP, SIB = 0, 1, 2, 3


def kernel(n_sp, nx, tok_h, gain_h, wq_h, wk_h, wv_h, wrq_h, wrk_h, wrv_h, wrg_h, sink_ref, dec_h, init_h, inv_h, oa_h, or_h,
           out_h,
           X, W1, W2, gain, dec, init, inv, Q, KV, V, G, SG, COS, SIN, QR, QB, QX, RL, TT, SL, A, R, WO, OA, OUT,
           XS, ZG, ZS, DX, DZ, crow, bl8, pre8,
           lsem, xs_s, xs_r, as_s, as_r, rs_s, rs_r, w1_s, w1_r, w2_s, w2_r, sx_s, sx_r, dx_s, dx_r, sz_s, sz_r, dz_s, dz_r,
           h_s, h_r):
    rows, cw = tok_h.shape
    nb = rows // BLK
    arows = 2 * BLK
    na = rows // arows
    width = 8 * cw
    ocw = OUT.shape[1]
    nz = n_sp // nx
    quarter = BLK // nx
    s, t = lax.axis_index("sp"), lax.axis_index("tp")
    z, x = s // nx, s % nx
    y, c = t // 2, t % 2
    right = 2 * ((y + 1) % 4) + c
    left = 2 * ((y + 3) % 4) + c
    opp = 2 * ((y + 2) % 4) + c
    sib = 2 * y + (1 - c)
    up, down = (s + 1) % n_sp, (s + n_sp - 1) % n_sp

    loads = [
        (dec_h, dec), (tok_h, X.at[t]), (gain_h, gain), (inv_h, inv), (init_h, init),
        (wq_h, W1.at[:, 0:128]), (wrv_h, W1.at[:, 128:256]), (wrg_h, W1.at[:, 256:384]),
        (wk_h, W2.at[0:64]), (wv_h, W2.at[64:128]), (wrq_h, W2.at[128:192]), (wrk_h, W2.at[192:256]),
    ]
    mine = pl.ds(pl.multiple_of(x * quarter, quarter), quarter)
    my_cols = pl.ds(pl.multiple_of(t * ocw, 128), ocw)
    loads += [(oa_h.at[mine, my_cols], WO.at[0, t, mine, :]), (or_h.at[mine, my_cols], WO.at[1, t, mine, :])]
    copies = [pltpu.make_async_copy(a, b, lsem.at[i]) for i, (a, b) in enumerate(loads)]
    for cp in copies:
        cp.start()

    barrier = pltpu.get_barrier_semaphore()
    partners = [(s, (t + d) % 8) for d in range(1, 8)]
    partners += [(z * nx + (x + d) % nx, t) for d in range(1, nx)]
    partners += [(((z + d) % nz) * nx + x, t) for d in range(1, nz)]
    partners += [(up, t), (down, t)]
    for p in partners:
        pl.semaphore_signal(barrier, inc=1, device_id=p, device_id_type=MESH)

    copies[0].wait()
    for b in range(nb):
        crow[b : b + 1, :] = dec[:, b * BLK : (b + 1) * BLK]
    cum = crow[...]
    lane = lax.broadcasted_iota(jnp.int32, (nb, BLK), 1)
    for sh in (1, 2, 4, 8, 16, 32, 64):
        cum = cum + jnp.where(lane >= sh, pltpu.roll(cum, sh, 1), 0.0)
    crow[...] = cum
    bl8[...] = jnp.broadcast_to(cum[:, BLK - 1 : BLK], (nb, BLK))
    run = jnp.zeros((1, BLK), F32)
    for b in range(nb):
        pre8[b : b + 1, :] = run
        run = run + bl8[b : b + 1, :]
    tot = run
    DX[x] = jnp.broadcast_to(tot, (8, BLK))
    for i in range(1, 5):
        copies[i].wait()

    pl.semaphore_wait(barrier, len(partners))

    def put(src, dst, send, recv, dev):
        return pltpu.make_async_remote_copy(src_ref=src, dst_ref=dst, send_sem=send, recv_sem=recv, device_id=dev, device_id_type=MESH)

    def gather(buf, n_rows, ss, rs):
        def part(b, k):
            return buf.at[b, pl.ds(pl.multiple_of(k * n_rows, n_rows), n_rows), :]

        def hop(b, k, send, recv, tp):
            ref = part(b, k)
            return put(ref, ref, ss.at[send, k], rs.at[recv, k], (s, tp))

        def own(k):
            hop(t, k, 0, L1, right).start()
            hop(t, k, 1, R1, left).start()
            hop(t, k, 2, SIB, sib).start()

        def pass_on(k):
            hop(left, k, 3, L1, right).wait_recv()
            even = k % 2 == 0

            @pl.when(even)
            def _():
                hop(left, k, 6, OPP, right).start()

            hop(left, k, 3, SIB + 1, sib).start()
            hop(right, k, 4, R1, left).wait_recv()

            @pl.when(k % 2 == 1)
            def _():
                hop(right, k, 6, OPP, left).start()

            hop(right, k, 4, SIB + 2, sib).start()

        def pass_last(k):
            hop(opp, k, 5, OPP, right).wait_recv()
            hop(opp, k, 5, SIB + 3, sib).start()

        def arrived(k):
            hop(sib, k, 2, SIB, sib).wait_recv()
            hop(2 * ((y + 3) % 4) + 1 - c, k, 3, SIB + 1, sib).wait_recv()
            hop(2 * ((y + 1) % 4) + 1 - c, k, 4, SIB + 2, sib).wait_recv()
            hop(2 * ((y + 2) % 4) + 1 - c, k, 5, SIB + 3, sib).wait_recv()

        def sent(k):
            for i in range(7):
                hop(t, k, i, L1, right).wait_send()

        return own, pass_on, pass_last, arrived, sent

    own, pass_on, pass_last, arrived, sent = gather(X, BLK, xs_s, xs_r)
    a_own, a_pass, a_last, a_arrived, a_sent = gather(A, arows, as_s, as_r)
    r_own, r_pass, r_last, r_arrived, r_sent = gather(R, BLK, rs_s, rs_r)

    for k in range(AHEAD):
        own(k)
    for d in range(1, nx):
        put(DX.at[x], DX.at[x], dx_s.at[d], dx_r.at[d], (z * nx + (x + d) % nx, t)).start()

    lane_b = lax.broadcasted_iota(jnp.int32, (BLK, BLK), 1)
    row_b = lax.broadcasted_iota(jnp.int32, (BLK, BLK), 0)
    low = lane_b < 64

    def blk(j):
        return pl.ds(pl.multiple_of(j * BLK, BLK), BLK)

    def column(j):
        row = jnp.broadcast_to(crow[pl.ds(j, 1), :], (BLK, BLK))
        return jnp.sum(jnp.where(lane_b == row_b, row, 0.0), axis=1, keepdims=True)

    def tables(j, carry):
        pos = (s * rows + j * BLK + row_b).astype(F32)
        angle = pos * inv[...]
        scale = jnp.where(low, 1.0, 64**-0.5).astype(F32)
        COS[blk(j), :] = jnp.cos(angle) * scale
        SIN[blk(j), :] = jnp.sin(angle) * jnp.where(lane_b % 64 < 32, -scale, scale)
        return carry

    def project(m):
        arrived(2 * m)
        arrived(2 * m + 1)
        two = pl.ds(pl.multiple_of(m * 2 * BLK, 2 * BLK), 2 * BLK)
        squares = jnp.zeros((2 * BLK, cw), F32)
        parts = []
        for b in range(8):
            xf = X[b, two, :].astype(F32)
            squares = squares + xf * xf
            parts.append((xf * gain[:, b * cw : (b + 1) * cw]).astype(BF16))
        normed = jnp.concatenate(parts, axis=1)
        inv_rms = lax.rsqrt(jnp.sum(squares, axis=1, keepdims=True) / width + NORM_EPS)
        p = (jnp.dot(normed, W1[...], preferred_element_type=F32) * inv_rms).astype(BF16)
        Q[two, :] = p[:, 0:128]
        V[two, :] = p[:, 128:256]
        G[two, :] = p[:, 256:384]
        KV[pl.ds(pl.multiple_of(m * 2 * BLK + BLK, BLK), 2 * BLK), :] = p[:, 384:512]
        for h in range(2):
            j = 2 * m + h
            cosine, sine, cc = COS[blk(j), :], SIN[blk(j), :], column(j)
            bl = bl8[pl.ds(j, 1), :]
            pre = pre8[pl.ds(j, 1), :]
            rqk = p[h * BLK : (h + 1) * BLK, 512:640].astype(F32)
            swapped = jnp.where(lane_b % 64 < 32, pltpu.roll(rqk, 96, 1), pltpu.roll(rqk, 32, 1))
            rot = rqk * cosine + swapped * sine
            QR[blk(j), :] = rot.astype(BF16)
            other = pltpu.roll(rot, 64, 1)
            qq = jnp.where(low, rot, other)
            kk = jnp.where(low, other, rot)
            to_end = jnp.exp(bl - cc)
            to_here = jnp.exp(jnp.broadcast_to(cc, (BLK, BLK)))
            QB[blk(j), :] = (qq * jnp.where(low, to_here, to_end)).astype(BF16)
            full = cc + pre
            QX[blk(j), :] = (qq * jnp.exp(jnp.where(low, full, tot - full))).astype(BF16)
            kw = (kk * jnp.where(low, to_end, to_here)).astype(BF16)
            v = p[h * BLK : (h + 1) * BLK, 128:256]
            TT[j] = lax.dot_general(kw, v, TN, preferred_element_type=F32)

    for i in range(5, 14):
        copies[i].wait()
    for b in range(8):
        W1[b * cw : (b + 1) * cw, 384:640] = W2[:, b * cw : (b + 1) * cw].T
    lax.fori_loop(0, nb, tables, 0)

    halo_up = put(KV.at[pl.ds(rows, BLK), :], KV.at[pl.ds(0, BLK), :], h_s.at[0], h_r.at[0], (up, t))
    halo_down = put(KV.at[pl.ds(BLK, BLK), :], KV.at[pl.ds(rows + BLK, BLK), :], h_s.at[1], h_r.at[1], (down, t))

    row_q = lax.broadcasted_iota(jnp.int32, (2 * BLK, BLK), 0) % BLK
    lane_q = lax.broadcasted_iota(jnp.int32, (2 * BLK, BLK), 1)
    sink = jnp.where(lax.broadcasted_iota(jnp.int32, (2 * BLK, 1), 0) < BLK, sink_ref[0], sink_ref[1])

    def attend(j):
        q = Q[blk(j), :]
        q2 = jnp.concatenate([q[:, 0:64], q[:, 64:128]], axis=0)
        kv = KV[pl.ds(pl.multiple_of(j * BLK, BLK), 3 * BLK), :]
        sc = lax.dot_general(q2, kv[:, 0:64], NT, preferred_element_type=F32) * HD**-0.5
        first = jnp.where(s * nb + j == 0, BLK, 0)
        last = jnp.where(s * nb + j == n_sp * nb - 1, BLK, 0)
        s0 = jnp.where(lane_q - first >= row_q, sc[:, 0:128], -jnp.inf)
        s1 = sc[:, 128:256]
        s2 = jnp.where(lane_q + last <= row_q, sc[:, 256:384], -jnp.inf)
        top = jnp.maximum(jnp.max(jnp.maximum(jnp.maximum(s0, s1), s2), axis=1, keepdims=True), sink)
        e0, e1, e2 = jnp.exp(s0 - top), jnp.exp(s1 - top), jnp.exp(s2 - top)
        den = jnp.sum(e0 + e1 + e2, axis=1, keepdims=True) + jnp.exp(sink - top)
        ee = jnp.concatenate([e0.astype(BF16), e1.astype(BF16), e2.astype(BF16)], axis=1)
        o = jnp.dot(ee, kv[:, 64:128], preferred_element_type=F32) / den
        A[t, blk(j), :] = jnp.concatenate([o[0:BLK], o[BLK : 2 * BLK]], axis=1).astype(BF16)

    def weights_out():
        for i, half in enumerate((oa_h, or_h)):
            for d in range(1, 8):
                to = (t + d) % 8
                cols = pl.ds(pl.multiple_of(to * ocw, 128), ocw)
                put(half.at[mine, cols], WO.at[i, t, mine, :], w1_s.at[i, d], w1_r.at[i, d], (s, to)).start()

    def on(k):
        pass_on(k)
        if k + AHEAD < nb:
            own(k + AHEAD)

    on(0)
    on(1)
    on(2)
    pass_last(0)
    on(3)
    pass_last(1)
    on(4)
    project(0)
    halo_down.start()
    pass_last(2)
    on(5)
    pass_last(3)
    on(6)
    project(1)
    pass_last(4)
    on(7)
    weights_out()
    pass_last(5)
    attend(1)
    attend(2)
    pass_last(6)
    project(2)
    pass_last(7)
    project(3)
    halo_up.start()

    f = jnp.zeros((64, RV), F32)
    g = jnp.zeros((64, RV), F32)
    for b in range(nb):
        SL[b, 0:64, :] = f.astype(BF16)
        f = jnp.exp(bl8[b : b + 1, :]) * f + TT[b, 0:64, :]
        e = nb - 1 - b
        SL[e, 64:128, :] = g.astype(BF16)
        g = jnp.exp(bl8[e : e + 1, :]) * g + TT[e, 64:128, :]
    XS[x, 0:64, :] = f.astype(BF16)
    XS[x, 64:128, :] = g.astype(BF16)
    for d in range(1, nx):
        put(XS.at[x], XS.at[x], sx_s.at[d], sx_r.at[d], (z * nx + (x + d) % nx, t)).start()

    for d in range(1, nx):
        o = (x + nx - d) % nx
        put(DX.at[o], DX.at[o], dx_s.at[d], dx_r.at[d], (s, sib)).wait_recv()
    total = DX[0]
    for i in range(1, nx):
        total = total + DX[i]
    DZ[z] = total
    for d in range(1, nz):
        put(DZ.at[z], DZ.at[z], dz_s.at[d], dz_r.at[d], (((z + d) % nz) * nx + x, t)).start()

    attend(3)
    attend(4)
    a_own(1)
    halo_down.wait_recv()
    attend(5)
    attend(6)
    attend(7)
    a_own(2)
    a_own(3)

    xr, xl = z * nx + (x + 1) % nx, z * nx + (x + nx - 1) % nx

    def quarter_of(o):
        return pl.ds(pl.multiple_of(((x + o + nx) % nx) * quarter, quarter), quarter)

    def w2_own(i):
        for d in range(1, 8):
            ref = WO.at[i, (t + 8 - d) % 8, mine, :]
            put(ref, ref, w1_s.at[i, d], w1_r.at[i, d], (s, sib)).wait_recv()
        ref = WO.at[i, :, mine, :]
        put(ref, ref, w2_s.at[i, 0], w2_r.at[i, 0], (xr, t)).start()
        put(ref, ref, w2_s.at[i, 1], w2_r.at[i, 1], (xl, t)).start()

    def w2_pass(i):
        from_left = WO.at[i, :, quarter_of(-1), :]
        from_right = WO.at[i, :, quarter_of(1), :]
        put(from_left, from_left, w2_s.at[i, 0], w2_r.at[i, 0], (xr, t)).wait_recv()
        half = WO.at[i, 0:4, quarter_of(-1), :]
        put(half, half, w2_s.at[i, 2], w2_r.at[i, 2], (xr, t)).start()
        put(from_right, from_right, w2_s.at[i, 1], w2_r.at[i, 1], (xl, t)).wait_recv()
        half = WO.at[i, 4:8, quarter_of(1), :]
        put(half, half, w2_s.at[i, 3], w2_r.at[i, 3], (xl, t)).start()

    def w2_done(i):
        half = WO.at[i, 0:4, quarter_of(2), :]
        put(half, half, w2_s.at[i, 2], w2_r.at[i, 2], (xr, t)).wait_recv()
        half = WO.at[i, 4:8, quarter_of(2), :]
        put(half, half, w2_s.at[i, 3], w2_r.at[i, 3], (xl, t)).wait_recv()

    def w2_sent(i):
        ref = WO.at[i, :, mine, :]
        half = WO.at[i, 0:4, mine, :]
        put(ref, ref, w2_s.at[i, 0], w2_r.at[i, 0], (xr, t)).wait_send()
        put(ref, ref, w2_s.at[i, 1], w2_r.at[i, 1], (xl, t)).wait_send()
        put(half, half, w2_s.at[i, 2], w2_r.at[i, 2], (xr, t)).wait_send()
        put(half, half, w2_s.at[i, 3], w2_r.at[i, 3], (xl, t)).wait_send()

    w2_own(0)
    w2_own(1)

    for d in range(1, nx):
        o = (x + nx - d) % nx
        put(XS.at[o], XS.at[o], sx_s.at[d], sx_r.at[d], (s, sib)).wait_recv()
    ex = [jnp.exp(DX[i][0:1, :]) for i in range(nx)]
    fx = jnp.zeros((64, RV), F32)
    gx = jnp.zeros((64, RV), F32)
    fall = jnp.zeros((64, RV), F32)
    gall = jnp.zeros((64, RV), F32)
    dfx = jnp.zeros((1, RV), F32)
    dgx = jnp.zeros((1, RV), F32)
    for i in range(nx):
        term = XS[i, 0:64, :].astype(F32)
        fx = jnp.where(i < x, ex[i] * fx + term, fx)
        dfx = jnp.where(i < x, dfx + DX[i][0:1, :], dfx)
        fall = ex[i] * fall + term
        o = nx - 1 - i
        term = XS[o, 64:128, :].astype(F32)
        gx = jnp.where(o > x, ex[o] * gx + term, gx)
        dgx = jnp.where(o > x, dgx + DX[o][0:1, :], dgx)
        gall = ex[o] * gall + term
    ZG[0] = fall.astype(BF16)
    ZG[1] = gall.astype(BF16)
    ZS[z] = jnp.zeros((64, RV), BF16)
    for d in range(1, nz):
        put(ZG.at[(z + d) // nz], ZS.at[z], sz_s.at[d], sz_r.at[d], (((z + d) % nz) * nx + x, t)).start()

    halo_up.wait_recv()
    attend(0)
    a_own(0)

    def inside(j):
        cc = column(j)
        cr = crow[pl.ds(j, 1), :]
        qk = QR[blk(j), :]
        sc = lax.dot_general(qk[:, 0:64], qk[:, 64:128], NT, preferred_element_type=F32)
        w = (sc * jnp.exp(-jnp.abs(cc - cr))).astype(BF16)
        RL[blk(j), :] = jnp.dot(w, V[blk(j), :], preferred_element_type=F32) + jnp.dot(
            QB[blk(j), :], SL[j], preferred_element_type=F32
        )
        gate = G[blk(j), :].astype(F32)
        SG[blk(j), :] = gate / (1.0 + jnp.exp(-gate))

    def inside_two(m, carry):
        inside(2 * m)
        inside(2 * m + 1)
        return carry

    lax.fori_loop(0, na, inside_two, 0)

    for k in range(1, na):
        a_pass(k)

    w2_pass(0)
    for k in range(1, na):
        a_last(k)
    w2_pass(1)
    a_pass(0)

    for d in range(1, nz):
        o = (z + nz - d) % nz
        put(DZ.at[o], DZ.at[o], dz_s.at[d], dz_r.at[d], (s, sib)).wait_recv()
        put(ZS.at[o], ZS.at[o], sz_s.at[d], sz_r.at[d], (s, sib)).wait_recv()
    fz = init[0:64, :]
    gz = init[64:128, :]
    for i in range(nz):
        term = ZS[i].astype(F32)
        fz = jnp.where(i < z, jnp.exp(DZ[i][0:1, :]) * fz + term, fz)
        o = nz - 1 - i
        term = ZS[o].astype(F32)
        gz = jnp.where(o > z, jnp.exp(DZ[o][0:1, :]) * gz + term, gz)
    ST = jnp.concatenate([fx + jnp.exp(dfx) * fz, gx + jnp.exp(dgx) * gz], axis=0).astype(BF16)

    def big(k):
        return pl.ds(pl.multiple_of(k * arows, arows), arows)

    def finish(k, carry):
        ret = RL[big(k), :] + jnp.dot(QX[big(k), :], carry, preferred_element_type=F32)
        cen = ret - jnp.mean(ret, axis=1, keepdims=True)
        nrm = cen * lax.rsqrt(jnp.mean(cen * cen, axis=1, keepdims=True) + NORM_EPS)
        R[t, big(k), :] = (SG[big(k), :] * nrm).astype(BF16)
        r_own(2 * k)
        r_own(2 * k + 1)
        return carry

    lax.fori_loop(0, na, finish, ST)

    def out_att(k):
        lhs = jnp.concatenate([A[b, big(k), :] for b in range(8)], axis=1)
        OA[big(k), :] = jnp.dot(lhs, WO[0].reshape(8 * BLK, ocw), preferred_element_type=F32)

    def out_ret(k, carry):
        r_arrived(k)
        lhs = jnp.concatenate([R[b, blk(k), :] for b in range(8)], axis=1)
        acc = OA[blk(k), :] + jnp.dot(lhs, WO[1].reshape(8 * BLK, ocw), preferred_element_type=F32)
        OUT[blk(k), :] = acc.astype(BF16)
        pltpu.make_async_copy(OUT.at[blk(k), :], out_h.at[blk(k), :], lsem.at[14 + k]).start()
        return carry

    for k in range(nb):
        r_pass(k)
        if k == 1:
            a_last(0)
        if k == nb // 2:
            for i in range(na):
                a_arrived(i)
            w2_done(0)
        if k >= nb // 2:
            out_att(k - nb // 2)
    for k in range(nb // 2):
        r_last(k)
    w2_done(1)
    for k in range(nb // 2, nb):
        out_ret(k - nb // 2, 0)
        r_last(k)
    lax.fori_loop(nb // 2, nb, out_ret, 0)

    def drain(k, carry):
        sent(k)
        r_sent(k)
        pltpu.make_async_copy(OUT.at[blk(k), :], out_h.at[blk(k), :], lsem.at[14 + k]).wait()
        return carry

    lax.fori_loop(0, nb, drain, 0)
    for k in range(na):
        a_sent(k)
    for i in range(2):
        for d in range(1, 8):
            put(oa_h.at[mine, my_cols], WO.at[i, t, mine, :], w1_s.at[i, d], w1_r.at[i, d], (s, sib)).wait_send()
        w2_sent(i)
    for d in range(1, nx):
        put(XS.at[x], XS.at[x], sx_s.at[d], sx_r.at[d], (s, sib)).wait_send()
        put(DX.at[x], DX.at[x], dx_s.at[d], dx_r.at[d], (s, sib)).wait_send()
    for d in range(1, nz):
        put(ZG.at[0], ZS.at[z], sz_s.at[d], sz_r.at[d], (s, sib)).wait_send()
        put(DZ.at[z], DZ.at[z], dz_s.at[d], dz_r.at[d], (s, sib)).wait_send()
    halo_up.wait_send()
    halo_down.wait_send()


def body(tokens, norm_gain, att_query, att_key, att_value, ret_query, ret_key, ret_value, ret_gate, att_sink, decay_log, init_state,
         out_att, out_ret, *, n_sp):
    rows, cw = tokens.shape
    width = 8 * cw
    ocw = out_att.shape[1] // 8
    nb, na = rows // BLK, rows // (2 * BLK)
    nx = 4
    nz = n_sp // nx
    inverse = (np.float64(ROPE_BASE) ** (-2.0 * (np.arange(128) % 32) / 64)).astype(np.float32)[None, :]
    dma = pltpu.SemaphoreType.DMA
    hbm = pl.BlockSpec(memory_space=pltpu.HBM)
    specs = [hbm] * 15
    specs[9] = pl.BlockSpec(memory_space=pltpu.SMEM)
    vm = pltpu.VMEM
    scratch = [
        vm((8, rows, cw), BF16), vm((width, 640), BF16), vm((256, width), BF16), vm((1, width), F32), vm((1, rows), F32),
        vm((128, 128), F32), vm((1, 128), F32),
        vm((rows, 128), BF16), vm((rows + 2 * BLK, 128), BF16), vm((rows, 128), BF16), vm((rows, 128), BF16), vm((rows, 128), F32),
        vm((rows, 128), F32), vm((rows, 128), F32), vm((rows, 128), BF16), vm((rows, 128), BF16), vm((rows, 128), BF16), vm((rows, 128), F32),
        vm((nb, 128, 128), F32), vm((nb, 128, 128), BF16),
        vm((8, rows, 128), BF16), vm((8, rows, 128), BF16), vm((2, 8, 128, ocw), BF16), vm((rows, ocw), F32), vm((rows, ocw), BF16),
        vm((nx, 128, 128), BF16), vm((2, 64, 128), BF16), vm((nz, 64, 128), BF16), vm((nx, 8, 128), F32), vm((nz, 8, 128), F32),
        vm((nb, 128), F32), vm((nb, 128), F32), vm((nb, 128), F32),
        dma((14 + nb,)), dma((7, nb)), dma((7, nb)), dma((7, na)), dma((7, na)), dma((7, nb)), dma((7, nb)),
        dma((2, 8)), dma((2, 8)), dma((2, 4)), dma((2, 4)), dma((nx,)), dma((nx,)), dma((nx,)), dma((nx,)),
        dma((max(nz, 2),)), dma((max(nz, 2),)), dma((max(nz, 2),)), dma((max(nz, 2),)), dma((2,)), dma((2,)),
    ]
    call = pl.pallas_call(
        functools.partial(kernel, n_sp, nx),
        out_shape=jax.ShapeDtypeStruct((rows, ocw), BF16),
        in_specs=specs,
        out_specs=hbm,
        scratch_shapes=scratch,
        compiler_params=pltpu.CompilerParams(collective_id=0, has_side_effects=True, vmem_limit_bytes=67_043_328),
        name="layer",
    )
    return call(
        tokens, norm_gain.reshape(1, width), att_query, att_key.T, att_value.T, ret_query.T, ret_key.T, ret_value, ret_gate,
        att_sink, decay_log, init_state.reshape(128, 128), inverse, out_att, out_ret,
    )


def solution(mesh):
    in_specs = (
        P("sp", "tp"), P(), P(None, "tp"), P(None, "tp"), P(None, "tp"), P(None, "tp"), P(None, "tp"), P(None, "tp"), P(None, "tp"),
        P("tp"), P("tp", "sp"), P(None, "tp", None, None), P("tp", None), P("tp", None),
    )
    return jax.shard_map(
        functools.partial(body, n_sp=mesh.shape["sp"]), mesh=mesh, in_specs=in_specs, out_specs=P("sp", "tp"), check_vma=False
    )
```

```python
import functools

import jax
import jax.numpy as jnp
import numpy as np
from jax import lax
from jax.experimental import pallas as pl
from jax.experimental.pallas import tpu as pltpu
from jax.sharding import PartitionSpec as P

HD = 64
RV = 128
BLK = 128
NORM_EPS = 1e-06
ROPE_BASE = 10000.0
MESH = pl.DeviceIdType.MESH
F32 = jnp.float32
BF16 = jnp.bfloat16
NT = (((1,), (1,)), ((), ()))
TN = (((0,), (0,)), ((), ()))
AHEAD = 5

L1, R1, OPP, SIB = 0, 1, 2, 3


def kernel(n_sp, nx, tok_h, gain_h, wq_h, wk_h, wv_h, wrq_h, wrk_h, wrv_h, wrg_h, sink_ref, dec_h, init_h, inv_h, oa_h, or_h,
           out_h,
           X, W1, W2, gain, dec, init, inv, Q, KV, V, G, SG, COS, SIN, ACC, SQ, QR, QB, QX, RL, TT, SL, A, R, WO, OA, OUT,
           XS, ZG, ZS, DX, DZ, crow, bl8, pre8,
           lsem, xs_s, xs_r, as_s, as_r, rs_s, rs_r, w1_s, w1_r, w2_s, w2_r, sx_s, sx_r, dx_s, dx_r, sz_s, sz_r, dz_s, dz_r,
           h_s, h_r):
    rows, cw = tok_h.shape
    nb = rows // BLK
    arows = 2 * BLK
    na = rows // arows
    width = 8 * cw
    ocw = OUT.shape[1]
    nz = n_sp // nx
    quarter = BLK // nx
    s, t = lax.axis_index("sp"), lax.axis_index("tp")
    z, x = s // nx, s % nx
    y, c = t // 2, t % 2
    right = 2 * ((y + 1) % 4) + c
    left = 2 * ((y + 3) % 4) + c
    opp = 2 * ((y + 2) % 4) + c
    sib = 2 * y + (1 - c)
    sib_right = 2 * ((y + 1) % 4) + 1 - c
    sib_left = 2 * ((y + 3) % 4) + 1 - c
    sib_opp = 2 * ((y + 2) % 4) + 1 - c
    up, down = (s + 1) % n_sp, (s + n_sp - 1) % n_sp

    loads = [
        (dec_h, dec), (tok_h, X.at[t]), (gain_h, gain), (inv_h, inv), (init_h, init),
        (wq_h, W1.at[:, 0:128]), (wrv_h, W1.at[:, 128:256]), (wrg_h, W1.at[:, 256:384]),
        (wk_h, W2.at[0:64]), (wv_h, W2.at[64:128]), (wrq_h, W2.at[128:192]), (wrk_h, W2.at[192:256]),
    ]
    mine = pl.ds(pl.multiple_of(x * quarter, quarter), quarter)
    my_cols = pl.ds(pl.multiple_of(t * ocw, 128), ocw)
    loads += [(oa_h.at[mine, my_cols], WO.at[0, t, mine, :]), (or_h.at[mine, my_cols], WO.at[1, t, mine, :])]
    copies = [pltpu.make_async_copy(a, b, lsem.at[i]) for i, (a, b) in enumerate(loads)]
    for cp in copies:
        cp.start()

    barrier = pltpu.get_barrier_semaphore()
    partners = [(s, (t + d) % 8) for d in range(1, 8)]
    partners += [(z * nx + (x + d) % nx, t) for d in range(1, nx)]
    partners += [(((z + d) % nz) * nx + x, t) for d in range(1, nz)]
    partners += [(up, t), (down, t)]
    for p in partners:
        pl.semaphore_signal(barrier, inc=1, device_id=p, device_id_type=MESH)

    copies[0].wait()
    for b in range(nb):
        crow[b : b + 1, :] = dec[:, b * BLK : (b + 1) * BLK]
    cum = crow[...]
    lane = lax.broadcasted_iota(jnp.int32, (nb, BLK), 1)
    for sh in (1, 2, 4, 8, 16, 32, 64):
        cum = cum + jnp.where(lane >= sh, pltpu.roll(cum, sh, 1), 0.0)
    crow[...] = cum
    bl8[...] = jnp.broadcast_to(cum[:, BLK - 1 : BLK], (nb, BLK))
    run = jnp.zeros((1, BLK), F32)
    for b in range(nb):
        pre8[b : b + 1, :] = run
        run = run + bl8[b : b + 1, :]
    tot = run
    DX[x] = jnp.broadcast_to(tot, (8, BLK))
    for i in range(1, 5):
        copies[i].wait()

    pl.semaphore_wait(barrier, len(partners))

    def put(src, dst, send, recv, dev):
        return pltpu.make_async_remote_copy(src_ref=src, dst_ref=dst, send_sem=send, recv_sem=recv, device_id=dev, device_id_type=MESH)

    def gather(buf, n_rows, ss, rs):
        def part(b, k):
            return buf.at[b, pl.ds(pl.multiple_of(k * n_rows, n_rows), n_rows), :]

        def hop(b, k, send, recv, tp):
            ref = part(b, k)
            return put(ref, ref, ss.at[send, k], rs.at[recv, k], (s, tp))

        def own(k):
            hop(t, k, 0, L1, right).start()
            hop(t, k, 1, R1, left).start()
            hop(t, k, 2, SIB, sib).start()

        def pass_on(k):
            hop(left, k, 3, L1, right).wait_recv()
            even = k % 2 == 0

            @pl.when(even)
            def _():
                hop(left, k, 6, OPP, right).start()

            hop(left, k, 3, SIB + 1, sib).start()
            hop(right, k, 4, R1, left).wait_recv()

            @pl.when(k % 2 == 1)
            def _():
                hop(right, k, 6, OPP, left).start()

            hop(right, k, 4, SIB + 2, sib).start()

        def pass_last(k):
            hop(opp, k, 5, OPP, right).wait_recv()
            hop(opp, k, 5, SIB + 3, sib).start()

        def arrived_near(k):
            hop(sib, k, 2, SIB, sib).wait_recv()
            hop(sib_left, k, 3, SIB + 1, sib).wait_recv()
            hop(sib_right, k, 4, SIB + 2, sib).wait_recv()

        def arrived_opp(k):
            hop(sib_opp, k, 5, SIB + 3, sib).wait_recv()

        def arrived(k):
            arrived_near(k)
            arrived_opp(k)

        def sent(k):
            for i in range(7):
                hop(t, k, i, L1, right).wait_send()

        return own, pass_on, pass_last, arrived, sent, arrived_near, arrived_opp

    own, pass_on, pass_last, arrived, sent, arrived_near, arrived_opp = gather(X, BLK, xs_s, xs_r)
    a_own, a_pass, a_last, a_arrived, a_sent, _, _ = gather(A, arows, as_s, as_r)
    r_own, r_pass, r_last, r_arrived, r_sent, _, _ = gather(R, BLK, rs_s, rs_r)

    for k in range(AHEAD):
        own(k)
    for d in range(1, nx):
        put(DX.at[x], DX.at[x], dx_s.at[d], dx_r.at[d], (z * nx + (x + d) % nx, t)).start()

    lane_b = lax.broadcasted_iota(jnp.int32, (BLK, BLK), 1)
    row_b = lax.broadcasted_iota(jnp.int32, (BLK, BLK), 0)
    low = lane_b < 64

    def blk(j):
        return pl.ds(pl.multiple_of(j * BLK, BLK), BLK)

    def column(j):
        row = jnp.broadcast_to(crow[pl.ds(j, 1), :], (BLK, BLK))
        return jnp.sum(jnp.where(lane_b == row_b, row, 0.0), axis=1, keepdims=True)

    def tables(j, carry):
        pos = (s * rows + j * BLK + row_b).astype(F32)
        angle = pos * inv[...]
        scale = jnp.where(low, 1.0, 64**-0.5).astype(F32)
        COS[blk(j), :] = jnp.cos(angle) * scale
        SIN[blk(j), :] = jnp.sin(angle) * jnp.where(lane_b % 64 < 32, -scale, scale)
        return carry

    def pair(m):
        return pl.ds(pl.multiple_of(m * 2 * BLK, 2 * BLK), 2 * BLK)

    def sums(m, acc, squares, blocks):
        for b in blocks:
            cols = pl.ds(pl.multiple_of(b * cw, cw), cw)
            xf = X[b, pair(m), :].astype(F32)
            sq = xf * xf
            squares = squares + sum(sq[:, i : i + 128] for i in range(0, cw, 128))
            acc = acc + jnp.dot((xf * gain[:, cols]).astype(BF16), W1[cols, :], preferred_element_type=F32)
        return acc, squares

    def project_near(m):
        arrived_near(2 * m)
        arrived_near(2 * m + 1)
        zero = jnp.zeros((2 * BLK, 640), F32), jnp.zeros((2 * BLK, 128), F32)
        ACC[m % 2], SQ[m % 2] = sums(m, *zero, (t, sib, left, right, sib_left, sib_right))

    def project(m):
        two = pair(m)
        arrived_opp(2 * m)
        arrived_opp(2 * m + 1)
        acc, squares = sums(m, ACC[m % 2], SQ[m % 2], (opp, sib_opp))
        inv_rms = lax.rsqrt(jnp.sum(squares, axis=1, keepdims=True) / width + NORM_EPS)
        p = (acc * inv_rms).astype(BF16)
        Q[two, :] = p[:, 0:128]
        V[two, :] = p[:, 128:256]
        G[two, :] = p[:, 256:384]
        KV[pl.ds(pl.multiple_of(m * 2 * BLK + BLK, BLK), 2 * BLK), :] = p[:, 384:512]
        for h in range(2):
            j = 2 * m + h
            cosine, sine, cc = COS[blk(j), :], SIN[blk(j), :], column(j)
            bl = bl8[pl.ds(j, 1), :]
            pre = pre8[pl.ds(j, 1), :]
            rqk = p[h * BLK : (h + 1) * BLK, 512:640].astype(F32)
            swapped = jnp.where(lane_b % 64 < 32, pltpu.roll(rqk, 96, 1), pltpu.roll(rqk, 32, 1))
            rot = rqk * cosine + swapped * sine
            QR[blk(j), :] = rot.astype(BF16)
            other = pltpu.roll(rot, 64, 1)
            qq = jnp.where(low, rot, other)
            kk = jnp.where(low, other, rot)
            to_end = jnp.exp(bl - cc)
            to_here = jnp.exp(jnp.broadcast_to(cc, (BLK, BLK)))
            QB[blk(j), :] = (qq * jnp.where(low, to_here, to_end)).astype(BF16)
            full = cc + pre
            QX[blk(j), :] = (qq * jnp.exp(jnp.where(low, full, tot - full))).astype(BF16)
            kw = (kk * jnp.where(low, to_end, to_here)).astype(BF16)
            v = p[h * BLK : (h + 1) * BLK, 128:256]
            TT[j] = lax.dot_general(kw, v, TN, preferred_element_type=F32)

    for i in range(5, 14):
        copies[i].wait()
    for b in range(8):
        W1[b * cw : (b + 1) * cw, 384:640] = W2[:, b * cw : (b + 1) * cw].T
    lax.fori_loop(0, nb, tables, 0)

    halo_up = put(KV.at[pl.ds(rows, BLK), :], KV.at[pl.ds(0, BLK), :], h_s.at[0], h_r.at[0], (up, t))
    halo_down = put(KV.at[pl.ds(BLK, BLK), :], KV.at[pl.ds(rows + BLK, BLK), :], h_s.at[1], h_r.at[1], (down, t))

    row_q = lax.broadcasted_iota(jnp.int32, (2 * BLK, BLK), 0) % BLK
    lane_q = lax.broadcasted_iota(jnp.int32, (2 * BLK, BLK), 1)
    sink = jnp.where(lax.broadcasted_iota(jnp.int32, (2 * BLK, 1), 0) < BLK, sink_ref[0], sink_ref[1])

    def attend(j):
        q = Q[blk(j), :]
        q2 = jnp.concatenate([q[:, 0:64], q[:, 64:128]], axis=0)
        kv = KV[pl.ds(pl.multiple_of(j * BLK, BLK), 3 * BLK), :]
        sc = lax.dot_general(q2, kv[:, 0:64], NT, preferred_element_type=F32) * HD**-0.5
        first = jnp.where(s * nb + j == 0, BLK, 0)
        last = jnp.where(s * nb + j == n_sp * nb - 1, BLK, 0)
        s0 = jnp.where(lane_q - first >= row_q, sc[:, 0:128], -jnp.inf)
        s1 = sc[:, 128:256]
        s2 = jnp.where(lane_q + last <= row_q, sc[:, 256:384], -jnp.inf)
        top = jnp.maximum(jnp.max(jnp.maximum(jnp.maximum(s0, s1), s2), axis=1, keepdims=True), sink)
        e0, e1, e2 = jnp.exp(s0 - top), jnp.exp(s1 - top), jnp.exp(s2 - top)
        den = jnp.sum(e0 + e1 + e2, axis=1, keepdims=True) + jnp.exp(sink - top)
        ee = jnp.concatenate([e0.astype(BF16), e1.astype(BF16), e2.astype(BF16)], axis=1)
        o = jnp.dot(ee, kv[:, 64:128], preferred_element_type=F32) / den
        A[t, blk(j), :] = jnp.concatenate([o[0:BLK], o[BLK : 2 * BLK]], axis=1).astype(BF16)

    def weights_out():
        for i, half in enumerate((oa_h, or_h)):
            for d in range(1, 8):
                to = (t + d) % 8
                cols = pl.ds(pl.multiple_of(to * ocw, 128), ocw)
                put(half.at[mine, cols], WO.at[i, t, mine, :], w1_s.at[i, d], w1_r.at[i, d], (s, to)).start()

    def on(k):
        pass_on(k)
        if k + AHEAD < nb:
            own(k + AHEAD)

    on(0)
    on(1)
    on(2)
    on(3)
    project_near(0)
    on(4)
    project_near(1)
    pass_last(0)
    on(5)
    pass_last(1)
    on(6)
    project(0)
    halo_down.start()
    pass_last(2)
    on(7)
    weights_out()
    pass_last(3)
    project_near(2)
    project(1)
    pass_last(4)
    pass_last(5)
    project_near(3)
    attend(1)
    pass_last(6)
    project(2)
    pass_last(7)
    attend(2)
    attend(3)
    a_own(1)
    project(3)
    halo_up.start()

    f = jnp.zeros((64, RV), F32)
    g = jnp.zeros((64, RV), F32)
    for b in range(nb):
        SL[b, 0:64, :] = f.astype(BF16)
        f = jnp.exp(bl8[b : b + 1, :]) * f + TT[b, 0:64, :]
        e = nb - 1 - b
        SL[e, 64:128, :] = g.astype(BF16)
        g = jnp.exp(bl8[e : e + 1, :]) * g + TT[e, 64:128, :]
    XS[x, 0:64, :] = f.astype(BF16)
    XS[x, 64:128, :] = g.astype(BF16)
    for d in range(1, nx):
        put(XS.at[x], XS.at[x], sx_s.at[d], sx_r.at[d], (z * nx + (x + d) % nx, t)).start()

    for d in range(1, nx):
        o = (x + nx - d) % nx
        put(DX.at[o], DX.at[o], dx_s.at[d], dx_r.at[d], (s, sib)).wait_recv()
    total = DX[0]
    for i in range(1, nx):
        total = total + DX[i]
    DZ[z] = total
    for d in range(1, nz):
        put(DZ.at[z], DZ.at[z], dz_s.at[d], dz_r.at[d], (((z + d) % nz) * nx + x, t)).start()

    attend(4)
    attend(5)
    a_own(2)
    halo_down.wait_recv()
    attend(6)
    attend(7)
    a_own(3)

    xr, xl = z * nx + (x + 1) % nx, z * nx + (x + nx - 1) % nx

    def quarter_of(o):
        return pl.ds(pl.multiple_of(((x + o + nx) % nx) * quarter, quarter), quarter)

    def w2_own(i):
        for d in range(1, 8):
            ref = WO.at[i, (t + 8 - d) % 8, mine, :]
            put(ref, ref, w1_s.at[i, d], w1_r.at[i, d], (s, sib)).wait_recv()
        ref = WO.at[i, :, mine, :]
        put(ref, ref, w2_s.at[i, 0], w2_r.at[i, 0], (xr, t)).start()
        put(ref, ref, w2_s.at[i, 1], w2_r.at[i, 1], (xl, t)).start()

    def w2_pass(i):
        from_left = WO.at[i, :, quarter_of(-1), :]
        from_right = WO.at[i, :, quarter_of(1), :]
        put(from_left, from_left, w2_s.at[i, 0], w2_r.at[i, 0], (xr, t)).wait_recv()
        half = WO.at[i, 0:4, quarter_of(-1), :]
        put(half, half, w2_s.at[i, 2], w2_r.at[i, 2], (xr, t)).start()
        put(from_right, from_right, w2_s.at[i, 1], w2_r.at[i, 1], (xl, t)).wait_recv()
        half = WO.at[i, 4:8, quarter_of(1), :]
        put(half, half, w2_s.at[i, 3], w2_r.at[i, 3], (xl, t)).start()

    def w2_done(i):
        half = WO.at[i, 0:4, quarter_of(2), :]
        put(half, half, w2_s.at[i, 2], w2_r.at[i, 2], (xr, t)).wait_recv()
        half = WO.at[i, 4:8, quarter_of(2), :]
        put(half, half, w2_s.at[i, 3], w2_r.at[i, 3], (xl, t)).wait_recv()

    def w2_sent(i):
        ref = WO.at[i, :, mine, :]
        half = WO.at[i, 0:4, mine, :]
        put(ref, ref, w2_s.at[i, 0], w2_r.at[i, 0], (xr, t)).wait_send()
        put(ref, ref, w2_s.at[i, 1], w2_r.at[i, 1], (xl, t)).wait_send()
        put(half, half, w2_s.at[i, 2], w2_r.at[i, 2], (xr, t)).wait_send()
        put(half, half, w2_s.at[i, 3], w2_r.at[i, 3], (xl, t)).wait_send()

    w2_own(0)
    w2_own(1)

    def inside(j):
        cc = column(j)
        cr = crow[pl.ds(j, 1), :]
        qk = QR[blk(j), :]
        sc = lax.dot_general(qk[:, 0:64], qk[:, 64:128], NT, preferred_element_type=F32)
        w = (sc * jnp.exp(-jnp.abs(cc - cr))).astype(BF16)
        RL[blk(j), :] = jnp.dot(w, V[blk(j), :], preferred_element_type=F32) + jnp.dot(
            QB[blk(j), :], SL[j], preferred_element_type=F32
        )
        gate = G[blk(j), :].astype(F32)
        SG[blk(j), :] = gate / (1.0 + jnp.exp(-gate))

    def inside_two(m, carry):
        inside(2 * m)
        inside(2 * m + 1)
        return carry

    lax.fori_loop(0, na, inside_two, 0)

    a_pass(1)

    for d in range(1, nx):
        o = (x + nx - d) % nx
        put(XS.at[o], XS.at[o], sx_s.at[d], sx_r.at[d], (s, sib)).wait_recv()
    ex = [jnp.exp(DX[i][0:1, :]) for i in range(nx)]
    fx = jnp.zeros((64, RV), F32)
    gx = jnp.zeros((64, RV), F32)
    fall = jnp.zeros((64, RV), F32)
    gall = jnp.zeros((64, RV), F32)
    dfx = jnp.zeros((1, RV), F32)
    dgx = jnp.zeros((1, RV), F32)
    for i in range(nx):
        term = XS[i, 0:64, :].astype(F32)
        fx = jnp.where(i < x, ex[i] * fx + term, fx)
        dfx = jnp.where(i < x, dfx + DX[i][0:1, :], dfx)
        fall = ex[i] * fall + term
        o = nx - 1 - i
        term = XS[o, 64:128, :].astype(F32)
        gx = jnp.where(o > x, ex[o] * gx + term, gx)
        dgx = jnp.where(o > x, dgx + DX[o][0:1, :], dgx)
        gall = ex[o] * gall + term
    ZG[0] = fall.astype(BF16)
    ZG[1] = gall.astype(BF16)
    ZS[z] = jnp.zeros((64, RV), BF16)
    for d in range(1, nz):
        put(ZG.at[(z + d) // nz], ZS.at[z], sz_s.at[d], sz_r.at[d], (((z + d) % nz) * nx + x, t)).start()

    halo_up.wait_recv()
    attend(0)
    a_own(0)

    for k in range(2, na):
        a_pass(k)

    def drain(k, carry):
        sent(k)
        return carry

    lax.fori_loop(0, nb, drain, 0)
    for i in range(2):
        for d in range(1, 8):
            put(oa_h.at[mine, my_cols], WO.at[i, t, mine, :], w1_s.at[i, d], w1_r.at[i, d], (s, sib)).wait_send()
    for d in range(1, nx):
        put(XS.at[x], XS.at[x], sx_s.at[d], sx_r.at[d], (s, sib)).wait_send()
        put(DX.at[x], DX.at[x], dx_s.at[d], dx_r.at[d], (s, sib)).wait_send()
    halo_up.wait_send()
    halo_down.wait_send()

    a_last(1)
    w2_pass(0)
    a_last(2)
    a_last(3)
    a_pass(0)
    w2_pass(1)

    for d in range(1, nz):
        o = (z + nz - d) % nz
        put(DZ.at[o], DZ.at[o], dz_s.at[d], dz_r.at[d], (s, sib)).wait_recv()
        put(ZS.at[o], ZS.at[o], sz_s.at[d], sz_r.at[d], (s, sib)).wait_recv()
    fz = init[0:64, :]
    gz = init[64:128, :]
    for i in range(nz):
        term = ZS[i].astype(F32)
        fz = jnp.where(i < z, jnp.exp(DZ[i][0:1, :]) * fz + term, fz)
        o = nz - 1 - i
        term = ZS[o].astype(F32)
        gz = jnp.where(o > z, jnp.exp(DZ[o][0:1, :]) * gz + term, gz)
    ST = jnp.concatenate([fx + jnp.exp(dfx) * fz, gx + jnp.exp(dgx) * gz], axis=0).astype(BF16)

    def big(k):
        return pl.ds(pl.multiple_of(k * arows, arows), arows)

    def finish(k, carry):
        ret = RL[big(k), :] + jnp.dot(QX[big(k), :], carry, preferred_element_type=F32)
        cen = ret - jnp.mean(ret, axis=1, keepdims=True)
        nrm = cen * lax.rsqrt(jnp.mean(cen * cen, axis=1, keepdims=True) + NORM_EPS)
        R[t, big(k), :] = (SG[big(k), :] * nrm).astype(BF16)
        r_own(2 * k)
        r_own(2 * k + 1)
        return carry

    lax.fori_loop(0, na, finish, ST)

    def out_att(k):
        lhs = jnp.concatenate([A[b, big(k), :] for b in range(8)], axis=1)
        OA[big(k), :] = jnp.dot(lhs, WO[0].reshape(8 * BLK, ocw), preferred_element_type=F32)

    def out_ret(k):
        r_arrived(2 * k)
        r_arrived(2 * k + 1)
        lhs = jnp.concatenate([R[b, big(k), :] for b in range(8)], axis=1)
        acc = OA[big(k), :] + jnp.dot(lhs, WO[1].reshape(8 * BLK, ocw), preferred_element_type=F32)
        OUT[big(k), :] = acc.astype(BF16)
        pltpu.make_async_copy(OUT.at[big(k), :], out_h.at[big(k), :], lsem.at[14 + k]).start()

    w2_done(0)
    for k in range(1, na):
        a_arrived(k)
        out_att(k)
    for k in range(nb):
        r_pass(k)
        if k == 1:
            a_last(0)
    a_arrived(0)
    out_att(0)
    for k in range(nb // 2):
        r_last(k)
    w2_done(1)
    for k in range(na):
        a_sent(k)
    for i in range(2):
        w2_sent(i)
    for d in range(1, nz):
        put(ZG.at[0], ZS.at[z], sz_s.at[d], sz_r.at[d], (s, sib)).wait_send()
        put(DZ.at[z], DZ.at[z], dz_s.at[d], dz_r.at[d], (s, sib)).wait_send()
    out_ret(0)
    r_last(4)
    r_last(5)
    out_ret(1)
    r_last(6)
    r_last(7)
    out_ret(2)
    for k in range(nb // 2):
        r_sent(k)
    out_ret(3)

    for k in range(nb // 2, nb):
        r_sent(k)
    for k in range(na):
        pltpu.make_async_copy(OUT.at[big(k), :], out_h.at[big(k), :], lsem.at[14 + k]).wait()


def body(tokens, norm_gain, att_query, att_key, att_value, ret_query, ret_key, ret_value, ret_gate, att_sink, decay_log, init_state,
         out_att, out_ret, *, n_sp):
    rows, cw = tokens.shape
    width = 8 * cw
    ocw = out_att.shape[1] // 8
    nb, na = rows // BLK, rows // (2 * BLK)
    nx = 4
    nz = n_sp // nx
    inverse = (np.float64(ROPE_BASE) ** (-2.0 * (np.arange(128) % 32) / 64)).astype(np.float32)[None, :]
    dma = pltpu.SemaphoreType.DMA
    hbm = pl.BlockSpec(memory_space=pltpu.HBM)
    specs = [hbm] * 15
    specs[9] = pl.BlockSpec(memory_space=pltpu.SMEM)
    vm = pltpu.VMEM
    scratch = [
        vm((8, rows, cw), BF16), vm((width, 640), BF16), vm((256, width), BF16), vm((1, width), F32), vm((1, rows), F32),
        vm((128, 128), F32), vm((1, 128), F32),
        vm((rows, 128), BF16), vm((rows + 2 * BLK, 128), BF16), vm((rows, 128), BF16), vm((rows, 128), BF16), vm((rows, 128), F32),
        vm((rows, 128), F32), vm((rows, 128), F32), vm((2, 2 * BLK, 640), F32), vm((2, 2 * BLK, 128), F32), vm((rows, 128), BF16), vm((rows, 128), BF16), vm((rows, 128), BF16), vm((rows, 128), F32),
        vm((nb, 128, 128), F32), vm((nb, 128, 128), BF16),
        vm((8, rows, 128), BF16), vm((8, rows, 128), BF16), vm((2, 8, 128, ocw), BF16), vm((rows, ocw), F32), vm((rows, ocw), BF16),
        vm((nx, 128, 128), BF16), vm((2, 64, 128), BF16), vm((nz, 64, 128), BF16), vm((nx, 8, 128), F32), vm((nz, 8, 128), F32),
        vm((nb, 128), F32), vm((nb, 128), F32), vm((nb, 128), F32),
        dma((14 + nb,)), dma((7, nb)), dma((7, nb)), dma((7, na)), dma((7, na)), dma((7, nb)), dma((7, nb)),
        dma((2, 8)), dma((2, 8)), dma((2, 4)), dma((2, 4)), dma((nx,)), dma((nx,)), dma((nx,)), dma((nx,)),
        dma((max(nz, 2),)), dma((max(nz, 2),)), dma((max(nz, 2),)), dma((max(nz, 2),)), dma((2,)), dma((2,)),
    ]
    call = pl.pallas_call(
        functools.partial(kernel, n_sp, nx),
        out_shape=jax.ShapeDtypeStruct((rows, ocw), BF16),
        in_specs=specs,
        out_specs=hbm,
        scratch_shapes=scratch,
        compiler_params=pltpu.CompilerParams(collective_id=0, has_side_effects=True, vmem_limit_bytes=67_043_328),
        name="layer",
    )
    return call(
        tokens, norm_gain.reshape(1, width), att_query, att_key.T, att_value.T, ret_query.T, ret_key.T, ret_value, ret_gate,
        att_sink, decay_log, init_state.reshape(128, 128), inverse, out_att, out_ret,
    )


def solution(mesh):
    in_specs = (
        P("sp", "tp"), P(), P(None, "tp"), P(None, "tp"), P(None, "tp"), P(None, "tp"), P(None, "tp"), P(None, "tp"), P(None, "tp"),
        P("tp"), P("tp", "sp"), P(None, "tp", None, None), P("tp", None), P("tp", None),
    )
    return jax.shard_map(
        functools.partial(body, n_sp=mesh.shape["sp"]), mesh=mesh, in_specs=in_specs, out_specs=P("sp", "tp"), check_vma=False
    )
```

```python
import functools

import jax
import jax.numpy as jnp
import numpy as np
from jax import lax
from jax.experimental import pallas as pl
from jax.experimental.pallas import tpu as pltpu
from jax.sharding import PartitionSpec as P

HD = 64
RV = 128
BLK = 128
NORM_EPS = 1e-06
ROPE_BASE = 10000.0
MESH = pl.DeviceIdType.MESH
F32 = jnp.float32
BF16 = jnp.bfloat16
NT = (((1,), (1,)), ((), ()))
TN = (((0,), (0,)), ((), ()))
AHEAD = 5

L1, R1, OPP, SIB = 0, 1, 2, 3


def kernel(n_sp, nx, tok_h, gain_h, wq_h, wk_h, wv_h, wrq_h, wrk_h, wrv_h, wrg_h, sink_ref, dec_h, init_h, inv_h, oa_h, or_h,
           out_h,
           X, W1, W2, gain, dec, init, inv, Q, KV, V, G, SG, COS, SIN, ACC, SQ, QR, QB, QX, RL, TT, SL, A, R, WO, OA, OUT,
           XS, ZG, ZS, DX, DZ, crow, bl8, pre8,
           lsem, xs_s, xs_r, xn_r, xf_r, as_s, as_r, an_r, af_r, rs_s, rs_r, rn_r, rf_r, w1_s, w1_r, w2_s, w2_r, sx_s, sx_r, dx_s, dx_r, sz_s, sz_r, dz_s, dz_r,
           h_s, h_r):
    rows, cw = tok_h.shape
    nb = rows // BLK
    arows = 2 * BLK
    na = rows // arows
    width = 8 * cw
    ocw = OUT.shape[1]
    nz = n_sp // nx
    quarter = BLK // nx
    s, t = lax.axis_index("sp"), lax.axis_index("tp")
    z, x = s // nx, s % nx
    y, c = t // 2, t % 2
    right = 2 * ((y + 1) % 4) + c
    left = 2 * ((y + 3) % 4) + c
    opp = 2 * ((y + 2) % 4) + c
    sib = 2 * y + (1 - c)
    sib_right = 2 * ((y + 1) % 4) + 1 - c
    sib_left = 2 * ((y + 3) % 4) + 1 - c
    sib_opp = 2 * ((y + 2) % 4) + 1 - c
    up, down = (s + 1) % n_sp, (s + n_sp - 1) % n_sp

    loads = [
        (dec_h, dec), (tok_h, X.at[t]), (gain_h, gain), (inv_h, inv), (init_h, init),
        (wq_h, W1.at[:, 0:128]), (wrv_h, W1.at[:, 128:256]), (wrg_h, W1.at[:, 256:384]),
        (wk_h, W2.at[0:64]), (wv_h, W2.at[64:128]), (wrq_h, W2.at[128:192]), (wrk_h, W2.at[192:256]),
    ]
    mine = pl.ds(pl.multiple_of(x * quarter, quarter), quarter)
    my_cols = pl.ds(pl.multiple_of(t * ocw, 128), ocw)
    loads += [(oa_h.at[mine, my_cols], WO.at[0, t, mine, :]), (or_h.at[mine, my_cols], WO.at[1, t, mine, :])]
    copies = [pltpu.make_async_copy(a, b, lsem.at[i]) for i, (a, b) in enumerate(loads)]
    for cp in copies:
        cp.start()

    barrier = pltpu.get_barrier_semaphore()
    partners = [(s, (t + d) % 8) for d in range(1, 8)]
    partners += [(z * nx + (x + d) % nx, t) for d in range(1, nx)]
    partners += [(((z + d) % nz) * nx + x, t) for d in range(1, nz)]
    has_up, has_down = 1 - (s + 1) // n_sp, (s + n_sp - 1) // n_sp
    for p in reversed(partners):
        pl.semaphore_signal(barrier, inc=1, device_id=p, device_id_type=MESH)

    @pl.when(has_up == 1)
    def _():
        pl.semaphore_signal(barrier, inc=1, device_id=(up, t), device_id_type=MESH)

    @pl.when(has_down == 1)
    def _():
        pl.semaphore_signal(barrier, inc=1, device_id=(down, t), device_id_type=MESH)

    copies[0].wait()
    for b in range(nb):
        crow[b : b + 1, :] = dec[:, b * BLK : (b + 1) * BLK]
    cum = crow[...]
    lane = lax.broadcasted_iota(jnp.int32, (nb, BLK), 1)
    for sh in (1, 2, 4, 8, 16, 32, 64):
        cum = cum + jnp.where(lane >= sh, pltpu.roll(cum, sh, 1), 0.0)
    crow[...] = cum
    bl8[...] = jnp.broadcast_to(cum[:, BLK - 1 : BLK], (nb, BLK))
    run = jnp.zeros((1, BLK), F32)
    for b in range(nb):
        pre8[b : b + 1, :] = run
        run = run + bl8[b : b + 1, :]
    tot = run
    DX[x] = jnp.broadcast_to(tot, (8, BLK))
    for i in range(1, 5):
        copies[i].wait()

    pl.semaphore_wait(barrier, len(partners) + has_up + has_down)

    def put(src, dst, send, recv, dev):
        return pltpu.make_async_remote_copy(src_ref=src, dst_ref=dst, send_sem=send, recv_sem=recv, device_id=dev, device_id_type=MESH)

    def gather(buf, n_rows, ss, rs, near, far):
        group = 2 * BLK // n_rows

        def part(b, k):
            return buf.at[b, pl.ds(pl.multiple_of(k * n_rows, n_rows), n_rows), :]

        def hop(b, k, send, recv, tp):
            ref = part(b, k)
            return put(ref, ref, ss.at[send], recv, (s, tp))

        def own(k):
            hop(t, k, 0, rs.at[L1, k], right).start()
            hop(t, k, 1, rs.at[R1, k], left).start()
            hop(t, k, 2, near.at[k // group], sib).start()

        def pass_on(k):
            hop(left, k, 3, rs.at[L1, k], right).wait_recv()
            if k % 2 == 0:
                hop(left, k, 6, rs.at[OPP, k], right).start()
            hop(left, k, 3, near.at[k // group], sib).start()
            hop(right, k, 4, rs.at[R1, k], left).wait_recv()
            if k % 2 == 1:
                hop(right, k, 6, rs.at[OPP, k], left).start()
            hop(right, k, 4, near.at[k // group], sib).start()

        def pass_last(k):
            hop(opp, k, 5, rs.at[OPP, k], right).wait_recv()
            hop(opp, k, 5, far.at[k // group], sib).start()

        def two(first, blocks, m):
            return buf.at[pl.ds(first, blocks), pl.ds(pl.multiple_of(m * 2 * BLK, 2 * BLK), 2 * BLK), :]

        def arrived_near(m):
            ref = two(0, 3, m)
            put(ref, ref, ss.at[2], near.at[m], (s, sib)).wait_recv()

        def arrived_far(m):
            ref = two(0, 1, m)
            put(ref, ref, ss.at[2], far.at[m], (s, sib)).wait_recv()

        def sent():
            for i in range(7):
                put(buf.at[t], buf.at[t], ss.at[i], near.at[0], (s, sib)).wait_send()

        return own, pass_on, pass_last, arrived_near, arrived_far, sent

    own, pass_on, pass_last, arrived_near, arrived_far, sent = gather(X, BLK, xs_s, xs_r, xn_r, xf_r)
    a_own, a_pass, a_last, a_near, a_far, a_sent = gather(A, arows, as_s, as_r, an_r, af_r)
    r_own, r_pass, r_last, r_near, r_far, r_sent = gather(R, BLK, rs_s, rs_r, rn_r, rf_r)

    for k in range(AHEAD):
        own(k)
    for d in range(1, nx):
        put(DX.at[x], DX.at[x], dx_s.at[0], dx_r.at[0], (z * nx + (x + d) % nx, t)).start()

    lane_b = lax.broadcasted_iota(jnp.int32, (BLK, BLK), 1)
    row_b = lax.broadcasted_iota(jnp.int32, (BLK, BLK), 0)
    low = lane_b < 64

    def blk(j):
        return pl.ds(pl.multiple_of(j * BLK, BLK), BLK)

    def column(j):
        row = jnp.broadcast_to(crow[pl.ds(j, 1), :], (BLK, BLK))
        return jnp.sum(jnp.where(lane_b == row_b, row, 0.0), axis=1, keepdims=True)

    def tables(j, carry):
        pos = (s * rows + j * BLK + row_b).astype(F32)
        angle = pos * inv[...]
        scale = jnp.where(low, 1.0, 64**-0.5).astype(F32)
        COS[blk(j), :] = jnp.cos(angle) * scale
        SIN[blk(j), :] = jnp.sin(angle) * jnp.where(lane_b % 64 < 32, -scale, scale)
        return carry

    def pair(m):
        return pl.ds(pl.multiple_of(m * 2 * BLK, 2 * BLK), 2 * BLK)

    def sums(m, acc, squares, blocks):
        for b in blocks:
            cols = pl.ds(pl.multiple_of(b * cw, cw), cw)
            xf = X[b, pair(m), :].astype(F32)
            sq = xf * xf
            squares = squares + sum(sq[:, i : i + 128] for i in range(0, cw, 128))
            acc = acc + jnp.dot((xf * gain[:, cols]).astype(BF16), W1[cols, :], preferred_element_type=F32)
        return acc, squares

    def project_near(m):
        arrived_near(m)
        zero = jnp.zeros((2 * BLK, 640), F32), jnp.zeros((2 * BLK, 128), F32)
        ACC[m], SQ[m] = sums(m, *zero, (t, sib, left, right, sib_left, sib_right))

    def project(m):
        two = pair(m)
        arrived_far(m)
        acc, squares = sums(m, ACC[m], SQ[m], (opp, sib_opp))
        inv_rms = lax.rsqrt(jnp.sum(squares, axis=1, keepdims=True) / width + NORM_EPS)
        p = (acc * inv_rms).astype(BF16)
        Q[two, :] = p[:, 0:128]
        V[two, :] = p[:, 128:256]
        G[two, :] = p[:, 256:384]
        KV[pl.ds(pl.multiple_of(m * 2 * BLK + BLK, BLK), 2 * BLK), :] = p[:, 384:512]
        for h in range(2):
            j = 2 * m + h
            cosine, sine, cc = COS[blk(j), :], SIN[blk(j), :], column(j)
            bl = bl8[pl.ds(j, 1), :]
            pre = pre8[pl.ds(j, 1), :]
            rqk = p[h * BLK : (h + 1) * BLK, 512:640].astype(F32)
            swapped = jnp.where(lane_b % 64 < 32, pltpu.roll(rqk, 96, 1), pltpu.roll(rqk, 32, 1))
            rot = rqk * cosine + swapped * sine
            QR[blk(j), :] = rot.astype(BF16)
            other = pltpu.roll(rot, 64, 1)
            qq = jnp.where(low, rot, other)
            kk = jnp.where(low, other, rot)
            to_end = jnp.exp(bl - cc)
            to_here = jnp.exp(jnp.broadcast_to(cc, (BLK, BLK)))
            QB[blk(j), :] = (qq * jnp.where(low, to_here, to_end)).astype(BF16)
            full = cc + pre
            QX[blk(j), :] = (qq * jnp.exp(jnp.where(low, full, tot - full))).astype(BF16)
            kw = (kk * jnp.where(low, to_end, to_here)).astype(BF16)
            v = p[h * BLK : (h + 1) * BLK, 128:256]
            TT[j] = lax.dot_general(kw, v, TN, preferred_element_type=F32)

    for i in range(5, 14):
        copies[i].wait()
    for b in range(8):
        W1[b * cw : (b + 1) * cw, 384:640] = W2[:, b * cw : (b + 1) * cw].T
    lax.fori_loop(0, nb, tables, 0)

    halo_up = put(KV.at[pl.ds(rows, BLK), :], KV.at[pl.ds(0, BLK), :], h_s.at[0], h_r.at[0], (up, t))
    halo_down = put(KV.at[pl.ds(BLK, BLK), :], KV.at[pl.ds(rows + BLK, BLK), :], h_s.at[1], h_r.at[1], (down, t))

    row_q = lax.broadcasted_iota(jnp.int32, (2 * BLK, BLK), 0) % BLK
    lane_q = lax.broadcasted_iota(jnp.int32, (2 * BLK, BLK), 1)
    sink = jnp.where(lax.broadcasted_iota(jnp.int32, (2 * BLK, 1), 0) < BLK, sink_ref[0], sink_ref[1])

    def attend(j):
        q = Q[blk(j), :]
        q2 = jnp.concatenate([q[:, 0:64], q[:, 64:128]], axis=0)
        kv = KV[pl.ds(pl.multiple_of(j * BLK, BLK), 3 * BLK), :]
        sc = lax.dot_general(q2, kv[:, 0:64], NT, preferred_element_type=F32) * HD**-0.5
        first = jnp.where(s * nb + j == 0, BLK, 0)
        last = jnp.where(s * nb + j == n_sp * nb - 1, BLK, 0)
        s0 = jnp.where(lane_q - first >= row_q, sc[:, 0:128], -jnp.inf)
        s1 = sc[:, 128:256]
        s2 = jnp.where(lane_q + last <= row_q, sc[:, 256:384], -jnp.inf)
        top = jnp.maximum(jnp.max(jnp.maximum(jnp.maximum(s0, s1), s2), axis=1, keepdims=True), sink)
        e0, e1, e2 = jnp.exp(s0 - top), jnp.exp(s1 - top), jnp.exp(s2 - top)
        den = jnp.sum(e0 + e1 + e2, axis=1, keepdims=True) + jnp.exp(sink - top)
        ee = jnp.concatenate([e0.astype(BF16), e1.astype(BF16), e2.astype(BF16)], axis=1)
        o = jnp.dot(ee, kv[:, 64:128], preferred_element_type=F32) / den
        A[t, blk(j), :] = jnp.concatenate([o[0:BLK], o[BLK : 2 * BLK]], axis=1).astype(BF16)

    def weights_out():
        for i, half in enumerate((oa_h, or_h)):
            for d in range(1, 8):
                to = (t + d) % 8
                cols = pl.ds(pl.multiple_of(to * ocw, 128), ocw)
                put(half.at[mine, cols], WO.at[i, t, mine, :], w1_s.at[i], w1_r.at[i], (s, to)).start()

    def on(k):
        pass_on(k)
        if k + AHEAD < nb:
            own(k + AHEAD)

    @pl.when(has_down == 0)
    def _():
        KV[0:BLK, :] = jnp.zeros((BLK, 128), BF16)

    @pl.when(has_up == 0)
    def _():
        KV[rows + BLK : rows + 2 * BLK, :] = jnp.zeros((BLK, 128), BF16)

    on(0)
    on(1)
    on(2)
    on(3)
    project_near(0)
    on(4)
    project_near(1)
    pass_last(0)
    on(5)
    pass_last(1)
    project_near(2)
    on(6)
    project(0)

    @pl.when(has_down == 1)
    def _():
        halo_down.start()

    pass_last(2)
    on(7)
    weights_out()
    pass_last(3)
    project(1)
    pass_last(4)
    pass_last(5)
    project_near(3)
    attend(1)
    pass_last(6)
    project(2)
    pass_last(7)
    project(3)

    f = jnp.zeros((64, RV), F32)
    g = jnp.zeros((64, RV), F32)
    for b in range(nb):
        SL[b, 0:64, :] = f.astype(BF16)
        f = jnp.exp(bl8[b : b + 1, :]) * f + TT[b, 0:64, :]
        e = nb - 1 - b
        SL[e, 64:128, :] = g.astype(BF16)
        g = jnp.exp(bl8[e : e + 1, :]) * g + TT[e, 64:128, :]
    XS[x, 0:64, :] = f.astype(BF16)
    XS[x, 64:128, :] = g.astype(BF16)
    for d in sorted(range(1, nx), key=lambda d: -min(d, nx - d)):
        put(XS.at[x], XS.at[x], sx_s.at[0], sx_r.at[0], (z * nx + (x + d) % nx, t)).start()

    @pl.when(has_up == 1)
    def _():
        halo_up.start()


    put(DX.at[0 : nx - 1], DX.at[0 : nx - 1], dx_s.at[0], dx_r.at[0], (s, sib)).wait_recv()
    total = DX[0]
    for i in range(1, nx):
        total = total + DX[i]
    DZ[z] = total
    for d in range(1, nz):
        put(DZ.at[z], DZ.at[z], dz_s.at[0], dz_r.at[0], (((z + d) % nz) * nx + x, t)).start()

    attend(2)
    attend(3)
    a_own(1)
    attend(4)
    attend(5)
    a_own(2)

    @pl.when(has_up == 1)
    def _():
        halo_down.wait_recv()

    attend(6)
    attend(7)
    a_own(3)

    xr, xl = z * nx + (x + 1) % nx, z * nx + (x + nx - 1) % nx

    def quarter_of(o):
        return pl.ds(pl.multiple_of(((x + o + nx) % nx) * quarter, quarter), quarter)

    def w2_own(i):
        ref = WO.at[i, 0:7, mine, :]
        put(ref, ref, w1_s.at[i], w1_r.at[i], (s, sib)).wait_recv()
        ref = WO.at[i, :, mine, :]
        put(ref, ref, w2_s.at[i, 0], w2_r.at[i, 0], (xr, t)).start()
        put(ref, ref, w2_s.at[i, 1], w2_r.at[i, 1], (xl, t)).start()

    def w2_pass(i):
        from_left = WO.at[i, :, quarter_of(-1), :]
        from_right = WO.at[i, :, quarter_of(1), :]
        put(from_left, from_left, w2_s.at[i, 0], w2_r.at[i, 0], (xr, t)).wait_recv()
        half = WO.at[i, 0:4, quarter_of(-1), :]
        put(half, half, w2_s.at[i, 2], w2_r.at[i, 2], (xr, t)).start()
        put(from_right, from_right, w2_s.at[i, 1], w2_r.at[i, 1], (xl, t)).wait_recv()
        half = WO.at[i, 4:8, quarter_of(1), :]
        put(half, half, w2_s.at[i, 3], w2_r.at[i, 3], (xl, t)).start()

    def w2_done(i):
        half = WO.at[i, 0:4, quarter_of(2), :]
        put(half, half, w2_s.at[i, 2], w2_r.at[i, 2], (xr, t)).wait_recv()
        half = WO.at[i, 4:8, quarter_of(2), :]
        put(half, half, w2_s.at[i, 3], w2_r.at[i, 3], (xl, t)).wait_recv()

    def w2_sent(i):
        ref = WO.at[i, :, mine, :]
        half = WO.at[i, 0:4, mine, :]
        put(ref, ref, w2_s.at[i, 0], w2_r.at[i, 0], (xr, t)).wait_send()
        put(ref, ref, w2_s.at[i, 1], w2_r.at[i, 1], (xl, t)).wait_send()
        put(half, half, w2_s.at[i, 2], w2_r.at[i, 2], (xr, t)).wait_send()
        put(half, half, w2_s.at[i, 3], w2_r.at[i, 3], (xl, t)).wait_send()

    put(XS.at[0 : nx - 1], XS.at[0 : nx - 1], sx_s.at[0], sx_r.at[0], (s, sib)).wait_recv()
    ex = [jnp.exp(DX[i][0:1, :]) for i in range(nx)]
    fx = jnp.zeros((64, RV), F32)
    gx = jnp.zeros((64, RV), F32)
    fall = jnp.zeros((64, RV), F32)
    gall = jnp.zeros((64, RV), F32)
    dfx = jnp.zeros((1, RV), F32)
    dgx = jnp.zeros((1, RV), F32)
    for i in range(nx):
        term = XS[i, 0:64, :].astype(F32)
        fx = jnp.where(i < x, ex[i] * fx + term, fx)
        dfx = jnp.where(i < x, dfx + DX[i][0:1, :], dfx)
        fall = ex[i] * fall + term
        o = nx - 1 - i
        term = XS[o, 64:128, :].astype(F32)
        gx = jnp.where(o > x, ex[o] * gx + term, gx)
        dgx = jnp.where(o > x, dgx + DX[o][0:1, :], dgx)
        gall = ex[o] * gall + term
    ZG[0] = fall.astype(BF16)
    ZG[1] = gall.astype(BF16)
    ZS[z] = jnp.zeros((64, RV), BF16)
    for d in sorted(range(1, nz), key=lambda d: -min(d, nz - d)):
        put(ZG.at[(z + d) // nz], ZS.at[z], sz_s.at[0], sz_r.at[0], (((z + d) % nz) * nx + x, t)).start()

    w2_own(0)
    w2_own(1)

    @pl.when(has_down == 1)
    def _():
        halo_up.wait_recv()

    attend(0)
    a_own(0)

    def inside(j):
        cc = column(j)
        cr = crow[pl.ds(j, 1), :]
        qk = QR[blk(j), :]
        sc = lax.dot_general(qk[:, 0:64], qk[:, 64:128], NT, preferred_element_type=F32)
        w = (sc * jnp.exp(-jnp.abs(cc - cr))).astype(BF16)
        RL[blk(j), :] = jnp.dot(w, V[blk(j), :], preferred_element_type=F32) + jnp.dot(
            QB[blk(j), :], SL[j], preferred_element_type=F32
        )
        gate = G[blk(j), :].astype(F32)
        SG[blk(j), :] = gate / (1.0 + jnp.exp(-gate))

    def inside_two(m, carry):
        inside(2 * m)
        inside(2 * m + 1)
        return carry


    a_pass(1)
    lax.fori_loop(0, na // 2, inside_two, 0)
    a_pass(2)
    lax.fori_loop(na // 2, na, inside_two, 0)
    a_pass(3)

    sent()
    for i in range(2):
        ref = WO.at[i, 0:7, mine, :]
        put(ref, ref, w1_s.at[i], w1_r.at[i], (s, sib)).wait_send()
    put(XS.at[0 : nx - 1], XS.at[0 : nx - 1], sx_s.at[0], sx_r.at[0], (s, sib)).wait_send()
    put(DX.at[0 : nx - 1], DX.at[0 : nx - 1], dx_s.at[0], dx_r.at[0], (s, sib)).wait_send()

    @pl.when(has_up == 1)
    def _():
        halo_up.wait_send()

    @pl.when(has_down == 1)
    def _():
        halo_down.wait_send()


    a_last(1)
    w2_pass(0)
    a_last(2)
    a_last(3)
    a_pass(0)
    w2_pass(1)

    if nz > 1:
        put(DZ.at[0 : nz - 1], DZ.at[0 : nz - 1], dz_s.at[0], dz_r.at[0], (s, sib)).wait_recv()
        put(ZS.at[0 : nz - 1], ZS.at[0 : nz - 1], sz_s.at[0], sz_r.at[0], (s, sib)).wait_recv()
    fz = init[0:64, :]
    gz = init[64:128, :]
    for i in range(nz):
        term = ZS[i].astype(F32)
        fz = jnp.where(i < z, jnp.exp(DZ[i][0:1, :]) * fz + term, fz)
        o = nz - 1 - i
        term = ZS[o].astype(F32)
        gz = jnp.where(o > z, jnp.exp(DZ[o][0:1, :]) * gz + term, gz)
    ST = jnp.concatenate([fx + jnp.exp(dfx) * fz, gx + jnp.exp(dgx) * gz], axis=0).astype(BF16)

    def big(k):
        return pl.ds(pl.multiple_of(k * arows, arows), arows)

    def finish(k, carry):
        ret = RL[big(k), :] + jnp.dot(QX[big(k), :], carry, preferred_element_type=F32)
        cen = ret - jnp.mean(ret, axis=1, keepdims=True)
        nrm = cen * lax.rsqrt(jnp.mean(cen * cen, axis=1, keepdims=True) + NORM_EPS)
        R[t, big(k), :] = (SG[big(k), :] * nrm).astype(BF16)
        r_own(2 * k)
        r_own(2 * k + 1)
        return carry

    lax.fori_loop(0, na, finish, ST)

    def out_att(k):
        lhs = jnp.concatenate([A[b, big(k), :] for b in range(8)], axis=1)
        OA[big(k), :] = jnp.dot(lhs, WO[0].reshape(8 * BLK, ocw), preferred_element_type=F32)

    def out_ret(k):
        r_near(k)
        r_far(k)
        lhs = jnp.concatenate([R[b, big(k), :] for b in range(8)], axis=1)
        acc = OA[big(k), :] + jnp.dot(lhs, WO[1].reshape(8 * BLK, ocw), preferred_element_type=F32)
        OUT[big(k), :] = acc.astype(BF16)
        pltpu.make_async_copy(OUT.at[big(k), :], out_h.at[big(k), :], lsem.at[14 + k]).start()

    for k in range(nb):
        r_pass(k)
        if k == 1:
            a_last(0)
        if k == nb // 2 - 1:
            w2_done(0)
        if nb // 2 <= k < nb - 1:
            a_near(k - nb // 2 + 1)
            a_far(k - nb // 2 + 1)
            out_att(k - nb // 2 + 1)
    a_near(0)
    a_far(0)
    out_att(0)
    for k in range(nb // 2):
        r_last(k)
    w2_done(1)
    a_sent()
    for i in range(2):
        w2_sent(i)
    if nz > 1:
        put(ZS.at[0 : nz - 1], ZS.at[0 : nz - 1], sz_s.at[0], sz_r.at[0], (s, sib)).wait_send()
        put(DZ.at[0 : nz - 1], DZ.at[0 : nz - 1], dz_s.at[0], dz_r.at[0], (s, sib)).wait_send()
    out_ret(0)
    r_last(4)
    r_last(5)
    out_ret(1)
    r_last(6)
    r_last(7)
    out_ret(2)
    out_ret(3)

    r_sent()
    for k in range(na):
        pltpu.make_async_copy(OUT.at[big(k), :], out_h.at[big(k), :], lsem.at[14 + k]).wait()


def body(tokens, norm_gain, att_query, att_key, att_value, ret_query, ret_key, ret_value, ret_gate, att_sink, decay_log, init_state,
         out_att, out_ret, *, n_sp):
    rows, cw = tokens.shape
    width = 8 * cw
    ocw = out_att.shape[1] // 8
    nb, na = rows // BLK, rows // (2 * BLK)
    nx = 4
    nz = n_sp // nx
    inverse = (np.float64(ROPE_BASE) ** (-2.0 * (np.arange(128) % 32) / 64)).astype(np.float32)[None, :]
    dma = pltpu.SemaphoreType.DMA
    hbm = pl.BlockSpec(memory_space=pltpu.HBM)
    specs = [hbm] * 15
    specs[9] = pl.BlockSpec(memory_space=pltpu.SMEM)
    vm = pltpu.VMEM
    scratch = [
        vm((8, rows, cw), BF16), vm((width, 640), BF16), vm((256, width), BF16), vm((1, width), F32), vm((1, rows), F32),
        vm((128, 128), F32), vm((1, 128), F32),
        vm((rows, 128), BF16), vm((rows + 2 * BLK, 128), BF16), vm((rows, 128), BF16), vm((rows, 128), BF16), vm((rows, 128), F32),
        vm((rows, 128), F32), vm((rows, 128), F32), vm((nb // 2, 2 * BLK, 640), F32), vm((nb // 2, 2 * BLK, 128), F32), vm((rows, 128), BF16), vm((rows, 128), BF16), vm((rows, 128), BF16), vm((rows, 128), F32),
        vm((nb, 128, 128), F32), vm((nb, 128, 128), BF16),
        vm((8, rows, 128), BF16), vm((8, rows, 128), BF16), vm((2, 8, 128, ocw), BF16), vm((rows, ocw), F32), vm((rows, ocw), BF16),
        vm((nx, 128, 128), BF16), vm((2, 64, 128), BF16), vm((nz, 64, 128), BF16), vm((nx, 8, 128), F32), vm((nz, 8, 128), F32),
        vm((nb, 128), F32), vm((nb, 128), F32), vm((nb, 128), F32),
        dma((14 + na,)), dma((7,)), dma((3, nb)), dma((na,)), dma((na,)), dma((7,)), dma((3, na)), dma((na,)), dma((na,)),
        dma((7,)), dma((3, nb)), dma((na,)), dma((na,)),
        dma((2,)), dma((2,)), dma((2, 4)), dma((2, 4)), dma((1,)), dma((1,)), dma((1,)), dma((1,)),
        dma((1,)), dma((1,)), dma((1,)), dma((1,)), dma((2,)), dma((2,)),
    ]
    call = pl.pallas_call(
        functools.partial(kernel, n_sp, nx),
        out_shape=jax.ShapeDtypeStruct((rows, ocw), BF16),
        in_specs=specs,
        out_specs=hbm,
        scratch_shapes=scratch,
        compiler_params=pltpu.CompilerParams(collective_id=0, has_side_effects=True, vmem_limit_bytes=67_043_328),
        name="layer",
    )
    return call(
        tokens, norm_gain.reshape(1, width), att_query, att_key.T, att_value.T, ret_query.T, ret_key.T, ret_value, ret_gate,
        att_sink, decay_log, init_state.reshape(128, 128), inverse, out_att, out_ret,
    )


def solution(mesh):
    in_specs = (
        P("sp", "tp"), P(), P(None, "tp"), P(None, "tp"), P(None, "tp"), P(None, "tp"), P(None, "tp"), P(None, "tp"), P(None, "tp"),
        P("tp"), P("tp", "sp"), P(None, "tp", None, None), P("tp", None), P("tp", None),
    )
    return jax.shard_map(
        functools.partial(body, n_sp=mesh.shape["sp"]), mesh=mesh, in_specs=in_specs, out_specs=P("sp", "tp"), check_vma=False
    )
```

```python
import functools

import jax
import jax.numpy as jnp
import numpy as np
from jax import lax
from jax.experimental import pallas as pl
from jax.experimental.pallas import tpu as pltpu
from jax.sharding import PartitionSpec as P

HD = 64
RV = 128
BLK = 128
NORM_EPS = 1e-06
ROPE_BASE = 10000.0
MESH = pl.DeviceIdType.MESH
F32 = jnp.float32
BF16 = jnp.bfloat16
NT = (((1,), (1,)), ((), ()))
TN = (((0,), (0,)), ((), ()))
AHEAD = 5

L1, R1, OPP, SIB = 0, 1, 2, 3


def kernel(n_sp, nx, tok_h, gain_h, wq_h, wk_h, wv_h, wrq_h, wrk_h, wrv_h, wrg_h, sink_ref, dec_h, init_h, inv_h, oa_h, or_h,
           out_h,
           X, W1, W2, gain, dec, init, inv, Q, KV, V, G, SG, COS, SIN, ACC, SQ, QR, QB, QX, RL, TT, SL, A, R, WO, OA, OUT,
           XS, ZG, ZS, DX, DZ, crow, bl8, pre8,
           lsem, xs_s, xs_r, xn_r, xf_r, as_s, as_r, an_r, af_r, rs_s, rs_r, rn_r, rf_r, w1_s, w1_r, w2_s, w2_r, sx_s, sx_r, dx_s, dx_r, sz_s, sz_r, dz_s, dz_r,
           h_s, h_r):
    rows, cw = tok_h.shape
    nb = rows // BLK
    arows = 2 * BLK
    na = rows // arows
    width = 8 * cw
    ocw = OUT.shape[1]
    nz = n_sp // nx
    quarter = BLK // nx
    s, t = lax.axis_index("sp"), lax.axis_index("tp")
    z, x = s // nx, s % nx
    y, c = t // 2, t % 2
    right = 2 * ((y + 1) % 4) + c
    left = 2 * ((y + 3) % 4) + c
    opp = 2 * ((y + 2) % 4) + c
    sib = 2 * y + (1 - c)
    sib_right = 2 * ((y + 1) % 4) + 1 - c
    sib_left = 2 * ((y + 3) % 4) + 1 - c
    sib_opp = 2 * ((y + 2) % 4) + 1 - c
    up, down = (s + 1) % n_sp, (s + n_sp - 1) % n_sp

    loads = [
        (dec_h, dec), (tok_h, X.at[t]), (gain_h, gain), (inv_h, inv), (init_h, init),
        (wq_h, W1.at[:, 0:128]), (wrv_h, W1.at[:, 128:256]), (wrg_h, W1.at[:, 256:384]),
        (wk_h, W2.at[0:64]), (wv_h, W2.at[64:128]), (wrq_h, W2.at[128:192]), (wrk_h, W2.at[192:256]),
    ]
    mine = pl.ds(pl.multiple_of(x * quarter, quarter), quarter)
    my_cols = pl.ds(pl.multiple_of(t * ocw, 128), ocw)
    loads += [(oa_h.at[mine, my_cols], WO.at[0, t, mine, :]), (or_h.at[mine, my_cols], WO.at[1, t, mine, :])]
    copies = [pltpu.make_async_copy(a, b, lsem.at[i]) for i, (a, b) in enumerate(loads)]
    for cp in copies:
        cp.start()

    barrier = pltpu.get_barrier_semaphore()
    partners = [(s, (t + d) % 8) for d in range(1, 8)]
    partners += [(z * nx + (x + d) % nx, t) for d in range(1, nx)]
    partners += [(((z + d) % nz) * nx + x, t) for d in range(1, nz)]
    has_up, has_down = 1 - (s + 1) // n_sp, (s + n_sp - 1) // n_sp
    for p in reversed(partners):
        pl.semaphore_signal(barrier, inc=1, device_id=p, device_id_type=MESH)

    @pl.when(has_up == 1)
    def _():
        pl.semaphore_signal(barrier, inc=1, device_id=(up, t), device_id_type=MESH)

    @pl.when(has_down == 1)
    def _():
        pl.semaphore_signal(barrier, inc=1, device_id=(down, t), device_id_type=MESH)

    copies[0].wait()
    for b in range(nb):
        crow[b : b + 1, :] = dec[:, b * BLK : (b + 1) * BLK]
    cum = crow[...]
    lane = lax.broadcasted_iota(jnp.int32, (nb, BLK), 1)
    for sh in (1, 2, 4, 8, 16, 32, 64):
        cum = cum + jnp.where(lane >= sh, pltpu.roll(cum, sh, 1), 0.0)
    crow[...] = cum
    bl8[...] = jnp.broadcast_to(cum[:, BLK - 1 : BLK], (nb, BLK))
    run = jnp.zeros((1, BLK), F32)
    for b in range(nb):
        pre8[b : b + 1, :] = run
        run = run + bl8[b : b + 1, :]
    tot = run
    DX[x] = jnp.broadcast_to(tot, (8, BLK))
    for i in range(1, 5):
        copies[i].wait()

    pl.semaphore_wait(barrier, len(partners) + has_up + has_down)

    def put(src, dst, send, recv, dev):
        return pltpu.make_async_remote_copy(src_ref=src, dst_ref=dst, send_sem=send, recv_sem=recv, device_id=dev, device_id_type=MESH)

    def gather(buf, n_rows, ss, rs, near, far):
        group = 2 * BLK // n_rows

        def part(b, k):
            return buf.at[b, pl.ds(pl.multiple_of(k * n_rows, n_rows), n_rows), :]

        def hop(b, k, recv, tp):
            ref = part(b, k)
            return put(ref, ref, ss.at[0], recv, (s, tp))

        def own(k):
            hop(t, k, rs.at[L1, k], right).start()
            hop(t, k, rs.at[R1, k], left).start()
            hop(t, k, near.at[k // group], sib).start()

        def pass_on(k):
            hop(left, k, rs.at[L1, k], right).wait_recv()
            if k % 2 == 0:
                hop(left, k, rs.at[OPP, k], right).start()
            hop(left, k, near.at[k // group], sib).start()
            hop(right, k, rs.at[R1, k], left).wait_recv()
            if k % 2 == 1:
                hop(right, k, rs.at[OPP, k], left).start()
            hop(right, k, near.at[k // group], sib).start()

        def pass_last(k):
            hop(opp, k, rs.at[OPP, k], right).wait_recv()
            hop(opp, k, far.at[k // group], sib).start()

        def two(first, blocks, m):
            return buf.at[pl.ds(first, blocks), pl.ds(pl.multiple_of(m * 2 * BLK, 2 * BLK), 2 * BLK), :]

        def arrived_near(m):
            ref = two(0, 3, m)
            put(ref, ref, ss.at[0], near.at[m], (s, sib)).wait_recv()

        def arrived_far(m):
            ref = two(0, 1, m)
            put(ref, ref, ss.at[0], far.at[m], (s, sib)).wait_recv()

        def sent():
            put(buf.at[0:7], buf.at[0:7], ss.at[0], near.at[0], (s, sib)).wait_send()

        return own, pass_on, pass_last, arrived_near, arrived_far, sent

    own, pass_on, pass_last, arrived_near, arrived_far, sent = gather(X, BLK, xs_s, xs_r, xn_r, xf_r)
    a_own, a_pass, a_last, a_near, a_far, a_sent = gather(A, arows, as_s, as_r, an_r, af_r)
    r_own, r_pass, r_last, r_near, r_far, r_sent = gather(R, BLK, rs_s, rs_r, rn_r, rf_r)

    for k in range(AHEAD):
        own(k)
    for d in range(1, nx):
        put(DX.at[x], DX.at[x], dx_s.at[0], dx_r.at[0], (z * nx + (x + d) % nx, t)).start()

    lane_b = lax.broadcasted_iota(jnp.int32, (BLK, BLK), 1)
    row_b = lax.broadcasted_iota(jnp.int32, (BLK, BLK), 0)
    low = lane_b < 64

    def blk(j):
        return pl.ds(pl.multiple_of(j * BLK, BLK), BLK)

    def column(j):
        row = jnp.broadcast_to(crow[pl.ds(j, 1), :], (BLK, BLK))
        return jnp.sum(jnp.where(lane_b == row_b, row, 0.0), axis=1, keepdims=True)

    def tables(j, carry):
        pos = (s * rows + j * BLK + row_b).astype(F32)
        angle = pos * inv[...]
        scale = jnp.where(low, 1.0, 64**-0.5).astype(F32)
        COS[blk(j), :] = jnp.cos(angle) * scale
        SIN[blk(j), :] = jnp.sin(angle) * jnp.where(lane_b % 64 < 32, -scale, scale)
        return carry

    def pair(m):
        return pl.ds(pl.multiple_of(m * 2 * BLK, 2 * BLK), 2 * BLK)

    def sums(m, acc, squares, blocks):
        for b in blocks:
            cols = pl.ds(pl.multiple_of(b * cw, cw), cw)
            xf = X[b, pair(m), :].astype(F32)
            sq = xf * xf
            squares = squares + sum(sq[:, i : i + 128] for i in range(0, cw, 128))
            acc = acc + jnp.dot((xf * gain[:, cols]).astype(BF16), W1[cols, :], preferred_element_type=F32)
        return acc, squares

    def project_near(m):
        arrived_near(m)
        zero = jnp.zeros((2 * BLK, 640), F32), jnp.zeros((2 * BLK, 128), F32)
        ACC[m], SQ[m] = sums(m, *zero, (t, sib, left, right, sib_left, sib_right))

    def project(m):
        two = pair(m)
        arrived_far(m)
        acc, squares = sums(m, ACC[m], SQ[m], (opp, sib_opp))
        inv_rms = lax.rsqrt(jnp.sum(squares, axis=1, keepdims=True) / width + NORM_EPS)
        p = (acc * inv_rms).astype(BF16)
        Q[two, :] = p[:, 0:128]
        V[two, :] = p[:, 128:256]
        G[two, :] = p[:, 256:384]
        KV[pl.ds(pl.multiple_of(m * 2 * BLK + BLK, BLK), 2 * BLK), :] = p[:, 384:512]
        for h in range(2):
            j = 2 * m + h
            cosine, sine, cc = COS[blk(j), :], SIN[blk(j), :], column(j)
            bl = bl8[pl.ds(j, 1), :]
            pre = pre8[pl.ds(j, 1), :]
            rqk = p[h * BLK : (h + 1) * BLK, 512:640].astype(F32)
            swapped = jnp.where(lane_b % 64 < 32, pltpu.roll(rqk, 96, 1), pltpu.roll(rqk, 32, 1))
            rot = rqk * cosine + swapped * sine
            QR[blk(j), :] = rot.astype(BF16)
            other = pltpu.roll(rot, 64, 1)
            qq = jnp.where(low, rot, other)
            kk = jnp.where(low, other, rot)
            to_end = jnp.exp(bl - cc)
            to_here = jnp.exp(jnp.broadcast_to(cc, (BLK, BLK)))
            QB[blk(j), :] = (qq * jnp.where(low, to_here, to_end)).astype(BF16)
            full = cc + pre
            QX[blk(j), :] = (qq * jnp.exp(jnp.where(low, full, tot - full))).astype(BF16)
            kw = (kk * jnp.where(low, to_end, to_here)).astype(BF16)
            v = p[h * BLK : (h + 1) * BLK, 128:256]
            TT[j] = lax.dot_general(kw, v, TN, preferred_element_type=F32)

    for i in range(5, 14):
        copies[i].wait()
    for b in range(8):
        W1[b * cw : (b + 1) * cw, 384:640] = W2[:, b * cw : (b + 1) * cw].T
    lax.fori_loop(0, nb, tables, 0)

    halo_up = put(KV.at[pl.ds(rows, BLK), :], KV.at[pl.ds(0, BLK), :], h_s.at[0], h_r.at[0], (up, t))
    halo_down = put(KV.at[pl.ds(BLK, BLK), :], KV.at[pl.ds(rows + BLK, BLK), :], h_s.at[1], h_r.at[1], (down, t))

    row_q = lax.broadcasted_iota(jnp.int32, (2 * BLK, BLK), 0) % BLK
    lane_q = lax.broadcasted_iota(jnp.int32, (2 * BLK, BLK), 1)
    sink = jnp.where(lax.broadcasted_iota(jnp.int32, (2 * BLK, 1), 0) < BLK, sink_ref[0], sink_ref[1])

    def attend(j):
        q = Q[blk(j), :]
        q2 = jnp.concatenate([q[:, 0:64], q[:, 64:128]], axis=0)
        kv = KV[pl.ds(pl.multiple_of(j * BLK, BLK), 3 * BLK), :]
        sc = lax.dot_general(q2, kv[:, 0:64], NT, preferred_element_type=F32) * HD**-0.5
        first = jnp.where(s * nb + j == 0, BLK, 0)
        last = jnp.where(s * nb + j == n_sp * nb - 1, BLK, 0)
        s0 = jnp.where(lane_q - first >= row_q, sc[:, 0:128], -jnp.inf)
        s1 = sc[:, 128:256]
        s2 = jnp.where(lane_q + last <= row_q, sc[:, 256:384], -jnp.inf)
        top = jnp.maximum(jnp.max(jnp.maximum(jnp.maximum(s0, s1), s2), axis=1, keepdims=True), sink)
        e0, e1, e2 = jnp.exp(s0 - top), jnp.exp(s1 - top), jnp.exp(s2 - top)
        den = jnp.sum(e0 + e1 + e2, axis=1, keepdims=True) + jnp.exp(sink - top)
        ee = jnp.concatenate([e0.astype(BF16), e1.astype(BF16), e2.astype(BF16)], axis=1)
        o = jnp.dot(ee, kv[:, 64:128], preferred_element_type=F32) / den
        A[t, blk(j), :] = jnp.concatenate([o[0:BLK], o[BLK : 2 * BLK]], axis=1).astype(BF16)

    def weights_out():
        for i, half in enumerate((oa_h, or_h)):
            for d in range(1, 8):
                to = (t + d) % 8
                cols = pl.ds(pl.multiple_of(to * ocw, 128), ocw)
                put(half.at[mine, cols], WO.at[i, t, mine, :], w1_s.at[i], w1_r.at[i], (s, to)).start()

    def on(k):
        pass_on(k)
        if k + AHEAD < nb:
            own(k + AHEAD)

    @pl.when(has_down == 0)
    def _():
        KV[0:BLK, :] = jnp.zeros((BLK, 128), BF16)

    @pl.when(has_up == 0)
    def _():
        KV[rows + BLK : rows + 2 * BLK, :] = jnp.zeros((BLK, 128), BF16)

    on(0)
    on(1)
    on(2)
    on(3)
    project_near(0)
    on(4)
    project_near(1)
    pass_last(0)
    on(5)
    pass_last(1)

    def keys_down():
        @pl.when(has_down == 1)
        def _():
            halo_down.start()

    @pl.when(c == 0)
    def _():
        project_near(2)
        on(6)
        project(0)
        keys_down()
        pass_last(2)
        on(7)
        weights_out()
        pass_last(3)
        project(1)
        project_near(3)
        pass_last(4)
        pass_last(5)
        project(2)
        pass_last(6)
        pass_last(7)
        project(3)

    @pl.when(c == 1)
    def _():
        on(6)
        pass_last(2)
        on(7)
        weights_out()
        project_near(2)
        project(0)
        keys_down()
        pass_last(3)
        pass_last(4)
        pass_last(5)
        project(1)
        pass_last(6)
        project_near(3)
        pass_last(7)
        project(2)
        project(3)

    f = jnp.zeros((64, RV), F32)
    g = jnp.zeros((64, RV), F32)
    for b in range(nb):
        SL[b, 0:64, :] = f.astype(BF16)
        f = jnp.exp(bl8[b : b + 1, :]) * f + TT[b, 0:64, :]
        e = nb - 1 - b
        SL[e, 64:128, :] = g.astype(BF16)
        g = jnp.exp(bl8[e : e + 1, :]) * g + TT[e, 64:128, :]
    XS[x, 0:64, :] = f.astype(BF16)
    XS[x, 64:128, :] = g.astype(BF16)
    for d in sorted(range(1, nx), key=lambda d: -min(d, nx - d)):
        put(XS.at[x], XS.at[x], sx_s.at[0], sx_r.at[0], (z * nx + (x + d) % nx, t)).start()

    @pl.when(has_up == 1)
    def _():
        halo_up.start()


    put(DX.at[0 : nx - 1], DX.at[0 : nx - 1], dx_s.at[0], dx_r.at[0], (s, sib)).wait_recv()
    total = DX[0]
    for i in range(1, nx):
        total = total + DX[i]
    DZ[z] = total
    for d in range(1, nz):
        put(DZ.at[z], DZ.at[z], dz_s.at[0], dz_r.at[0], (((z + d) % nz) * nx + x, t)).start()

    attend(1)
    attend(2)
    attend(3)
    a_own(1)
    attend(4)
    attend(5)
    a_own(2)

    @pl.when(has_up == 1)
    def _():
        halo_down.wait_recv()

    attend(6)
    attend(7)
    a_own(3)

    xr, xl = z * nx + (x + 1) % nx, z * nx + (x + nx - 1) % nx

    def quarter_of(o):
        return pl.ds(pl.multiple_of(((x + o + nx) % nx) * quarter, quarter), quarter)

    def w2_own(i):
        ref = WO.at[i, 0:7, mine, :]
        put(ref, ref, w1_s.at[i], w1_r.at[i], (s, sib)).wait_recv()
        ref = WO.at[i, :, mine, :]
        put(ref, ref, w2_s.at[i], w2_r.at[i, 0], (xr, t)).start()
        put(ref, ref, w2_s.at[i], w2_r.at[i, 1], (xl, t)).start()

    def w2_pass(i):
        from_left = WO.at[i, :, quarter_of(-1), :]
        from_right = WO.at[i, :, quarter_of(1), :]
        put(from_left, from_left, w2_s.at[i], w2_r.at[i, 0], (xr, t)).wait_recv()
        half = WO.at[i, 0:4, quarter_of(-1), :]
        put(half, half, w2_s.at[i], w2_r.at[i, 2], (xr, t)).start()
        put(from_right, from_right, w2_s.at[i], w2_r.at[i, 1], (xl, t)).wait_recv()
        half = WO.at[i, 4:8, quarter_of(1), :]
        put(half, half, w2_s.at[i], w2_r.at[i, 3], (xl, t)).start()

    def w2_done(i):
        half = WO.at[i, 0:4, quarter_of(2), :]
        put(half, half, w2_s.at[i], w2_r.at[i, 2], (xr, t)).wait_recv()
        half = WO.at[i, 4:8, quarter_of(2), :]
        put(half, half, w2_s.at[i], w2_r.at[i, 3], (xl, t)).wait_recv()

    def w2_sent(i):
        ref = WO.at[i, :, 0 : 3 * quarter, :]
        put(ref, ref, w2_s.at[i], w2_r.at[i, 0], (xr, t)).wait_send()

    put(XS.at[0 : nx - 1], XS.at[0 : nx - 1], sx_s.at[0], sx_r.at[0], (s, sib)).wait_recv()
    ex = [jnp.exp(DX[i][0:1, :]) for i in range(nx)]
    fx = jnp.zeros((64, RV), F32)
    gx = jnp.zeros((64, RV), F32)
    fall = jnp.zeros((64, RV), F32)
    gall = jnp.zeros((64, RV), F32)
    dfx = jnp.zeros((1, RV), F32)
    dgx = jnp.zeros((1, RV), F32)
    for i in range(nx):
        term = XS[i, 0:64, :].astype(F32)
        fx = jnp.where(i < x, ex[i] * fx + term, fx)
        dfx = jnp.where(i < x, dfx + DX[i][0:1, :], dfx)
        fall = ex[i] * fall + term
        o = nx - 1 - i
        term = XS[o, 64:128, :].astype(F32)
        gx = jnp.where(o > x, ex[o] * gx + term, gx)
        dgx = jnp.where(o > x, dgx + DX[o][0:1, :], dgx)
        gall = ex[o] * gall + term
    ZG[0] = fall.astype(BF16)
    ZG[1] = gall.astype(BF16)
    ZS[z] = jnp.zeros((64, RV), BF16)
    for d in sorted(range(1, nz), key=lambda d: -min(d, nz - d)):
        put(ZG.at[(z + d) // nz], ZS.at[z], sz_s.at[0], sz_r.at[0], (((z + d) % nz) * nx + x, t)).start()

    w2_own(0)
    w2_own(1)

    @pl.when(has_down == 1)
    def _():
        halo_up.wait_recv()

    attend(0)
    a_own(0)

    def inside(j):
        cc = column(j)
        cr = crow[pl.ds(j, 1), :]
        qk = QR[blk(j), :]
        sc = lax.dot_general(qk[:, 0:64], qk[:, 64:128], NT, preferred_element_type=F32)
        w = (sc * jnp.exp(-jnp.abs(cc - cr))).astype(BF16)
        RL[blk(j), :] = jnp.dot(w, V[blk(j), :], preferred_element_type=F32) + jnp.dot(
            QB[blk(j), :], SL[j], preferred_element_type=F32
        )
        gate = G[blk(j), :].astype(F32)
        SG[blk(j), :] = gate / (1.0 + jnp.exp(-gate))

    def inside_two(m, carry):
        inside(2 * m)
        inside(2 * m + 1)
        return carry


    a_pass(1)
    lax.fori_loop(0, na // 2, inside_two, 0)
    a_pass(2)
    lax.fori_loop(na // 2, na, inside_two, 0)
    a_pass(3)

    sent()
    for i in range(2):
        ref = WO.at[i, 0:7, mine, :]
        put(ref, ref, w1_s.at[i], w1_r.at[i], (s, sib)).wait_send()
    put(XS.at[0 : nx - 1], XS.at[0 : nx - 1], sx_s.at[0], sx_r.at[0], (s, sib)).wait_send()
    put(DX.at[0 : nx - 1], DX.at[0 : nx - 1], dx_s.at[0], dx_r.at[0], (s, sib)).wait_send()

    @pl.when(has_up == 1)
    def _():
        halo_up.wait_send()

    @pl.when(has_down == 1)
    def _():
        halo_down.wait_send()


    a_pass(0)

    if nz > 1:
        put(DZ.at[0 : nz - 1], DZ.at[0 : nz - 1], dz_s.at[0], dz_r.at[0], (s, sib)).wait_recv()
        put(ZS.at[0 : nz - 1], ZS.at[0 : nz - 1], sz_s.at[0], sz_r.at[0], (s, sib)).wait_recv()
    fz = init[0:64, :]
    gz = init[64:128, :]
    for i in range(nz):
        term = ZS[i].astype(F32)
        fz = jnp.where(i < z, jnp.exp(DZ[i][0:1, :]) * fz + term, fz)
        o = nz - 1 - i
        term = ZS[o].astype(F32)
        gz = jnp.where(o > z, jnp.exp(DZ[o][0:1, :]) * gz + term, gz)
    ST = jnp.concatenate([fx + jnp.exp(dfx) * fz, gx + jnp.exp(dgx) * gz], axis=0).astype(BF16)

    def big(k):
        return pl.ds(pl.multiple_of(k * arows, arows), arows)

    def finish(k, carry):
        ret = RL[big(k), :] + jnp.dot(QX[big(k), :], carry, preferred_element_type=F32)
        cen = ret - jnp.mean(ret, axis=1, keepdims=True)
        nrm = cen * lax.rsqrt(jnp.mean(cen * cen, axis=1, keepdims=True) + NORM_EPS)
        R[t, big(k), :] = (SG[big(k), :] * nrm).astype(BF16)
        r_own(2 * k)
        r_own(2 * k + 1)
        return carry

    lax.fori_loop(0, na, finish, ST)

    def out_att(k):
        lhs = jnp.concatenate([A[b, big(k), :] for b in range(8)], axis=1)
        OA[big(k), :] = jnp.dot(lhs, WO[0].reshape(8 * BLK, ocw), preferred_element_type=F32)

    def out_ret(k):
        r_near(k)
        r_far(k)
        lhs = jnp.concatenate([R[b, big(k), :] for b in range(8)], axis=1)
        acc = OA[big(k), :] + jnp.dot(lhs, WO[1].reshape(8 * BLK, ocw), preferred_element_type=F32)
        OUT[big(k), :] = acc.astype(BF16)
        pltpu.make_async_copy(OUT.at[big(k), :], out_h.at[big(k), :], lsem.at[14 + k]).start()

    for k in range(nb):
        if k == 0:
            for i in range(1, na):
                a_last(i)
            w2_pass(0)
            a_last(0)
            w2_pass(1)
        r_pass(k)
        if k == nb // 2 - 1:
            w2_done(0)
        if nb // 2 <= k < nb - 1:
            a_near(k - nb // 2 + 1)
            a_far(k - nb // 2 + 1)
            out_att(k - nb // 2 + 1)
    a_near(0)
    a_far(0)
    out_att(0)
    for k in range(nb // 2):
        r_last(k)
    w2_done(1)
    a_sent()
    for i in range(2):
        w2_sent(i)
    if nz > 1:
        put(ZS.at[0 : nz - 1], ZS.at[0 : nz - 1], sz_s.at[0], sz_r.at[0], (s, sib)).wait_send()
        put(DZ.at[0 : nz - 1], DZ.at[0 : nz - 1], dz_s.at[0], dz_r.at[0], (s, sib)).wait_send()
    out_ret(0)
    r_last(4)
    r_last(5)
    out_ret(1)
    r_last(6)
    r_last(7)
    out_ret(2)
    out_ret(3)

    r_sent()
    for k in range(na):
        pltpu.make_async_copy(OUT.at[big(k), :], out_h.at[big(k), :], lsem.at[14 + k]).wait()


def body(tokens, norm_gain, att_query, att_key, att_value, ret_query, ret_key, ret_value, ret_gate, att_sink, decay_log, init_state,
         out_att, out_ret, *, n_sp):
    rows, cw = tokens.shape
    width = 8 * cw
    ocw = out_att.shape[1] // 8
    nb, na = rows // BLK, rows // (2 * BLK)
    nx = 4
    nz = n_sp // nx
    inverse = (np.float64(ROPE_BASE) ** (-2.0 * (np.arange(128) % 32) / 64)).astype(np.float32)[None, :]
    dma = pltpu.SemaphoreType.DMA
    hbm = pl.BlockSpec(memory_space=pltpu.HBM)
    specs = [hbm] * 15
    specs[9] = pl.BlockSpec(memory_space=pltpu.SMEM)
    vm = pltpu.VMEM
    scratch = [
        vm((8, rows, cw), BF16), vm((width, 640), BF16), vm((256, width), BF16), vm((1, width), F32), vm((1, rows), F32),
        vm((128, 128), F32), vm((1, 128), F32),
        vm((rows, 128), BF16), vm((rows + 2 * BLK, 128), BF16), vm((rows, 128), BF16), vm((rows, 128), BF16), vm((rows, 128), F32),
        vm((rows, 128), F32), vm((rows, 128), F32), vm((nb // 2, 2 * BLK, 640), F32), vm((nb // 2, 2 * BLK, 128), F32), vm((rows, 128), BF16), vm((rows, 128), BF16), vm((rows, 128), BF16), vm((rows, 128), F32),
        vm((nb, 128, 128), F32), vm((nb, 128, 128), BF16),
        vm((8, rows, 128), BF16), vm((8, rows, 128), BF16), vm((2, 8, 128, ocw), BF16), vm((rows, ocw), F32), vm((rows, ocw), BF16),
        vm((nx, 128, 128), BF16), vm((2, 64, 128), BF16), vm((nz, 64, 128), BF16), vm((nx, 8, 128), F32), vm((nz, 8, 128), F32),
        vm((nb, 128), F32), vm((nb, 128), F32), vm((nb, 128), F32),
        dma((14 + na,)), dma((1,)), dma((3, nb)), dma((na,)), dma((na,)), dma((1,)), dma((3, na)), dma((na,)), dma((na,)),
        dma((1,)), dma((3, nb)), dma((na,)), dma((na,)),
        dma((2,)), dma((2,)), dma((2,)), dma((2, 4)), dma((1,)), dma((1,)), dma((1,)), dma((1,)),
        dma((1,)), dma((1,)), dma((1,)), dma((1,)), dma((2,)), dma((2,)),
    ]
    call = pl.pallas_call(
        functools.partial(kernel, n_sp, nx),
        out_shape=jax.ShapeDtypeStruct((rows, ocw), BF16),
        in_specs=specs,
        out_specs=hbm,
        scratch_shapes=scratch,
        compiler_params=pltpu.CompilerParams(collective_id=0, has_side_effects=True, vmem_limit_bytes=67_043_328),
        name="layer",
    )
    return call(
        tokens, norm_gain.reshape(1, width), att_query, att_key.T, att_value.T, ret_query.T, ret_key.T, ret_value, ret_gate,
        att_sink, decay_log, init_state.reshape(128, 128), inverse, out_att, out_ret,
    )


def solution(mesh):
    in_specs = (
        P("sp", "tp"), P(), P(None, "tp"), P(None, "tp"), P(None, "tp"), P(None, "tp"), P(None, "tp"), P(None, "tp"), P(None, "tp"),
        P("tp"), P("tp", "sp"), P(None, "tp", None, None), P("tp", None), P("tp", None),
    )
    return jax.shard_map(
        functools.partial(body, n_sp=mesh.shape["sp"]), mesh=mesh, in_specs=in_specs, out_specs=P("sp", "tp"), check_vma=False
    )
```

```python
import functools

import jax
import jax.numpy as jnp
import numpy as np
from jax import lax
from jax.experimental import pallas as pl
from jax.experimental.pallas import tpu as pltpu
from jax.sharding import PartitionSpec as P

HD = 64
RV = 128
BLK = 128
NORM_EPS = 1e-06
ROPE_BASE = 10000.0
MESH = pl.DeviceIdType.MESH
F32 = jnp.float32
BF16 = jnp.bfloat16
NT = (((1,), (1,)), ((), ()))
TN = (((0,), (0,)), ((), ()))
AHEAD = 5

L1, R1, OPP, SIB = 0, 1, 2, 3


def kernel(n_sp, nx, tok_h, gain_h, wq_h, wk_h, wv_h, wrq_h, wrk_h, wrv_h, wrg_h, sink_ref, dec_h, init_h, inv_h, oa_h, or_h,
           OUT,
           X, W1, W2, gain, dec, init, inv, Q, KV, V, G, SG, COS, SIN, ACC, SQ, QR, QB, QX, RL, TT, SL, A, R, WO, OA,
           XS, ZG, ZS, DX, DZ, crow, bl8, pre8,
           lsem, xs_s, xs_r, xn_r, xf_r, as_s, as_r, an_r, af_r, rs_s, rs_r, rn_r, rf_r, w1_s, w1_r, w2_s, w2_r, sx_s, sx_r, dx_s, dx_r, sz_s, sz_r, dz_s, dz_r,
           h_s, h_r):
    rows, cw = tok_h.shape
    nb = rows // BLK
    arows = 2 * BLK
    na = rows // arows
    width = 8 * cw
    ocw = OUT.shape[1]
    nz = n_sp // nx
    quarter = BLK // nx
    s, t = lax.axis_index("sp"), lax.axis_index("tp")
    z, x = s // nx, s % nx
    y, c = t // 2, t % 2
    right = 2 * ((y + 1) % 4) + c
    left = 2 * ((y + 3) % 4) + c
    opp = 2 * ((y + 2) % 4) + c
    sib = 2 * y + (1 - c)
    sib_right = 2 * ((y + 1) % 4) + 1 - c
    sib_left = 2 * ((y + 3) % 4) + 1 - c
    sib_opp = 2 * ((y + 2) % 4) + 1 - c
    up, down = (s + 1) % n_sp, (s + n_sp - 1) % n_sp

    loads = [
        (dec_h, dec), (tok_h, X.at[t]), (gain_h, gain), (inv_h, inv), (init_h, init),
        (wq_h, W1.at[:, 0:128]), (wrv_h, W1.at[:, 128:256]), (wrg_h, W1.at[:, 256:384]),
        (wk_h, W2.at[0:64]), (wv_h, W2.at[64:128]), (wrq_h, W2.at[128:192]), (wrk_h, W2.at[192:256]),
    ]
    mine = pl.ds(pl.multiple_of(x * quarter, quarter), quarter)
    my_cols = pl.ds(pl.multiple_of(t * ocw, 128), ocw)
    loads += [(oa_h.at[mine, my_cols], WO.at[0, t, mine, :]), (or_h.at[mine, my_cols], WO.at[1, t, mine, :])]
    copies = [pltpu.make_async_copy(a, b, lsem.at[i]) for i, (a, b) in enumerate(loads)]
    for cp in copies:
        cp.start()

    barrier = pltpu.get_barrier_semaphore()
    partners = [(s, (t + d) % 8) for d in range(1, 8)]
    partners += [(z * nx + (x + d) % nx, t) for d in range(1, nx)]
    partners += [(((z + d) % nz) * nx + x, t) for d in range(1, nz)]
    has_up, has_down = 1 - (s + 1) // n_sp, (s + n_sp - 1) // n_sp
    for p in reversed(partners):
        pl.semaphore_signal(barrier, inc=1, device_id=p, device_id_type=MESH)

    @pl.when(has_up == 1)
    def _():
        pl.semaphore_signal(barrier, inc=1, device_id=(up, t), device_id_type=MESH)

    @pl.when(has_down == 1)
    def _():
        pl.semaphore_signal(barrier, inc=1, device_id=(down, t), device_id_type=MESH)

    copies[0].wait()
    for b in range(nb):
        crow[b : b + 1, :] = dec[:, b * BLK : (b + 1) * BLK]
    cum = crow[...]
    lane = lax.broadcasted_iota(jnp.int32, (nb, BLK), 1)
    for sh in (1, 2, 4, 8, 16, 32, 64):
        cum = cum + jnp.where(lane >= sh, pltpu.roll(cum, sh, 1), 0.0)
    crow[...] = cum
    bl8[...] = jnp.broadcast_to(cum[:, BLK - 1 : BLK], (nb, BLK))
    run = jnp.zeros((1, BLK), F32)
    for b in range(nb):
        pre8[b : b + 1, :] = run
        run = run + bl8[b : b + 1, :]
    tot = run
    DX[x] = jnp.broadcast_to(tot, (8, BLK))
    for i in range(1, 5):
        copies[i].wait()

    pl.semaphore_wait(barrier, len(partners) + has_up + has_down)

    def put(src, dst, send, recv, dev):
        return pltpu.make_async_remote_copy(src_ref=src, dst_ref=dst, send_sem=send, recv_sem=recv, device_id=dev, device_id_type=MESH)

    def gather(buf, n_rows, ss, rs, near, far):
        group = 2 * BLK // n_rows

        def part(b, k):
            return buf.at[b, pl.ds(pl.multiple_of(k * n_rows, n_rows), n_rows), :]

        def hop(b, k, recv, tp):
            ref = part(b, k)
            return put(ref, ref, ss.at[0], recv, (s, tp))

        def own(k):
            hop(t, k, rs.at[L1, k], right).start()
            hop(t, k, rs.at[R1, k], left).start()
            hop(t, k, near.at[k // group], sib).start()

        def pass_on(k):
            hop(left, k, rs.at[L1, k], right).wait_recv()
            if k % 2 == 0:
                hop(left, k, rs.at[OPP, k], right).start()
            hop(left, k, near.at[k // group], sib).start()
            hop(right, k, rs.at[R1, k], left).wait_recv()
            if k % 2 == 1:
                hop(right, k, rs.at[OPP, k], left).start()
            hop(right, k, near.at[k // group], sib).start()

        def pass_last(k):
            hop(opp, k, rs.at[OPP, k], right).wait_recv()
            hop(opp, k, far.at[k // group], sib).start()

        def two(first, blocks, m):
            return buf.at[pl.ds(first, blocks), pl.ds(pl.multiple_of(m * 2 * BLK, 2 * BLK), 2 * BLK), :]

        def arrived_near(m):
            ref = two(0, 3, m)
            put(ref, ref, ss.at[0], near.at[m], (s, sib)).wait_recv()

        def arrived_far(m):
            ref = two(0, 1, m)
            put(ref, ref, ss.at[0], far.at[m], (s, sib)).wait_recv()

        def sent():
            put(buf.at[0:7], buf.at[0:7], ss.at[0], near.at[0], (s, sib)).wait_send()

        return own, pass_on, pass_last, arrived_near, arrived_far, sent

    own, pass_on, pass_last, arrived_near, arrived_far, sent = gather(X, BLK, xs_s, xs_r, xn_r, xf_r)
    a_own, a_pass, a_last, a_near, a_far, a_sent = gather(A, arows, as_s, as_r, an_r, af_r)
    r_own, r_pass, r_last, r_near, r_far, r_sent = gather(R, BLK, rs_s, rs_r, rn_r, rf_r)

    for k in range(AHEAD):
        own(k)
    for d in range(1, nx):
        put(DX.at[x], DX.at[x], dx_s.at[0], dx_r.at[0], (z * nx + (x + d) % nx, t)).start()

    lane_b = lax.broadcasted_iota(jnp.int32, (BLK, BLK), 1)
    row_b = lax.broadcasted_iota(jnp.int32, (BLK, BLK), 0)
    low = lane_b < 64

    def blk(j):
        return pl.ds(pl.multiple_of(j * BLK, BLK), BLK)

    def column(j):
        row = jnp.broadcast_to(crow[pl.ds(j, 1), :], (BLK, BLK))
        return jnp.sum(jnp.where(lane_b == row_b, row, 0.0), axis=1, keepdims=True)

    def tables(j, carry):
        pos = (s * rows + j * BLK + row_b).astype(F32)
        angle = pos * inv[...]
        scale = jnp.where(low, 1.0, 64**-0.5).astype(F32)
        COS[blk(j), :] = jnp.cos(angle) * scale
        SIN[blk(j), :] = jnp.sin(angle) * jnp.where(lane_b % 64 < 32, -scale, scale)
        return carry

    def pair(m):
        return pl.ds(pl.multiple_of(m * 2 * BLK, 2 * BLK), 2 * BLK)

    def sums(m, acc, squares, blocks):
        for b in blocks:
            cols = pl.ds(pl.multiple_of(b * cw, cw), cw)
            xf = X[b, pair(m), :].astype(F32)
            sq = xf * xf
            squares = squares + sum(sq[:, i : i + 128] for i in range(0, cw, 128))
            acc = acc + jnp.dot((xf * gain[:, cols]).astype(BF16), W1[cols, :], preferred_element_type=F32)
        return acc, squares

    def project_near(m):
        arrived_near(m)
        zero = jnp.zeros((2 * BLK, 640), F32), jnp.zeros((2 * BLK, 128), F32)
        ACC[m], SQ[m] = sums(m, *zero, (t, sib, left, right, sib_left, sib_right))

    def project(m):
        two = pair(m)
        arrived_far(m)
        acc, squares = sums(m, ACC[m], SQ[m], (opp, sib_opp))
        inv_rms = lax.rsqrt(jnp.sum(squares, axis=1, keepdims=True) / width + NORM_EPS)
        p = (acc * inv_rms).astype(BF16)
        Q[two, :] = p[:, 0:128]
        V[two, :] = p[:, 128:256]
        G[two, :] = p[:, 256:384]
        KV[pl.ds(pl.multiple_of(m * 2 * BLK + BLK, BLK), 2 * BLK), :] = p[:, 384:512]
        for h in range(2):
            j = 2 * m + h
            cosine, sine, cc = COS[blk(j), :], SIN[blk(j), :], column(j)
            bl = bl8[pl.ds(j, 1), :]
            pre = pre8[pl.ds(j, 1), :]
            rqk = p[h * BLK : (h + 1) * BLK, 512:640].astype(F32)
            swapped = jnp.where(lane_b % 64 < 32, pltpu.roll(rqk, 96, 1), pltpu.roll(rqk, 32, 1))
            rot = rqk * cosine + swapped * sine
            QR[blk(j), :] = rot.astype(BF16)
            other = pltpu.roll(rot, 64, 1)
            qq = jnp.where(low, rot, other)
            kk = jnp.where(low, other, rot)
            to_end = jnp.exp(bl - cc)
            to_here = jnp.exp(jnp.broadcast_to(cc, (BLK, BLK)))
            QB[blk(j), :] = (qq * jnp.where(low, to_here, to_end)).astype(BF16)
            full = cc + pre
            QX[blk(j), :] = (qq * jnp.exp(jnp.where(low, full, tot - full))).astype(BF16)
            kw = (kk * jnp.where(low, to_end, to_here)).astype(BF16)
            v = p[h * BLK : (h + 1) * BLK, 128:256]
            TT[j] = lax.dot_general(kw, v, TN, preferred_element_type=F32)

    for i in range(5, 14):
        copies[i].wait()
    for b in range(8):
        W1[b * cw : (b + 1) * cw, 384:640] = W2[:, b * cw : (b + 1) * cw].T
    lax.fori_loop(0, nb, tables, 0)

    halo_up = put(KV.at[pl.ds(rows, BLK), :], KV.at[pl.ds(0, BLK), :], h_s.at[0], h_r.at[0], (up, t))
    halo_down = put(KV.at[pl.ds(BLK, BLK), :], KV.at[pl.ds(rows + BLK, BLK), :], h_s.at[1], h_r.at[1], (down, t))

    row_q = lax.broadcasted_iota(jnp.int32, (2 * BLK, BLK), 0) % BLK
    lane_q = lax.broadcasted_iota(jnp.int32, (2 * BLK, BLK), 1)
    sink = jnp.where(lax.broadcasted_iota(jnp.int32, (2 * BLK, 1), 0) < BLK, sink_ref[0], sink_ref[1])

    def attend(j):
        q = Q[blk(j), :]
        q2 = jnp.concatenate([q[:, 0:64], q[:, 64:128]], axis=0)
        kv = KV[pl.ds(pl.multiple_of(j * BLK, BLK), 3 * BLK), :]
        sc = lax.dot_general(q2, kv[:, 0:64], NT, preferred_element_type=F32) * HD**-0.5
        first = jnp.where(s * nb + j == 0, BLK, 0)
        last = jnp.where(s * nb + j == n_sp * nb - 1, BLK, 0)
        s0 = jnp.where(lane_q - first >= row_q, sc[:, 0:128], -jnp.inf)
        s1 = sc[:, 128:256]
        s2 = jnp.where(lane_q + last <= row_q, sc[:, 256:384], -jnp.inf)
        top = jnp.maximum(jnp.max(jnp.maximum(jnp.maximum(s0, s1), s2), axis=1, keepdims=True), sink)
        e0, e1, e2 = jnp.exp(s0 - top), jnp.exp(s1 - top), jnp.exp(s2 - top)
        den = jnp.sum(e0 + e1 + e2, axis=1, keepdims=True) + jnp.exp(sink - top)
        ee = jnp.concatenate([e0.astype(BF16), e1.astype(BF16), e2.astype(BF16)], axis=1)
        o = jnp.dot(ee, kv[:, 64:128], preferred_element_type=F32) / den
        A[t, blk(j), :] = jnp.concatenate([o[0:BLK], o[BLK : 2 * BLK]], axis=1).astype(BF16)

    def weights_out():
        for i, half in enumerate((oa_h, or_h)):
            for d in range(1, 8):
                to = (t + d) % 8
                cols = pl.ds(pl.multiple_of(to * ocw, 128), ocw)
                put(half.at[mine, cols], WO.at[i, t, mine, :], w1_s.at[i], w1_r.at[i], (s, to)).start()

    def on(k):
        pass_on(k)
        if k + AHEAD < nb:
            own(k + AHEAD)

    @pl.when(has_down == 0)
    def _():
        KV[0:BLK, :] = jnp.zeros((BLK, 128), BF16)

    @pl.when(has_up == 0)
    def _():
        KV[rows + BLK : rows + 2 * BLK, :] = jnp.zeros((BLK, 128), BF16)

    on(0)
    on(1)
    on(2)
    on(3)
    project_near(0)
    on(4)
    project_near(1)
    pass_last(0)
    on(5)
    pass_last(1)

    def keys_down():
        @pl.when(has_down == 1)
        def _():
            halo_down.start()

    @pl.when(c == 0)
    def _():
        project_near(2)
        on(6)
        project(0)
        keys_down()
        pass_last(2)
        on(7)
        weights_out()
        pass_last(3)
        project(1)
        project_near(3)
        pass_last(4)
        pass_last(5)
        project(2)
        pass_last(6)
        pass_last(7)
        project(3)

    @pl.when(c == 1)
    def _():
        on(6)
        pass_last(2)
        on(7)
        weights_out()
        project_near(2)
        project(0)
        keys_down()
        pass_last(3)
        pass_last(4)
        pass_last(5)
        project(1)
        pass_last(6)
        project_near(3)
        pass_last(7)
        project(2)
        project(3)

    f = jnp.zeros((64, RV), F32)
    g = jnp.zeros((64, RV), F32)
    for b in range(nb):
        SL[b, 0:64, :] = f.astype(BF16)
        f = jnp.exp(bl8[b : b + 1, :]) * f + TT[b, 0:64, :]
        e = nb - 1 - b
        SL[e, 64:128, :] = g.astype(BF16)
        g = jnp.exp(bl8[e : e + 1, :]) * g + TT[e, 64:128, :]
    XS[x, 0:64, :] = f.astype(BF16)
    XS[x, 64:128, :] = g.astype(BF16)
    for d in sorted(range(1, nx), key=lambda d: -min(d, nx - d)):
        put(XS.at[x], XS.at[x], sx_s.at[0], sx_r.at[0], (z * nx + (x + d) % nx, t)).start()

    @pl.when(has_up == 1)
    def _():
        halo_up.start()


    put(DX.at[0 : nx - 1], DX.at[0 : nx - 1], dx_s.at[0], dx_r.at[0], (s, sib)).wait_recv()
    total = DX[0]
    for i in range(1, nx):
        total = total + DX[i]
    DZ[z] = total
    for d in range(1, nz):
        put(DZ.at[z], DZ.at[z], dz_s.at[0], dz_r.at[0], (((z + d) % nz) * nx + x, t)).start()

    attend(1)
    attend(2)
    attend(3)
    a_own(1)
    attend(4)
    attend(5)
    a_own(2)

    @pl.when(has_up == 1)
    def _():
        halo_down.wait_recv()

    attend(6)
    attend(7)
    a_own(3)

    xr, xl = z * nx + (x + 1) % nx, z * nx + (x + nx - 1) % nx

    def quarter_of(o):
        return pl.ds(pl.multiple_of(((x + o + nx) % nx) * quarter, quarter), quarter)

    def w2_own(i):
        ref = WO.at[i, 0:7, mine, :]
        put(ref, ref, w1_s.at[i], w1_r.at[i], (s, sib)).wait_recv()
        ref = WO.at[i, :, mine, :]
        put(ref, ref, w2_s.at[i], w2_r.at[i, 0], (xr, t)).start()
        put(ref, ref, w2_s.at[i], w2_r.at[i, 1], (xl, t)).start()

    def w2_pass(i):
        from_left = WO.at[i, :, quarter_of(-1), :]
        from_right = WO.at[i, :, quarter_of(1), :]
        put(from_left, from_left, w2_s.at[i], w2_r.at[i, 0], (xr, t)).wait_recv()
        half = WO.at[i, 0:4, quarter_of(-1), :]
        put(half, half, w2_s.at[i], w2_r.at[i, 2], (xr, t)).start()
        put(from_right, from_right, w2_s.at[i], w2_r.at[i, 1], (xl, t)).wait_recv()
        half = WO.at[i, 4:8, quarter_of(1), :]
        put(half, half, w2_s.at[i], w2_r.at[i, 3], (xl, t)).start()

    def w2_done(i):
        half = WO.at[i, 0:4, quarter_of(2), :]
        put(half, half, w2_s.at[i], w2_r.at[i, 2], (xr, t)).wait_recv()
        half = WO.at[i, 4:8, quarter_of(2), :]
        put(half, half, w2_s.at[i], w2_r.at[i, 3], (xl, t)).wait_recv()

    def w2_sent(i):
        ref = WO.at[i, :, 0 : 3 * quarter, :]
        put(ref, ref, w2_s.at[i], w2_r.at[i, 0], (xr, t)).wait_send()

    put(XS.at[0 : nx - 1], XS.at[0 : nx - 1], sx_s.at[0], sx_r.at[0], (s, sib)).wait_recv()
    ex = [jnp.exp(DX[i][0:1, :]) for i in range(nx)]
    fx = jnp.zeros((64, RV), F32)
    gx = jnp.zeros((64, RV), F32)
    fall = jnp.zeros((64, RV), F32)
    gall = jnp.zeros((64, RV), F32)
    dfx = jnp.zeros((1, RV), F32)
    dgx = jnp.zeros((1, RV), F32)
    for i in range(nx):
        term = XS[i, 0:64, :].astype(F32)
        fx = jnp.where(i < x, ex[i] * fx + term, fx)
        dfx = jnp.where(i < x, dfx + DX[i][0:1, :], dfx)
        fall = ex[i] * fall + term
        o = nx - 1 - i
        term = XS[o, 64:128, :].astype(F32)
        gx = jnp.where(o > x, ex[o] * gx + term, gx)
        dgx = jnp.where(o > x, dgx + DX[o][0:1, :], dgx)
        gall = ex[o] * gall + term
    ZG[0] = fall.astype(BF16)
    ZG[1] = gall.astype(BF16)
    ZS[z] = jnp.zeros((64, RV), BF16)
    for d in sorted(range(1, nz), key=lambda d: -min(d, nz - d)):
        put(ZG.at[(z + d) // nz], ZS.at[z], sz_s.at[0], sz_r.at[0], (((z + d) % nz) * nx + x, t)).start()

    w2_own(0)
    w2_own(1)

    @pl.when(has_down == 1)
    def _():
        halo_up.wait_recv()

    attend(0)
    a_own(0)

    def inside(j):
        cc = column(j)
        cr = crow[pl.ds(j, 1), :]
        qk = QR[blk(j), :]
        sc = lax.dot_general(qk[:, 0:64], qk[:, 64:128], NT, preferred_element_type=F32)
        w = (sc * jnp.exp(-jnp.abs(cc - cr))).astype(BF16)
        RL[blk(j), :] = jnp.dot(w, V[blk(j), :], preferred_element_type=F32) + jnp.dot(
            QB[blk(j), :], SL[j], preferred_element_type=F32
        )
        gate = G[blk(j), :].astype(F32)
        SG[blk(j), :] = gate / (1.0 + jnp.exp(-gate))

    def inside_two(m, carry):
        inside(2 * m)
        inside(2 * m + 1)
        return carry


    a_pass(1)
    lax.fori_loop(0, na // 2, inside_two, 0)
    a_pass(2)
    lax.fori_loop(na // 2, na, inside_two, 0)
    a_pass(3)

    sent()
    for i in range(2):
        ref = WO.at[i, 0:7, mine, :]
        put(ref, ref, w1_s.at[i], w1_r.at[i], (s, sib)).wait_send()
    put(XS.at[0 : nx - 1], XS.at[0 : nx - 1], sx_s.at[0], sx_r.at[0], (s, sib)).wait_send()
    put(DX.at[0 : nx - 1], DX.at[0 : nx - 1], dx_s.at[0], dx_r.at[0], (s, sib)).wait_send()

    @pl.when(has_up == 1)
    def _():
        halo_up.wait_send()

    @pl.when(has_down == 1)
    def _():
        halo_down.wait_send()


    a_pass(0)

    if nz > 1:
        put(DZ.at[0 : nz - 1], DZ.at[0 : nz - 1], dz_s.at[0], dz_r.at[0], (s, sib)).wait_recv()
        put(ZS.at[0 : nz - 1], ZS.at[0 : nz - 1], sz_s.at[0], sz_r.at[0], (s, sib)).wait_recv()
    fz = init[0:64, :]
    gz = init[64:128, :]
    for i in range(nz):
        term = ZS[i].astype(F32)
        fz = jnp.where(i < z, jnp.exp(DZ[i][0:1, :]) * fz + term, fz)
        o = nz - 1 - i
        term = ZS[o].astype(F32)
        gz = jnp.where(o > z, jnp.exp(DZ[o][0:1, :]) * gz + term, gz)
    ST = jnp.concatenate([fx + jnp.exp(dfx) * fz, gx + jnp.exp(dgx) * gz], axis=0).astype(BF16)

    def big(k):
        return pl.ds(pl.multiple_of(k * arows, arows), arows)

    def finish(k, carry):
        ret = RL[big(k), :] + jnp.dot(QX[big(k), :], carry, preferred_element_type=F32)
        cen = ret - jnp.mean(ret, axis=1, keepdims=True)
        nrm = cen * lax.rsqrt(jnp.mean(cen * cen, axis=1, keepdims=True) + NORM_EPS)
        R[t, big(k), :] = (SG[big(k), :] * nrm).astype(BF16)
        r_own(2 * k)
        r_own(2 * k + 1)
        return carry

    lax.fori_loop(0, na, finish, ST)

    def out_att(k):
        lhs = jnp.concatenate([A[b, big(k), :] for b in range(8)], axis=1)
        OA[big(k), :] = jnp.dot(lhs, WO[0].reshape(8 * BLK, ocw), preferred_element_type=F32)

    def out_ret(k):
        r_near(k)
        r_far(k)
        lhs = jnp.concatenate([R[b, big(k), :] for b in range(8)], axis=1)
        acc = OA[big(k), :] + jnp.dot(lhs, WO[1].reshape(8 * BLK, ocw), preferred_element_type=F32)
        OUT[big(k), :] = acc.astype(BF16)

    for k in range(nb):
        if k == 0:
            for i in range(1, na):
                a_last(i)
            w2_pass(0)
            a_last(0)
            w2_pass(1)
        r_pass(k)
        if k == nb // 2 - 1:
            w2_done(0)
        if nb // 2 <= k < nb - 1:
            a_near(k - nb // 2 + 1)
            a_far(k - nb // 2 + 1)
            out_att(k - nb // 2 + 1)
    a_near(0)
    a_far(0)
    out_att(0)
    for k in range(nb // 2):
        r_last(k)
    w2_done(1)
    a_sent()
    for i in range(2):
        w2_sent(i)
    if nz > 1:
        put(ZS.at[0 : nz - 1], ZS.at[0 : nz - 1], sz_s.at[0], sz_r.at[0], (s, sib)).wait_send()
        put(DZ.at[0 : nz - 1], DZ.at[0 : nz - 1], dz_s.at[0], dz_r.at[0], (s, sib)).wait_send()
    out_ret(0)
    r_last(4)
    r_last(5)
    out_ret(1)
    r_last(6)
    r_last(7)
    out_ret(2)
    out_ret(3)

    r_sent()


def body(tokens, norm_gain, att_query, att_key, att_value, ret_query, ret_key, ret_value, ret_gate, att_sink, decay_log, init_state,
         out_att, out_ret, *, n_sp):
    rows, cw = tokens.shape
    width = 8 * cw
    ocw = out_att.shape[1] // 8
    nb, na = rows // BLK, rows // (2 * BLK)
    nx = 4
    nz = n_sp // nx
    inverse = (np.float64(ROPE_BASE) ** (-2.0 * (np.arange(128) % 32) / 64)).astype(np.float32)[None, :]
    dma = pltpu.SemaphoreType.DMA
    hbm = pl.BlockSpec(memory_space=pltpu.HBM)
    specs = [hbm] * 15
    specs[9] = pl.BlockSpec(memory_space=pltpu.SMEM)
    vm = pltpu.VMEM
    scratch = [
        vm((8, rows, cw), BF16), vm((width, 640), BF16), vm((256, width), BF16), vm((1, width), F32), vm((1, rows), F32),
        vm((128, 128), F32), vm((1, 128), F32),
        vm((rows, 128), BF16), vm((rows + 2 * BLK, 128), BF16), vm((rows, 128), BF16), vm((rows, 128), BF16), vm((rows, 128), F32),
        vm((rows, 128), F32), vm((rows, 128), F32), vm((nb // 2, 2 * BLK, 640), F32), vm((nb // 2, 2 * BLK, 128), F32), vm((rows, 128), BF16), vm((rows, 128), BF16), vm((rows, 128), BF16), vm((rows, 128), F32),
        vm((nb, 128, 128), F32), vm((nb, 128, 128), BF16),
        vm((8, rows, 128), BF16), vm((8, rows, 128), BF16), vm((2, 8, 128, ocw), BF16), vm((rows, ocw), F32),
        vm((nx, 128, 128), BF16), vm((2, 64, 128), BF16), vm((nz, 64, 128), BF16), vm((nx, 8, 128), F32), vm((nz, 8, 128), F32),
        vm((nb, 128), F32), vm((nb, 128), F32), vm((nb, 128), F32),
        dma((14,)), dma((1,)), dma((3, nb)), dma((na,)), dma((na,)), dma((1,)), dma((3, na)), dma((na,)), dma((na,)),
        dma((1,)), dma((3, nb)), dma((na,)), dma((na,)),
        dma((2,)), dma((2,)), dma((2,)), dma((2, 4)), dma((1,)), dma((1,)), dma((1,)), dma((1,)),
        dma((1,)), dma((1,)), dma((1,)), dma((1,)), dma((2,)), dma((2,)),
    ]
    call = pl.pallas_call(
        functools.partial(kernel, n_sp, nx),
        out_shape=pltpu.VMEM((rows, ocw), BF16),
        in_specs=specs,
        out_specs=pl.BlockSpec(memory_space=pltpu.VMEM),
        scratch_shapes=scratch,
        compiler_params=pltpu.CompilerParams(collective_id=0, has_side_effects=True, vmem_limit_bytes=66_000_000),
        name="layer",
    )
    return call(
        tokens, norm_gain.reshape(1, width), att_query, att_key.T, att_value.T, ret_query.T, ret_key.T, ret_value, ret_gate,
        att_sink, decay_log, init_state.reshape(128, 128), inverse, out_att, out_ret,
    )


def solution(mesh):
    in_specs = (
        P("sp", "tp"), P(), P(None, "tp"), P(None, "tp"), P(None, "tp"), P(None, "tp"), P(None, "tp"), P(None, "tp"), P(None, "tp"),
        P("tp"), P("tp", "sp"), P(None, "tp", None, None), P("tp", None), P("tp", None),
    )
    return jax.shard_map(
        functools.partial(body, n_sp=mesh.shape["sp"]), mesh=mesh, in_specs=in_specs, out_specs=P("sp", "tp"), check_vma=False
    )
```

```python
import functools

import jax
import jax.numpy as jnp
import numpy as np
from jax import lax
from jax.experimental import pallas as pl
from jax.experimental.pallas import tpu as pltpu
from jax.sharding import PartitionSpec as P

HD = 64
RV = 128
BLK = 128
NORM_EPS = 1e-06
ROPE_BASE = 10000.0
MESH = pl.DeviceIdType.MESH
F32 = jnp.float32
BF16 = jnp.bfloat16
NT = (((1,), (1,)), ((), ()))
TN = (((0,), (0,)), ((), ()))
AHEAD = 5

L1, R1, OPP, SIB = 0, 1, 2, 3


def kernel(n_sp, nx, tok_h, gain_h, wq_h, wk_h, wv_h, wrq_h, wrk_h, wrv_h, wrg_h, sink_ref, dec_h, init_h, inv_h, oa_h, or_h,
           OUT,
           X, W1, W2, gain, dec, init, inv, Q, KV, V, G, SG, COS, SIN, ACC, SQ, QR, QB, QX, RL, TT, SL, A, R, WO, OA,
           XS, ZG, ZS, DX, DZ, crow, bl8, pre8,
           lsem, xs_s, xs_r, xn_r, xf_r, as_s, as_r, an_r, af_r, rs_s, rs_r, rn_r, rf_r, w1_s, w1_r, w2_s, w2_r, sx_s, sx_r, dx_s, dx_r, sz_s, sz_r, dz_s, dz_r,
           h_s, h_r):
    rows, cw = tok_h.shape
    nb = rows // BLK
    arows = 2 * BLK
    na = rows // arows
    width = 8 * cw
    ocw = OUT.shape[1]
    nz = n_sp // nx
    quarter = BLK // nx
    s, t = lax.axis_index("sp"), lax.axis_index("tp")
    z, x = s // nx, s % nx
    y, c = t // 2, t % 2
    right = 2 * ((y + 1) % 4) + c
    left = 2 * ((y + 3) % 4) + c
    opp = 2 * ((y + 2) % 4) + c
    sib = 2 * y + (1 - c)
    sib_right = 2 * ((y + 1) % 4) + 1 - c
    sib_left = 2 * ((y + 3) % 4) + 1 - c
    sib_opp = 2 * ((y + 2) % 4) + 1 - c
    up, down = (s + 1) % n_sp, (s + n_sp - 1) % n_sp

    loads = [
        (dec_h, dec), (tok_h, X.at[t]), (gain_h, gain), (inv_h, inv), (init_h, init),
        (wq_h, W1.at[:, 0:128]), (wrv_h, W1.at[:, 128:256]), (wrg_h, W1.at[:, 256:384]),
        (wk_h, W2.at[0:64]), (wv_h, W2.at[64:128]), (wrq_h, W2.at[128:192]), (wrk_h, W2.at[192:256]),
    ]
    mine = pl.ds(pl.multiple_of(x * quarter, quarter), quarter)
    my_cols = pl.ds(pl.multiple_of(t * ocw, 128), ocw)
    loads += [(oa_h.at[mine, my_cols], WO.at[0, t, mine, :]), (or_h.at[mine, my_cols], WO.at[1, t, mine, :])]
    copies = [pltpu.make_async_copy(a, b, lsem.at[i]) for i, (a, b) in enumerate(loads)]
    for cp in copies:
        cp.start()

    barrier = pltpu.get_barrier_semaphore()
    partners = [(s, (t + d) % 8) for d in range(1, 8)]
    partners += [(z * nx + (x + d) % nx, t) for d in range(1, nx)]
    partners += [(((z + d) % nz) * nx + x, t) for d in range(1, nz)]
    has_up, has_down = 1 - (s + 1) // n_sp, (s + n_sp - 1) // n_sp
    for p in reversed(partners):
        pl.semaphore_signal(barrier, inc=1, device_id=p, device_id_type=MESH)

    @pl.when(has_up == 1)
    def _():
        pl.semaphore_signal(barrier, inc=1, device_id=(up, t), device_id_type=MESH)

    @pl.when(has_down == 1)
    def _():
        pl.semaphore_signal(barrier, inc=1, device_id=(down, t), device_id_type=MESH)

    copies[0].wait()
    for b in range(nb):
        crow[b : b + 1, :] = dec[:, b * BLK : (b + 1) * BLK]
    cum = crow[...]
    lane = lax.broadcasted_iota(jnp.int32, (nb, BLK), 1)
    for sh in (1, 2, 4, 8, 16, 32, 64):
        cum = cum + jnp.where(lane >= sh, pltpu.roll(cum, sh, 1), 0.0)
    crow[...] = cum
    bl8[...] = jnp.broadcast_to(cum[:, BLK - 1 : BLK], (nb, BLK))
    run = jnp.zeros((1, BLK), F32)
    for b in range(nb):
        pre8[b : b + 1, :] = run
        run = run + bl8[b : b + 1, :]
    tot = run
    DX[x] = jnp.broadcast_to(tot, (8, BLK))
    for i in range(1, 5):
        copies[i].wait()

    pl.semaphore_wait(barrier, len(partners) + has_up + has_down)

    def put(src, dst, send, recv, dev):
        return pltpu.make_async_remote_copy(src_ref=src, dst_ref=dst, send_sem=send, recv_sem=recv, device_id=dev, device_id_type=MESH)

    def gather(buf, n_rows, ss, rs, near, far):
        group = 2 * BLK // n_rows

        def part(b, k):
            return buf.at[b, pl.ds(pl.multiple_of(k * n_rows, n_rows), n_rows), :]

        def hop(b, k, recv, tp):
            ref = part(b, k)
            return put(ref, ref, ss.at[0], recv, (s, tp))

        def own(k):
            hop(t, k, rs.at[L1, k], right).start()
            hop(t, k, rs.at[R1, k], left).start()
            hop(t, k, near.at[k // group], sib).start()

        def pass_on(k):
            hop(left, k, rs.at[L1, k], right).wait_recv()
            if k % 2 == 0:
                hop(left, k, rs.at[OPP, k], right).start()
            hop(left, k, near.at[k // group], sib).start()
            hop(right, k, rs.at[R1, k], left).wait_recv()
            if k % 2 == 1:
                hop(right, k, rs.at[OPP, k], left).start()
            hop(right, k, near.at[k // group], sib).start()

        def pass_last(k):
            hop(opp, k, rs.at[OPP, k], right).wait_recv()
            hop(opp, k, far.at[k // group], sib).start()

        def two(first, blocks, m):
            return buf.at[pl.ds(first, blocks), pl.ds(pl.multiple_of(m * 2 * BLK, 2 * BLK), 2 * BLK), :]

        def arrived_near(m):
            ref = two(0, 3, m)
            put(ref, ref, ss.at[0], near.at[m], (s, sib)).wait_recv()

        def arrived_far(m):
            ref = two(0, 1, m)
            put(ref, ref, ss.at[0], far.at[m], (s, sib)).wait_recv()

        def sent():
            put(buf.at[0:7], buf.at[0:7], ss.at[0], near.at[0], (s, sib)).wait_send()

        return own, pass_on, pass_last, arrived_near, arrived_far, sent

    own, pass_on, pass_last, arrived_near, arrived_far, sent = gather(X, BLK, xs_s, xs_r, xn_r, xf_r)
    a_own, a_pass, a_last, a_near, a_far, a_sent = gather(A, arows, as_s, as_r, an_r, af_r)
    r_own, r_pass, r_last, r_near, r_far, r_sent = gather(R, BLK, rs_s, rs_r, rn_r, rf_r)

    for k in range(AHEAD):
        own(k)
    for d in range(1, nx):
        put(DX.at[x], DX.at[x], dx_s.at[0], dx_r.at[0], (z * nx + (x + d) % nx, t)).start()

    lane_b = lax.broadcasted_iota(jnp.int32, (BLK, BLK), 1)
    row_b = lax.broadcasted_iota(jnp.int32, (BLK, BLK), 0)
    low = lane_b < 64

    def blk(j):
        return pl.ds(pl.multiple_of(j * BLK, BLK), BLK)

    def column(j):
        row = jnp.broadcast_to(crow[pl.ds(j, 1), :], (BLK, BLK))
        return jnp.sum(jnp.where(lane_b == row_b, row, 0.0), axis=1, keepdims=True)

    def tables(j, carry):
        pos = (s * rows + j * BLK + row_b).astype(F32)
        angle = pos * inv[...]
        scale = jnp.where(low, 1.0, 64**-0.5).astype(F32)
        COS[blk(j), :] = jnp.cos(angle) * scale
        SIN[blk(j), :] = jnp.sin(angle) * jnp.where(lane_b % 64 < 32, -scale, scale)
        return carry

    def pair(m):
        return pl.ds(pl.multiple_of(m * 2 * BLK, 2 * BLK), 2 * BLK)

    def sums(m, acc, squares, blocks):
        for b in blocks:
            cols = pl.ds(pl.multiple_of(b * cw, cw), cw)
            xf = X[b, pair(m), :].astype(F32)
            sq = xf * xf
            squares = squares + sum(sq[:, i : i + 128] for i in range(0, cw, 128))
            acc = acc + jnp.dot((xf * gain[:, cols]).astype(BF16), W1[cols, :], preferred_element_type=F32)
        return acc, squares

    def project_near(m):
        arrived_near(m)
        zero = jnp.zeros((2 * BLK, 640), F32), jnp.zeros((2 * BLK, 128), F32)
        ACC[m], SQ[m] = sums(m, *zero, (t, sib, left, right, sib_left, sib_right))

    def project(m):
        two = pair(m)
        arrived_far(m)
        acc, squares = sums(m, ACC[m], SQ[m], (opp, sib_opp))
        inv_rms = lax.rsqrt(jnp.sum(squares, axis=1, keepdims=True) / width + NORM_EPS)
        p = (acc * inv_rms).astype(BF16)
        Q[two, :] = p[:, 0:128]
        V[two, :] = p[:, 128:256]
        G[two, :] = p[:, 256:384]
        KV[pl.ds(pl.multiple_of(m * 2 * BLK + BLK, BLK), 2 * BLK), :] = p[:, 384:512]
        for h in range(2):
            j = 2 * m + h
            cosine, sine, cc = COS[blk(j), :], SIN[blk(j), :], column(j)
            bl = bl8[pl.ds(j, 1), :]
            pre = pre8[pl.ds(j, 1), :]
            rqk = p[h * BLK : (h + 1) * BLK, 512:640].astype(F32)
            swapped = jnp.where(lane_b % 64 < 32, pltpu.roll(rqk, 96, 1), pltpu.roll(rqk, 32, 1))
            rot = rqk * cosine + swapped * sine
            QR[blk(j), :] = rot.astype(BF16)
            other = pltpu.roll(rot, 64, 1)
            qq = jnp.where(low, rot, other)
            kk = jnp.where(low, other, rot)
            to_end = jnp.exp(bl - cc)
            to_here = jnp.exp(jnp.broadcast_to(cc, (BLK, BLK)))
            QB[blk(j), :] = (qq * jnp.where(low, to_here, to_end)).astype(BF16)
            full = cc + pre
            QX[blk(j), :] = (qq * jnp.exp(jnp.where(low, full, tot - full))).astype(BF16)
            kw = (kk * jnp.where(low, to_end, to_here)).astype(BF16)
            v = p[h * BLK : (h + 1) * BLK, 128:256]
            TT[j] = lax.dot_general(kw, v, TN, preferred_element_type=F32)

    for i in range(5, 14):
        copies[i].wait()
    for b in range(8):
        W1[b * cw : (b + 1) * cw, 384:640] = W2[:, b * cw : (b + 1) * cw].T
    lax.fori_loop(0, nb, tables, 0)

    halo_up = put(KV.at[pl.ds(rows, BLK), :], KV.at[pl.ds(0, BLK), :], h_s.at[0], h_r.at[0], (up, t))
    halo_down = put(KV.at[pl.ds(BLK, BLK), :], KV.at[pl.ds(rows + BLK, BLK), :], h_s.at[1], h_r.at[1], (down, t))

    row_q = lax.broadcasted_iota(jnp.int32, (2 * BLK, BLK), 0) % BLK
    lane_q = lax.broadcasted_iota(jnp.int32, (2 * BLK, BLK), 1)
    sink = jnp.where(lax.broadcasted_iota(jnp.int32, (2 * BLK, 1), 0) < BLK, sink_ref[0], sink_ref[1])

    def attend(j):
        q = Q[blk(j), :]
        q2 = jnp.concatenate([q[:, 0:64], q[:, 64:128]], axis=0)
        kv = KV[pl.ds(pl.multiple_of(j * BLK, BLK), 3 * BLK), :]
        sc = lax.dot_general(q2, kv[:, 0:64], NT, preferred_element_type=F32) * HD**-0.5
        first = jnp.where(s * nb + j == 0, BLK, 0)
        last = jnp.where(s * nb + j == n_sp * nb - 1, BLK, 0)
        s0 = jnp.where(lane_q - first >= row_q, sc[:, 0:128], -jnp.inf)
        s1 = sc[:, 128:256]
        s2 = jnp.where(lane_q + last <= row_q, sc[:, 256:384], -jnp.inf)
        top = jnp.maximum(jnp.max(jnp.maximum(jnp.maximum(s0, s1), s2), axis=1, keepdims=True), sink)
        e0, e1, e2 = jnp.exp(s0 - top), jnp.exp(s1 - top), jnp.exp(s2 - top)
        den = jnp.sum(e0 + e1 + e2, axis=1, keepdims=True) + jnp.exp(sink - top)
        ee = jnp.concatenate([e0.astype(BF16), e1.astype(BF16), e2.astype(BF16)], axis=1)
        o = jnp.dot(ee, kv[:, 64:128], preferred_element_type=F32) / den
        A[t, blk(j), :] = jnp.concatenate([o[0:BLK], o[BLK : 2 * BLK]], axis=1).astype(BF16)

    def weights_out():
        for i, half in enumerate((oa_h, or_h)):
            for d in range(1, 8):
                to = (t + d) % 8
                cols = pl.ds(pl.multiple_of(to * ocw, 128), ocw)
                put(half.at[mine, cols], WO.at[i, t, mine, :], w1_s.at[i], w1_r.at[i], (s, to)).start()

    def on(k):
        pass_on(k)
        if k + AHEAD < nb:
            own(k + AHEAD)

    @pl.when(has_down == 0)
    def _():
        KV[0:BLK, :] = jnp.zeros((BLK, 128), BF16)

    @pl.when(has_up == 0)
    def _():
        KV[rows + BLK : rows + 2 * BLK, :] = jnp.zeros((BLK, 128), BF16)

    on(0)
    on(1)
    on(2)
    on(3)
    project_near(0)
    on(4)
    project_near(1)
    pass_last(0)
    on(5)
    pass_last(1)

    def keys_down():
        @pl.when(has_down == 1)
        def _():
            halo_down.start()

    @pl.when(c == 0)
    def _():
        project_near(2)
        on(6)
        project(0)
        keys_down()
        pass_last(2)
        on(7)
        weights_out()
        pass_last(3)
        project(1)
        project_near(3)
        pass_last(4)
        pass_last(5)
        project(2)
        pass_last(6)
        pass_last(7)
        project(3)

    @pl.when(c == 1)
    def _():
        on(6)
        pass_last(2)
        on(7)
        weights_out()
        project_near(2)
        project(0)
        keys_down()
        pass_last(3)
        pass_last(4)
        pass_last(5)
        project(1)
        pass_last(6)
        project_near(3)
        pass_last(7)
        project(2)
        project(3)

    f = jnp.zeros((64, RV), F32)
    g = jnp.zeros((64, RV), F32)
    for b in range(nb):
        SL[b, 0:64, :] = f.astype(BF16)
        f = jnp.exp(bl8[b : b + 1, :]) * f + TT[b, 0:64, :]
        e = nb - 1 - b
        SL[e, 64:128, :] = g.astype(BF16)
        g = jnp.exp(bl8[e : e + 1, :]) * g + TT[e, 64:128, :]
    XS[x, 0:64, :] = f.astype(BF16)
    XS[x, 64:128, :] = g.astype(BF16)
    for d in sorted(range(1, nx), key=lambda d: -min(d, nx - d)):
        put(XS.at[x], XS.at[x], sx_s.at[0], sx_r.at[0], (z * nx + (x + d) % nx, t)).start()

    @pl.when(has_up == 1)
    def _():
        halo_up.start()


    put(DX.at[0 : nx - 1], DX.at[0 : nx - 1], dx_s.at[0], dx_r.at[0], (s, sib)).wait_recv()
    total = DX[0]
    for i in range(1, nx):
        total = total + DX[i]
    DZ[z] = total
    for d in range(1, nz):
        put(DZ.at[z], DZ.at[z], dz_s.at[0], dz_r.at[0], (((z + d) % nz) * nx + x, t)).start()

    attend(1)
    attend(2)
    attend(3)
    a_own(1)
    attend(4)
    attend(5)
    a_own(2)

    @pl.when(has_up == 1)
    def _():
        halo_down.wait_recv()

    attend(6)
    attend(7)
    a_own(3)

    xr, xl = z * nx + (x + 1) % nx, z * nx + (x + nx - 1) % nx

    def quarter_of(o):
        return pl.ds(pl.multiple_of(((x + o + nx) % nx) * quarter, quarter), quarter)

    def w2_own(i):
        ref = WO.at[i, 0:7, mine, :]
        put(ref, ref, w1_s.at[i], w1_r.at[i], (s, sib)).wait_recv()
        ref = WO.at[i, :, mine, :]
        put(ref, ref, w2_s.at[i], w2_r.at[i, 0], (xr, t)).start()
        put(ref, ref, w2_s.at[i], w2_r.at[i, 1], (xl, t)).start()

    def w2_pass(i):
        from_left = WO.at[i, :, quarter_of(-1), :]
        from_right = WO.at[i, :, quarter_of(1), :]
        put(from_left, from_left, w2_s.at[i], w2_r.at[i, 0], (xr, t)).wait_recv()
        half = WO.at[i, 0:4, quarter_of(-1), :]
        put(half, half, w2_s.at[i], w2_r.at[i, 2], (xr, t)).start()
        put(from_right, from_right, w2_s.at[i], w2_r.at[i, 1], (xl, t)).wait_recv()
        half = WO.at[i, 4:8, quarter_of(1), :]
        put(half, half, w2_s.at[i], w2_r.at[i, 3], (xl, t)).start()

    def w2_done(i):
        half = WO.at[i, 0:4, quarter_of(2), :]
        put(half, half, w2_s.at[i], w2_r.at[i, 2], (xr, t)).wait_recv()
        half = WO.at[i, 4:8, quarter_of(2), :]
        put(half, half, w2_s.at[i], w2_r.at[i, 3], (xl, t)).wait_recv()

    def w2_sent(i):
        ref = WO.at[i, :, 0 : 3 * quarter, :]
        put(ref, ref, w2_s.at[i], w2_r.at[i, 0], (xr, t)).wait_send()

    put(XS.at[0 : nx - 1], XS.at[0 : nx - 1], sx_s.at[0], sx_r.at[0], (s, sib)).wait_recv()
    ex = [jnp.exp(DX[i][0:1, :]) for i in range(nx)]
    fx = jnp.zeros((64, RV), F32)
    gx = jnp.zeros((64, RV), F32)
    fall = jnp.zeros((64, RV), F32)
    gall = jnp.zeros((64, RV), F32)
    dfx = jnp.zeros((1, RV), F32)
    dgx = jnp.zeros((1, RV), F32)
    for i in range(nx):
        term = XS[i, 0:64, :].astype(F32)
        fx = jnp.where(i < x, ex[i] * fx + term, fx)
        dfx = jnp.where(i < x, dfx + DX[i][0:1, :], dfx)
        fall = ex[i] * fall + term
        o = nx - 1 - i
        term = XS[o, 64:128, :].astype(F32)
        gx = jnp.where(o > x, ex[o] * gx + term, gx)
        dgx = jnp.where(o > x, dgx + DX[o][0:1, :], dgx)
        gall = ex[o] * gall + term
    ZG[0] = fall.astype(BF16)
    ZG[1] = gall.astype(BF16)
    ZS[z] = jnp.zeros((64, RV), BF16)
    for d in sorted(range(1, nz), key=lambda d: -min(d, nz - d)):
        put(ZG.at[(z + d) // nz], ZS.at[z], sz_s.at[0], sz_r.at[0], (((z + d) % nz) * nx + x, t)).start()

    w2_own(0)
    w2_own(1)

    @pl.when(has_down == 1)
    def _():
        halo_up.wait_recv()

    attend(0)
    a_own(0)

    def inside(j):
        cc = column(j)
        cr = crow[pl.ds(j, 1), :]
        qk = QR[blk(j), :]
        sc = lax.dot_general(qk[:, 0:64], qk[:, 64:128], NT, preferred_element_type=F32)
        w = (sc * jnp.exp(-jnp.abs(cc - cr))).astype(BF16)
        RL[blk(j), :] = jnp.dot(w, V[blk(j), :], preferred_element_type=F32) + jnp.dot(
            QB[blk(j), :], SL[j], preferred_element_type=F32
        )
        gate = G[blk(j), :].astype(F32)
        SG[blk(j), :] = gate / (1.0 + jnp.exp(-gate))

    def inside_two(m, carry):
        inside(2 * m)
        inside(2 * m + 1)
        return carry


    a_pass(1)
    lax.fori_loop(0, na // 2, inside_two, 0)
    a_pass(2)
    lax.fori_loop(na // 2, na, inside_two, 0)
    a_pass(3)

    sent()
    for i in range(2):
        ref = WO.at[i, 0:7, mine, :]
        put(ref, ref, w1_s.at[i], w1_r.at[i], (s, sib)).wait_send()
    put(XS.at[0 : nx - 1], XS.at[0 : nx - 1], sx_s.at[0], sx_r.at[0], (s, sib)).wait_send()
    put(DX.at[0 : nx - 1], DX.at[0 : nx - 1], dx_s.at[0], dx_r.at[0], (s, sib)).wait_send()

    @pl.when(has_up == 1)
    def _():
        halo_up.wait_send()

    @pl.when(has_down == 1)
    def _():
        halo_down.wait_send()


    a_pass(0)

    if nz > 1:
        put(DZ.at[0 : nz - 1], DZ.at[0 : nz - 1], dz_s.at[0], dz_r.at[0], (s, sib)).wait_recv()
        put(ZS.at[0 : nz - 1], ZS.at[0 : nz - 1], sz_s.at[0], sz_r.at[0], (s, sib)).wait_recv()
    fz = init[0:64, :]
    gz = init[64:128, :]
    for i in range(nz):
        term = ZS[i].astype(F32)
        fz = jnp.where(i < z, jnp.exp(DZ[i][0:1, :]) * fz + term, fz)
        o = nz - 1 - i
        term = ZS[o].astype(F32)
        gz = jnp.where(o > z, jnp.exp(DZ[o][0:1, :]) * gz + term, gz)
    ST = jnp.concatenate([fx + jnp.exp(dfx) * fz, gx + jnp.exp(dgx) * gz], axis=0).astype(BF16)

    def big(k):
        return pl.ds(pl.multiple_of(k * arows, arows), arows)

    def finish(k, carry):
        ret = RL[big(k), :] + jnp.dot(QX[big(k), :], carry, preferred_element_type=F32)
        cen = ret - jnp.mean(ret, axis=1, keepdims=True)
        nrm = cen * lax.rsqrt(jnp.mean(cen * cen, axis=1, keepdims=True) + NORM_EPS)
        R[t, big(k), :] = (SG[big(k), :] * nrm).astype(BF16)
        r_own(2 * k)
        r_own(2 * k + 1)
        return carry

    lax.fori_loop(0, na, finish, ST)

    def out_att(k):
        lhs = jnp.concatenate([A[b, big(k), :] for b in range(8)], axis=1)
        OA[big(k), :] = jnp.dot(lhs, WO[0].reshape(8 * BLK, ocw), preferred_element_type=F32)

    def ret_sum(k, blocks):
        lhs = jnp.concatenate([R[b, big(k), :] for b in blocks], axis=1)
        rhs = jnp.concatenate([WO[1, b] for b in blocks], axis=0)
        return OA[big(k), :] + jnp.dot(lhs, rhs, preferred_element_type=F32)

    def out_near(k):
        r_near(k)
        OA[big(k), :] = ret_sum(k, (t, sib, left, right, sib_left, sib_right))

    def out_ret(k):
        r_far(k)
        OUT[big(k), :] = ret_sum(k, (opp, sib_opp)).astype(BF16)

    for k in range(nb):
        if k == 0:
            for i in range(1, na):
                a_last(i)
            w2_pass(0)
            a_last(0)
            w2_pass(1)
        r_pass(k)
        if k == nb // 2 - 1:
            w2_done(0)
        if nb // 2 <= k < nb - 1:
            a_near(k - nb // 2 + 1)
            a_far(k - nb // 2 + 1)
            out_att(k - nb // 2 + 1)
    a_near(0)
    a_far(0)
    out_att(0)
    for k in range(nb // 2):
        r_last(k)
    w2_done(1)
    a_sent()
    for i in range(2):
        w2_sent(i)
    if nz > 1:
        put(ZS.at[0 : nz - 1], ZS.at[0 : nz - 1], sz_s.at[0], sz_r.at[0], (s, sib)).wait_send()
        put(DZ.at[0 : nz - 1], DZ.at[0 : nz - 1], dz_s.at[0], dz_r.at[0], (s, sib)).wait_send()
    out_near(0)
    out_near(1)
    r_last(4)
    r_last(5)
    out_near(2)
    out_near(3)
    r_last(6)
    r_last(7)
    for k in range(na):
        out_ret(k)

    r_sent()


def body(tokens, norm_gain, att_query, att_key, att_value, ret_query, ret_key, ret_value, ret_gate, att_sink, decay_log, init_state,
         out_att, out_ret, *, n_sp):
    rows, cw = tokens.shape
    width = 8 * cw
    ocw = out_att.shape[1] // 8
    nb, na = rows // BLK, rows // (2 * BLK)
    nx = 4
    nz = n_sp // nx
    inverse = (np.float64(ROPE_BASE) ** (-2.0 * (np.arange(128) % 32) / 64)).astype(np.float32)[None, :]
    dma = pltpu.SemaphoreType.DMA
    hbm = pl.BlockSpec(memory_space=pltpu.HBM)
    specs = [hbm] * 15
    specs[9] = pl.BlockSpec(memory_space=pltpu.SMEM)
    vm = pltpu.VMEM
    scratch = [
        vm((8, rows, cw), BF16), vm((width, 640), BF16), vm((256, width), BF16), vm((1, width), F32), vm((1, rows), F32),
        vm((128, 128), F32), vm((1, 128), F32),
        vm((rows, 128), BF16), vm((rows + 2 * BLK, 128), BF16), vm((rows, 128), BF16), vm((rows, 128), BF16), vm((rows, 128), F32),
        vm((rows, 128), F32), vm((rows, 128), F32), vm((nb // 2, 2 * BLK, 640), F32), vm((nb // 2, 2 * BLK, 128), F32), vm((rows, 128), BF16), vm((rows, 128), BF16), vm((rows, 128), BF16), vm((rows, 128), F32),
        vm((nb, 128, 128), F32), vm((nb, 128, 128), BF16),
        vm((8, rows, 128), BF16), vm((8, rows, 128), BF16), vm((2, 8, 128, ocw), BF16), vm((rows, ocw), F32),
        vm((nx, 128, 128), BF16), vm((2, 64, 128), BF16), vm((nz, 64, 128), BF16), vm((nx, 8, 128), F32), vm((nz, 8, 128), F32),
        vm((nb, 128), F32), vm((nb, 128), F32), vm((nb, 128), F32),
        dma((14,)), dma((1,)), dma((3, nb)), dma((na,)), dma((na,)), dma((1,)), dma((3, na)), dma((na,)), dma((na,)),
        dma((1,)), dma((3, nb)), dma((na,)), dma((na,)),
        dma((2,)), dma((2,)), dma((2,)), dma((2, 4)), dma((1,)), dma((1,)), dma((1,)), dma((1,)),
        dma((1,)), dma((1,)), dma((1,)), dma((1,)), dma((2,)), dma((2,)),
    ]
    call = pl.pallas_call(
        functools.partial(kernel, n_sp, nx),
        out_shape=pltpu.VMEM((rows, ocw), BF16),
        in_specs=specs,
        out_specs=pl.BlockSpec(memory_space=pltpu.VMEM),
        scratch_shapes=scratch,
        compiler_params=pltpu.CompilerParams(collective_id=0, has_side_effects=True, vmem_limit_bytes=66_000_000),
        name="layer",
    )
    return call(
        tokens, norm_gain.reshape(1, width), att_query, att_key.T, att_value.T, ret_query.T, ret_key.T, ret_value, ret_gate,
        att_sink, decay_log, init_state.reshape(128, 128), inverse, out_att, out_ret,
    )


def solution(mesh):
    in_specs = (
        P("sp", "tp"), P(), P(None, "tp"), P(None, "tp"), P(None, "tp"), P(None, "tp"), P(None, "tp"), P(None, "tp"), P(None, "tp"),
        P("tp"), P("tp", "sp"), P(None, "tp", None, None), P("tp", None), P("tp", None),
    )
    return jax.shard_map(
        functools.partial(body, n_sp=mesh.shape["sp"]), mesh=mesh, in_specs=in_specs, out_specs=P("sp", "tp"), check_vma=False
    )
```
